256 devices in a mesh: ep: 16 (over y, x), tp: 16 (over z, core).
Axes of the slice: x: 4, y: 4, z: 8, core: 2. Of those that a mesh axis runs over, the one named last changes fastest.
Arguments:
- tokens: bfloat16 [512, 4096], P('ep'), may hold values from -6 to 6
- state_matrix: float32 [512, 16, 128, 128], P('ep', 'tp'), may hold values from -1.5 to 1.5
- state_norm: float32 [512, 16, 128], P('ep', 'tp'), may hold values from -4 to 4
- state_max: float32 [512, 16], P('ep', 'tp'), may hold values from -5 to 5
- mixer_gain: float32 [4096], replicated, may hold values from 0.1 to 1.9
- w_query: bfloat16 [4096, 2048], P('ep', 'tp'), may hold values from -0.09375 to 0.09375
- w_key: bfloat16 [4096, 2048], P('ep', 'tp'), may hold values from -0.09375 to 0.09375
- w_value: bfloat16 [4096, 2048], P('ep', 'tp'), may hold values from -0.09375 to 0.09375
- w_outgate: bfloat16 [4096, 2048], P('ep', 'tp'), may hold values from -0.09375 to 0.09375
- w_ingate: bfloat16 [4096, 16], replicated, may hold values from -0.09375 to 0.09375
- w_forget: bfloat16 [4096, 16], replicated, may hold values from -0.09375 to 0.09375
- forget_bias: float32 [16], replicated, may hold values from -2 to 4
- w_proj: bfloat16 [2048, 4096], P('tp', 'ep'), may hold values from -0.125 to 0.125
- ffn_gain: float32 [4096], replicated, may hold values from 0.1 to 1.9
- w_branch: bfloat16 [4096], replicated, may hold values from -0.09375 to 0.09375
- routes: int32 [512, 2], P('ep'), may hold values from 0 to 15, all different within a row; in each aligned block of 32 rows (0 to 31, 32 to 63, ...) at most 6 rows name the same one
- route_weight: float32 [512, 2], P('ep'), may hold values from 0.2 to 1
- expert_gate: bfloat16 [16, 4096, 4096], P('ep', None, 'tp'), may hold values from -0.09375 to 0.09375
- expert_up: bfloat16 [16, 4096, 4096], P('ep', None, 'tp'), may hold values from -0.09375 to 0.09375
- expert_down: bfloat16 [16, 4096, 4096], P('ep', 'tp'), may hold values from -0.09375 to 0.09375
- dense_gate: bfloat16 [4096, 8192], P('ep', 'tp'), may hold values from -0.09375 to 0.09375
- dense_up: bfloat16 [4096, 8192], P('ep', 'tp'), may hold values from -0.09375 to 0.09375
- dense_down: bfloat16 [8192, 4096], P('tp', 'ep'), may hold values from -0.0625 to 0.0625
Outputs:
- layer_out: bfloat16 [512, 4096], P('ep')
- new_matrix: float32 [512, 16, 128, 128], P('ep', 'tp')
- new_norm: float32 [512, 16, 128], P('ep', 'tp')
- new_max: float32 [512, 16], P('ep', 'tp')
The draws below stay inside these ranges and needn't reach their ends.
Inputs may be any that keep to these rules, and one draw needn't show every extreme that they name: `routes`: each row names 2 different experts. Among the rows of one index of ep (32 sequences) no expert is named more than 6 times, and in some such group one expert is named exactly 6 times.
All inputs are finite; a program needn't handle non-finite values.
Results may differ from the reference program's by a relative error of at most 0.012.
Values may be sent and summed in bfloat16 or wider, within the bound.
A program may use at most 64 MiB of HBM per device.

```python
import math
import jax
import jax.numpy as jnp
import numpy as np
from jax import lax

D = 4096
HEADS = 16
HDIM = 128
MW = 2048
FFD = 8192
FFE = 4096
TOPK = 2
SEQS = 32
BATCH = 512
EXPERTS = 16
CAP = 6
N_EP = 16


def shard_levels(stream_key, shape, pieces, low, high):
    def one(axis_at, parts):
        draws = jax.random.uniform(jax.random.fold_in(jax.random.fold_in(stream_key, 6), axis_at), (parts,), jnp.float32, low / len(pieces), high / len(pieces))
        return jnp.repeat(jnp.exp(draws), shape[axis_at] // parts).reshape((-1,) + (1,) * (len(shape) - axis_at - 1))

    level = one(*pieces[0])
    for cut in pieces[1:]:
        level = level * one(*cut)
    return level


def shared_out(key, own, number, rows, amount, top, limit, slope):
    ranking = jax.random.permutation(key, amount)
    crowded, usual = load_shares(amount, rows * top, limit, slope, True), load_shares(amount, rows * top, limit, slope, False)
    places = jnp.arange(amount)

    def named(lengths, turn):
        used = int((lengths > 0).sum())
        fixed = max(1, used // 4)
        shifted = fixed + (places - fixed + turn * (used - fixed)) % max(1, amount - fixed)
        return jnp.zeros((amount,), jnp.int32).at[ranking[jnp.where(places < fixed, places, shifted)]].set(jnp.asarray(lengths, jnp.int32))

    lengths = jnp.where(number % 4 == 0, named(crowded, number // 4), named(usual, number - number // 4 - 1))
    mixed = jax.random.permutation(jax.random.fold_in(own, 3), amount)
    giver, receiver = mixed[0:amount // 2 * 2:2], mixed[1:amount // 2 * 2:2]
    slack = jnp.minimum(lengths[giver] - 1, limit - lengths[receiver]) // 2
    slack = jnp.where((giver == ranking[0]) | (receiver == ranking[0]) | (lengths[receiver] == 0), 0, jnp.maximum(slack, 0))
    shifted = jax.random.randint(jax.random.fold_in(own, 4), (amount // 2,), 0, 1 << 20) % (slack + 1)
    lengths = lengths.at[giver].add(-shifted).at[receiver].add(shifted)
    members = jnp.searchsorted(jnp.cumsum(lengths), jnp.arange(rows * top), side="right").astype(jnp.int32)
    grid = members.reshape(top, rows).T
    grid = grid[jax.random.permutation(jax.random.fold_in(own, 1), rows)]
    turn = jax.random.randint(jax.random.fold_in(own, 2), (rows, 1), 0, top)
    return jnp.take_along_axis(grid, (jnp.arange(top)[None, :] + turn) % top, axis=1)


def load_shares(number_of, total, limit, lean, full):
    portions = [(1 << 20) // math.isqrt(standing ** lean) + 1 for standing in range(1, number_of + 1)]
    largest = limit if full else min(limit, max(-(-total // number_of), total * portions[0] // sum(portions)))
    least = 1 if total - largest >= number_of - 1 else 0
    given, surplus = [largest] + [least] * (number_of - 1), total - largest - least * (number_of - 1)
    while surplus > 0:
        movable = [i for i in range(1, number_of) if given[i] < largest] or [i for i in range(1, number_of) if given[i] < limit]
        pool, left = sum([portions[i] for i in movable]), surplus
        for i in movable:
            addition = min(limit - given[i], max(1, left * portions[i] // pool), surplus)
            given[i] = given[i] + addition
            surplus = surplus - addition
    return np.array(given)


def bell_draw(stream_key, extent, spread, reach, pieces=(), held_as=jnp.bfloat16):
    result = spread * jax.random.normal(stream_key, extent, jnp.float32)
    if pieces:
        result = result * shard_levels(stream_key, extent, pieces, -0.22, 0.18)
    return jnp.clip(result, -reach, reach).astype(held_as)


def setup_inputs(seed: int = 0) -> dict:
    key_of = jax.random.split(jax.random.key(seed), 24)
    tokens = bell_draw(key_of[0], (BATCH, D), 1.0, 6.0, ((0, 16),))
    state_matrix = bell_draw(key_of[1], (BATCH, HEADS, HDIM, HDIM), 0.1, 1.5, ((0, 16), (1, 16)), jnp.float32)
    state_norm = bell_draw(key_of[2], (BATCH, HEADS, HDIM), 0.3, 4.0, ((0, 16), (1, 16)), jnp.float32)
    state_max = bell_draw(key_of[3], (BATCH, HEADS), 1.0, 5.0, ((0, 16), (1, 16)), jnp.float32)
    mixer_gain = jnp.clip(1.0 + 0.18 * jax.random.normal(key_of[4], (D,), jnp.float32), 0.1, 1.9)
    w_query = bell_draw(key_of[5], (D, MW), D ** -0.5, 0.09375, ((0, 16), (1, 16)))
    w_key = bell_draw(key_of[6], (D, MW), D ** -0.5, 0.09375, ((0, 16), (1, 16)))
    w_value = bell_draw(key_of[7], (D, MW), D ** -0.5, 0.09375, ((0, 16), (1, 16)))
    w_outgate = bell_draw(key_of[8], (D, MW), D ** -0.5, 0.09375, ((0, 16), (1, 16)))
    w_ingate = bell_draw(key_of[9], (D, HEADS), D ** -0.5, 0.09375)
    w_forget = bell_draw(key_of[10], (D, HEADS), D ** -0.5, 0.09375)
    forget_bias = jnp.clip(jax.random.uniform(key_of[11], (HEADS,), jnp.float32, -2.0, 4.0), -2.0, 4.0)
    w_proj = bell_draw(key_of[12], (MW, D), MW ** -0.5, 0.125, ((0, 16), (1, 16)))
    ffn_gain = jnp.clip(1.0 + 0.18 * jax.random.normal(key_of[13], (D,), jnp.float32), 0.1, 1.9)
    w_branch = bell_draw(key_of[14], (D,), D ** -0.5, 0.09375)
    routes_keys = jax.random.split(jax.random.fold_in(key_of[15], 1), BATCH // SEQS)
    routes_turns = jax.random.permutation(jax.random.fold_in(key_of[15], 3), BATCH // SEQS)
    routes = jax.vmap(lambda own, number: shared_out(jax.random.fold_in(key_of[15], 2), own, number, SEQS, EXPERTS, TOPK, CAP, 2))(routes_keys, routes_turns).reshape((BATCH, TOPK))
    route_weight = jnp.clip(jnp.exp(math.log(1.0) - 1.609438 * jax.random.uniform(key_of[16], (BATCH, TOPK), jnp.float32) ** shard_levels(key_of[16], (BATCH, TOPK), ((0, 16),), -0.2, 0.2)), 0.2, 1.0)
    expert_gate = bell_draw(key_of[17], (EXPERTS, D, FFE), D ** -0.5, 0.09375, ((0, 16), (2, 16)))
    expert_up = bell_draw(key_of[18], (EXPERTS, D, FFE), D ** -0.5, 0.09375, ((0, 16), (2, 16)))
    expert_down = bell_draw(key_of[19], (EXPERTS, FFE, D), FFE ** -0.5, 0.09375, ((0, 16), (1, 16)))
    dense_gate = bell_draw(key_of[20], (D, FFD), D ** -0.5, 0.09375, ((0, 16), (1, 16)))
    dense_up = bell_draw(key_of[21], (D, FFD), D ** -0.5, 0.09375, ((0, 16), (1, 16)))
    dense_down = bell_draw(key_of[22], (FFD, D), FFD ** -0.5, 0.0625, ((0, 16), (1, 16)))
    return dict(tokens=tokens, state_matrix=state_matrix, state_norm=state_norm, state_max=state_max, mixer_gain=mixer_gain, w_query=w_query, w_key=w_key, w_value=w_value, w_outgate=w_outgate, w_ingate=w_ingate, w_forget=w_forget, forget_bias=forget_bias, w_proj=w_proj, ffn_gain=ffn_gain, w_branch=w_branch, routes=routes, route_weight=route_weight, expert_gate=expert_gate, expert_up=expert_up, expert_down=expert_down, dense_gate=dense_gate, dense_up=dense_up, dense_down=dense_down)


EPS = 1e-06

def rms_scale(values, gain):
    wide = values.astype(jnp.float32)
    return wide * lax.rsqrt(lax.optimization_barrier(jnp.mean(wide * wide, axis=-1, keepdims=True)) + EPS) * gain.astype(jnp.float32)

def slot_numbers(flat_routes, experts_all):
    onehot = (flat_routes[:, None] == jnp.arange(experts_all, dtype=jnp.int32)[None, :]).astype(jnp.int32)
    before = jnp.cumsum(onehot, axis=0) - onehot
    return lax.optimization_barrier(jnp.sum(before * onehot, axis=1)).astype(jnp.int32)

def memory_step(query_all, key_all, value_all, outgate, gate_in, gate_forget, state_matrix, state_norm, state_max):
    row_count, head_count = gate_in.shape
    head_size = state_matrix.shape[-1]
    heads_q = query_all.reshape(row_count, head_count, head_size)
    heads_k = key_all.reshape(row_count, head_count, head_size) * head_size ** (-0.5)
    heads_v = value_all.reshape(row_count, head_count, head_size)
    log_keep = jax.nn.log_sigmoid(gate_forget)
    new_max = jnp.maximum(log_keep + state_max, gate_in)
    keep_factor = jnp.exp(log_keep + state_max - new_max)
    write_factor = jnp.exp(gate_in - new_max)
    new_matrix = keep_factor[:, :, None, None] * state_matrix + write_factor[:, :, None, None] * heads_k[:, :, :, None] * heads_v[:, :, None, :]
    new_norm = keep_factor[:, :, None] * state_norm + write_factor[:, :, None] * heads_k
    numer = jnp.einsum('bhk,bhkv->bhv', heads_q, new_matrix, precision=lax.Precision.HIGHEST)
    denom = lax.optimization_barrier(jnp.sum(heads_q * new_norm, axis=-1))
    cell = numer / jnp.maximum(jnp.abs(denom), 1.0)[:, :, None]
    gated = jax.nn.sigmoid(outgate.reshape(row_count, head_count, head_size)) * cell
    mixed_heads = gated.reshape(row_count, head_count * head_size).astype(jnp.bfloat16)
    return (mixed_heads, new_matrix, new_norm, new_max)

def reference(tokens, state_matrix, state_norm, state_max, mixer_gain, w_query, w_key, w_value, w_outgate, w_ingate, w_forget, forget_bias, w_proj, ffn_gain, w_branch, routes, route_weight, expert_gate, expert_up, expert_down, dense_gate, dense_up, dense_down):
    normed = rms_scale(tokens, mixer_gain).astype(jnp.bfloat16)
    query_all = jnp.dot(normed, w_query, preferred_element_type=jnp.float32)
    key_all = jnp.dot(normed, w_key, preferred_element_type=jnp.float32)
    value_all = jnp.dot(normed, w_value, preferred_element_type=jnp.float32)
    outgate = jnp.dot(normed, w_outgate, preferred_element_type=jnp.float32)
    gate_in = jnp.dot(normed, w_ingate, preferred_element_type=jnp.float32)
    gate_forget = jnp.dot(normed, w_forget, preferred_element_type=jnp.float32) + forget_bias
    mixed_heads, new_matrix, new_norm, new_max = memory_step(query_all, key_all, value_all, outgate, gate_in, gate_forget, state_matrix, state_norm, state_max)
    mixer_out = jnp.dot(mixed_heads, w_proj, preferred_element_type=jnp.float32)
    residual = (tokens.astype(jnp.float32) + mixer_out).astype(jnp.bfloat16)
    ffn_in = rms_scale(residual, ffn_gain).astype(jnp.bfloat16)
    branch_share = jax.nn.sigmoid(jnp.dot(ffn_in, w_branch, preferred_element_type=jnp.float32))
    dense_hidden = (jax.nn.silu(jnp.dot(ffn_in, dense_gate, preferred_element_type=jnp.float32)) * jnp.dot(ffn_in, dense_up, preferred_element_type=jnp.float32)).astype(jnp.bfloat16)
    dense_out = jnp.dot(dense_hidden, dense_down, preferred_element_type=jnp.float32)
    group_routes = routes.reshape(N_EP, SEQS * TOPK)
    slots = jax.vmap(lambda group_row: slot_numbers(group_row, EXPERTS))(group_routes)
    group_ids = jnp.broadcast_to(jnp.arange(N_EP, dtype=jnp.int32)[:, None], group_routes.shape)
    repeated = jnp.repeat(ffn_in, TOPK, axis=0).reshape(N_EP, SEQS * TOPK, D)
    buffers = jnp.zeros((EXPERTS, N_EP, CAP, D), jnp.bfloat16).at[group_routes, group_ids, slots].set(repeated)

    def one_expert(index):
        rows_in = buffers[index].reshape(N_EP * CAP, D)
        hidden = (jax.nn.silu(jnp.dot(rows_in, expert_gate[index], preferred_element_type=jnp.float32)) * jnp.dot(rows_in, expert_up[index], preferred_element_type=jnp.float32)).astype(jnp.bfloat16)
        return jnp.dot(hidden, expert_down[index], preferred_element_type=jnp.float32).reshape(N_EP, CAP, D)
    results = lax.map(one_expert, jnp.arange(EXPERTS, dtype=jnp.int32))
    picked = results[group_routes, group_ids, slots].reshape(N_EP * SEQS, TOPK, D)
    shares = route_weight / lax.optimization_barrier(jnp.sum(route_weight, axis=1, keepdims=True))
    expert_rows = lax.optimization_barrier(jnp.sum(shares[:, :, None] * picked, axis=1))
    total_ffn = expert_rows + branch_share[:, None] * dense_out
    layer_out = (residual.astype(jnp.float32) + total_ffn).astype(jnp.bfloat16)
    return (layer_out, new_matrix, new_norm, new_max)
```

```python
import functools

import jax
import jax.numpy as jnp
from jax import lax
from jax.experimental import pallas as pl
from jax.experimental.pallas import tpu as pltpu
from jax.sharding import PartitionSpec as P

EPS = 1e-06
LANES = 128
CAP = 6
PAD = 8
F32 = jnp.float32
BF16 = jnp.bfloat16
MESH = pl.DeviceIdType.MESH


def dot(a, b):
    return jnp.dot(a, b, preferred_element_type=F32)


def dot_t(a, b):
    return lax.dot_general(a, b, (((1,), (1,)), ((), ())), preferred_element_type=F32)


def iota(shape, dim):
    return lax.broadcasted_iota(jnp.int32, shape, dim)


def layer_kernel(
    n_ep,
    n_tp,
    tokens_ref,
    gain_ref,
    win_ref,
    wfo_ref,
    bias_ref,
    norm_ref,
    smax_ref,
    fgain_ref,
    branch_ref,
    routes_ref,
    weight_ref,
    state_hbm,
    wq_hbm,
    wk_hbm,
    wv_hbm,
    wo_hbm,
    wproj_hbm,
    eg_hbm,
    eu_hbm,
    ed_hbm,
    dg_hbm,
    du_hbm,
    dd_hbm,
    out_ref,
    norm_out_ref,
    max_out_ref,
    keyw_ref,
    value_ref,
    keep_ref,
    state,
    wcat,
    wproj,
    eg,
    eu,
    ed,
    dgu,
    dd,
    nrm,
    x_all,
    info,
    info_recv,
    part_send,
    part_recv,
    numer,
    mix_send,
    mix_all,
    raw_blk,
    res_all,
    res_t,
    xg,
    gmat,
    stat,
    stat_recv,
    dense_send,
    dense_recv,
    disp_send,
    xrecv,
    hid_all,
    fin_send,
    fin_recv,
    dn_send,
    dn_recv,
    tp_send,
    tp_recv,
    out_all,
    load_sems,
    send_ep,
    recv_ep,
    send_tp,
    recv_tp,
    send_mx,
    recv_mx,
    send_tr,
    recv_tr,
):
    e = lax.axis_index("ep")
    t = lax.axis_index("tp")
    R, D = tokens_ref.shape
    N = R * n_ep
    Dc = D // n_ep
    Dt = D // n_tp
    W = mix_send.shape[1]
    F = dd.shape[0]
    EX = {16: 4, 4: 2}[n_ep]
    EY = n_ep // EX
    TZ = n_tp // 2
    S = CAP * n_ep
    S8 = PAD * n_ep
    Q = N // LANES
    PER = LANES // R
    RC = R * EX
    ey, ex = e // EX, lax.rem(e, EX)
    tz, tc = t // 2, lax.rem(t, 2)

    def at(index, size):
        return pl.ds(pl.multiple_of(index * size, size), size)

    def ring(d, n):
        return min(d, n - d)

    ep_far = sorted(range(1, n_ep), key=lambda k: -(ring(k // EX, EY) + ring(k % EX, EX)))
    tp_far = sorted(range(1, n_tp), key=lambda k: -(ring(k // 2, TZ) * 2 + k % 2))
    dy_far = sorted(range(EY), key=lambda d: -ring(d, EY))
    dx_far = sorted(range(EX), key=lambda d: -ring(d, EX))

    def ep_peer(k):
        return lax.rem(ey + k // EX, EY) * EX + lax.rem(ex + k % EX, EX)

    def tp_peer(k):
        return lax.rem(tz + k // 2, TZ) * 2 + lax.rem(tc + k % 2, 2)

    loads = []

    def load(src, dst):
        copy = pltpu.make_async_copy(src, dst, load_sems.at[len(loads)])
        copy.start()
        loads.append(copy)
        return copy

    pending = []

    def ep_start(phase, k, src, dst):
        copy = pltpu.make_async_remote_copy(
            src_ref=src,
            dst_ref=dst,
            send_sem=send_ep.at[phase, k],
            recv_sem=recv_ep.at[phase, k],
            device_id={"ep": ep_peer(k)},
            device_id_type=MESH,
        )
        copy.start()
        pending.append(copy)
        return copy

    def tp_start(phase, k, src, dst):
        copy = pltpu.make_async_remote_copy(
            src_ref=src,
            dst_ref=dst,
            send_sem=send_tp.at[phase, k],
            recv_sem=recv_tp.at[phase, k],
            device_id={"tp": tp_peer(k)},
            device_id_type=MESH,
        )
        copy.start()
        pending.append(copy)
        return copy

    def cross(phase, src, dst):
        return pltpu.make_async_remote_copy(
            src_ref=src,
            dst_ref=dst,
            send_sem=send_tr.at[phase],
            recv_sem=recv_tr.at[phase],
            device_id={"ep": t, "tp": e},
            device_id_type=MESH,
        )

    barrier = pltpu.get_barrier_semaphore()
    for k in ep_far:
        pl.semaphore_signal(barrier, inc=1, device_id={"ep": ep_peer(k)}, device_id_type=MESH)
    for k in tp_far:
        pl.semaphore_signal(barrier, inc=1, device_id={"tp": tp_peer(k)}, device_id_type=MESH)

    load_w = [
        load(src, wcat.at[:, pl.ds(i * W, W)])
        for i, src in enumerate((wq_hbm, wk_hbm, wv_hbm, wo_hbm))
    ]
    load_proj = load(wproj_hbm, wproj.at[at(t, W), :])
    load_state = load(state_hbm, state)
    load_dg, load_du = load(dg_hbm, dgu.at[:, pl.ds(0, F)]), load(du_hbm, dgu.at[:, pl.ds(F, F)])
    load_eg, load_eu = load(eg_hbm, eg), load(eu_hbm, eu)
    load_ed, load_dd = load(ed_hbm, ed), load(dd_hbm, dd)

    wide = tokens_ref[...].astype(F32)
    scale = lax.rsqrt(jnp.mean(wide * wide, axis=-1, keepdims=True) + EPS)
    nrm[...] = (wide * scale * gain_ref[...]).astype(BF16)

    r0, r1 = routes_ref[0:1, :], routes_ref[1:2, :]
    w0, w1 = weight_ref[0:1, :], weight_ref[1:2, :]
    total = w0 + w1
    which = iota((n_ep, R), 0)
    hit0, hit1 = which == r0, which == r1
    named = jnp.where(jnp.logical_or(hit0, hit1), 1.0, 0.0)
    earlier = jnp.where(iota((R, R), 0) < iota((R, R), 1), 1.0, 0.0).astype(BF16)
    slot = dot(named.astype(BF16), earlier)
    code = jnp.where(named > 0.0, slot + 1.0, 0.0)
    group_at = (e * CAP).astype(F32)
    rowcode = jnp.where(named > 0.0, slot + (1.0 + group_at), 0.0)
    shares = jnp.where(hit0, w0 / total, 0.0) + jnp.where(hit1, w1 / total, 0.0)
    info[:, 0:R] = rowcode
    info[:, R : 2 * R] = shares
    info[:, 2 * R : LANES] = jnp.zeros((n_ep, LANES - 2 * R), F32)

    pl.semaphore_wait(barrier, n_ep - 1 + n_tp - 1)
    got_x = {k: ep_start(0, k, nrm.at[:, at(ep_peer(k), Dc)], x_all.at[at(e, R), :]) for k in ep_far}
    x_all[at(e, R), :] = nrm[:, at(e, Dc)]
    load_proj.wait()
    got_wp = {
        k: tp_start(0, k, wproj.at[at(t, W), :], wproj.at[at(t, W), :]) for k in tp_far
    }

    gate_in = dot_t(nrm[...], win_ref[...])
    gate_fo = dot_t(nrm[...], wfo_ref[...]) + bias_ref[...]
    mine = iota(gate_in.shape, 1) == t
    g_in = jnp.sum(jnp.where(mine, gate_in, 0.0), axis=1, keepdims=True)
    g_fo = jnp.sum(jnp.where(mine, gate_fo, 0.0), axis=1, keepdims=True)
    eye = iota((R, R), 0) == iota((R, R), 1)
    smax = jnp.sum(jnp.where(eye, smax_ref[...], 0.0), axis=1, keepdims=True)
    log_keep = jnp.minimum(g_fo, 0.0) - jnp.log(1.0 + jnp.exp(-jnp.abs(g_fo)))
    carried = log_keep + smax
    new_max = jnp.maximum(carried, g_in)
    keep = jnp.exp(carried - new_max)
    write = jnp.exp(g_in - new_max)
    max_out_ref[...] = jnp.sum(jnp.where(eye, new_max, 0.0), axis=0, keepdims=True)
    keep_ref[...] = jnp.broadcast_to(keep, keep_ref.shape)

    for copy in load_w:
        copy.wait()
    got_part = {}
    for dy in [(EY - d) % EY for d in range(EY)]:
        back = (EY - dy) % EY
        for dx in range(EX):
            k = dy * EX + dx
            if k:
                got_x[k].wait_recv()
        rows = at(lax.rem(ey + back, EY), RC)
        part_send[rows, :] = dot(x_all[rows, :], wcat[...]).astype(BF16)
        for dx in dx_far:
            k = back * EX + dx
            if k:
                got_part[k] = ep_start(1, k, part_send.at[at(ep_peer(k), R), :], part_recv.at[k])
    got_info = {k: ep_start(2, k, info, info_recv.at[k]) for k in ep_far}

    @pl.when(e != t)
    def _():
        cross(0, tokens_ref.at[:, at(t, Dc)], raw_blk).start()

    @pl.when(e == t)
    def _():
        raw_blk[...] = tokens_ref[:, at(t, Dc)]

    proj = part_send[at(e, R), :].astype(F32)
    for k in reversed(ep_far):
        got_part[k].wait_recv()
        proj += part_recv[k].astype(F32)

    load_state.wait()
    q = proj[:, 0:W]
    key = proj[:, W : 2 * W] * W ** (-0.5)
    val = proj[:, 2 * W : 3 * W]
    og = proj[:, 3 * W : 4 * W]
    key_w = write * key
    new_norm = keep * norm_ref[...] + key_w
    q_t = q.T
    for b in range(R):
        numer[b : b + 1, :] = jnp.sum(q_t[:, b : b + 1] * state[b, 0], axis=0, keepdims=True)
    top = keep * numer[...] + jnp.sum(q * key_w, axis=1, keepdims=True) * val
    denom = jnp.sum(q * new_norm, axis=1, keepdims=True)
    cell = top / jnp.maximum(jnp.abs(denom), 1.0)
    mix_send[...] = (cell / (1.0 + jnp.exp(-og))).astype(BF16)

    def mix_copy(k):
        return pltpu.make_async_remote_copy(
            src_ref=mix_send,
            dst_ref=mix_all.at[:, at(t, W)],
            send_sem=send_mx.at[k],
            recv_sem=recv_mx.at[t],
            device_id={"ep": ep_peer(k), "tp": e},
            device_id_type=MESH,
        )

    for k in ep_far:
        mix_copy(k).start()

    @pl.when(e != t)
    def _():
        mix_copy(0).start()

    @pl.when(e == t)
    def _():
        mix_all[:, at(t, W)] = mix_send[...]

    norm_out_ref[...] = new_norm
    keyw_ref[...] = key_w
    value_ref[...] = val

    for k in ep_far:
        got_info[k].wait_recv()
    quarter = iota((n_ep, LANES), 1) // R
    codes, sharesl = [], []

    info_recv[0] = info[...]
    for qq in range(Q):
        ctile = jnp.zeros((n_ep, LANES), F32)
        stile = jnp.zeros((n_ep, LANES), F32)
        for j in range(PER):
            g = qq * PER + j
            gy, gx = g // EX, g % EX
            slot_k = lax.rem(ey + (EY - gy), EY) * EX + lax.rem(ex + (EX - gx), EX)
            tile = info_recv[slot_k]
            there = quarter == j
            ctile += jnp.where(there, tile if j == 0 else pltpu.roll(tile, j * R, 1), 0.0)
            back = (j - 1) % PER * R
            stile += jnp.where(there, tile if back == 0 else pltpu.roll(tile, back, 1), 0.0)
        codes.append(ctile)
        sharesl.append(stile)
    code_all = jnp.concatenate(codes, axis=1) if Q > 1 else codes[0]
    share_all = jnp.concatenate(sharesl, axis=1) if Q > 1 else sharesl[0]
    row_no = (iota((S, N), 0) + 1).astype(F32)
    for p in range(n_ep):
        gmat[p * S : (p + 1) * S, :] = jnp.where(row_no == code_all[p : p + 1, :], 1.0, 0.0).astype(
            BF16
        )
    is_mine = iota((n_ep, N), 0) == e
    my_code = jnp.sum(jnp.where(is_mine, code_all, 0.0), axis=0, keepdims=True)
    my_share = jnp.sum(jnp.where(is_mine, share_all, 0.0), axis=0, keepdims=True)
    my_code8 = jnp.where(
        my_code > 0.0, my_code + ((PAD - CAP) * (iota((1, N), 1) // R)).astype(F32), 0.0
    )
    row_share = jnp.sum(
        jnp.where((iota((S8, N), 0) + 1).astype(F32) == my_code8, my_share, 0.0),
        axis=1,
        keepdims=True,
    )
    spread = jnp.where(
        jnp.logical_and(
            iota((S8, S), 0) // PAD * CAP + iota((S8, S), 0) % PAD == iota((S8, S), 1),
            iota((S8, S), 0) % PAD < CAP,
        ),
        1.0,
        0.0,
    ).astype(BF16)
    repeat = jnp.where(iota((S8, n_ep), 0) // PAD == iota((S8, n_ep), 1), 1.0, 0.0).astype(BF16)
    code_rep = dot(repeat, code.astype(BF16))
    pick_t = jnp.where((iota((S8, R), 0) % PAD + 1).astype(F32) == code_rep, 1.0, 0.0)
    pick = pick_t.T.astype(BF16)

    for k in tp_far:
        got_wp[k].wait_recv()

    @pl.when(e != t)
    def _():
        cross(0, tokens_ref.at[:, at(t, Dc)], raw_blk).wait()

    for tt in range(n_tp):

        @pl.when(jnp.logical_or(e != t, t != tt))
        def _():
            pltpu.make_async_remote_copy(
                src_ref=mix_send,
                dst_ref=mix_all.at[:, pl.ds(tt * W, W)],
                send_sem=send_mx.at[0],
                recv_sem=recv_mx.at[tt],
                device_id={"ep": t, "tp": e},
                device_id_type=MESH,
            ).wait_recv()

    mine_res = raw_blk[...].astype(F32) + dot(mix_all[...], wproj[...])
    res_all[at(t, R), :] = mine_res.astype(BF16)
    got_res = {
        k: tp_start(1, k, res_all.at[at(t, R), :], res_all.at[at(t, R), :]) for k in tp_far
    }

    @pl.when(e != t)
    def _():
        cross(1, res_all.at[at(t, R), :], res_t).start()

    @pl.when(e == t)
    def _():
        res_t[...] = res_all[at(t, R), :]

    load_dg.wait()
    load_du.wait()
    my_fgain = fgain_ref[:, at(e, Dc)]
    wide_branch = branch_ref[...].astype(F32)
    pieces = Dc // LANES
    branch_rows = [
        jnp.sum(
            jnp.where(iota(wide_branch.shape, 0) == e * pieces + i, wide_branch, 0.0),
            axis=0,
            keepdims=True,
        )
        for i in range(pieces)
    ]
    my_branch = jnp.concatenate(branch_rows, axis=1) if pieces > 1 else branch_rows[0]
    my_branch = jnp.broadcast_to(my_branch, (8, Dc)).astype(BF16)
    ones = jnp.ones((8, Dc), BF16)

    for k in reversed(tp_far):
        got_res[k].wait_recv()
    block = res_all[...].astype(F32)
    xg[...] = (block * my_fgain).astype(BF16)
    square = block * block
    high = square.astype(BF16)
    low = (square - high.astype(F32)).astype(BF16)
    sums = dot_t(ones, high) + dot_t(ones, low)
    branch = dot_t(my_branch, xg[...])
    row8 = iota((8, LANES), 0)
    tile = jnp.zeros((8, LANES), F32)
    for qq in range(Q):
        cols = slice(qq * LANES, (qq + 1) * LANES)
        tile += jnp.where(row8 == qq, sums[:, cols], 0.0)
        tile += jnp.where(row8 == 4 + qq, branch[:, cols], 0.0)
    stat[...] = tile
    got_stat = {k: ep_start(3, k, stat, stat_recv.at[k]) for k in ep_far}

    got_dense = {}
    for dy in dy_far:
        rows = at(lax.rem(ey + dy, EY), RC)
        dense_send[rows, :] = dot(xg[rows, :], dgu[...]).astype(BF16)
        for dx in dx_far:
            k = dy * EX + dx
            if k:
                got_dense[k] = ep_start(
                    4, k, dense_send.at[at(ep_peer(k), R), :], dense_recv.at[k]
                )
    got_disp = {}
    for dy in dy_far:
        rows = at(lax.rem(ey + dy, EY), S * EX)
        disp_send[rows, :] = dot(gmat[rows, :], xg[...]).astype(BF16)
        for dx in dx_far:
            k = dy * EX + dx
            if k:
                got_disp[k] = ep_start(
                    5, k, disp_send.at[at(ep_peer(k), S), :], xrecv.at[:, at(e, Dc)]
                )
    xrecv[:, at(e, Dc)] = disp_send[at(e, S), :]

    for k in reversed(ep_far):
        got_stat[k].wait_recv()
        tile += stat_recv[k]
    scale_l = lax.rsqrt(tile[0:Q, :] * (1.0 / D) + EPS)
    share_l = 1.0 / (1.0 + jnp.exp(-(scale_l * tile[4 : 4 + Q, :])))
    my_scale = jnp.zeros((R, 1), F32)
    my_bshare = jnp.zeros((R, 1), F32)
    for qq in range(Q):
        here = iota((R, LANES), 1) + qq * LANES == iota((R, LANES), 0) + e * R
        my_scale += jnp.sum(jnp.where(here, scale_l[qq : qq + 1, :], 0.0), axis=1, keepdims=True)
        my_bshare += jnp.sum(jnp.where(here, share_l[qq : qq + 1, :], 0.0), axis=1, keepdims=True)
    scale_row = (
        jnp.concatenate([scale_l[qq : qq + 1, :] for qq in range(Q)], axis=1) if Q > 1 else scale_l
    )
    row_scale = jnp.sum(jnp.where(row_no == my_code, scale_row, 0.0), axis=1, keepdims=True)

    both = dense_send[at(e, R), :].astype(F32)
    for k in reversed(ep_far):
        got_dense[k].wait_recv()
        both += dense_recv[k].astype(F32)
    both *= my_scale
    g, u = both[:, :F], both[:, F:]
    hid_all[at(e, R), :] = (g / (1.0 + jnp.exp(-g)) * u).astype(BF16)
    got_hid = {
        k: ep_start(6, k, hid_all.at[at(e, R), :], hid_all.at[at(e, R), :]) for k in ep_far
    }

    load_eg.wait()
    load_eu.wait()
    for k in reversed(ep_far):
        got_disp[k].wait_recv()
    gp = dot(xrecv[...], eg[0]) * row_scale
    up = dot(xrecv[...], eu[0]) * row_scale
    ehid = (gp / (1.0 + jnp.exp(-gp)) * up).astype(BF16)
    ehid8 = dot(spread, ehid).astype(BF16)
    load_ed.wait()
    step = min(512, D)
    for c in range(D // step):
        cols = slice(c * step, (c + 1) * step)
        y = dot(ehid8, ed[0, :, cols]) * row_share
        fin_send[:, :, cols] = y.reshape(n_ep, PAD, step).astype(BF16)
    got_fin = {k: ep_start(7, k, fin_send.at[ep_peer(k)], fin_recv.at[e]) for k in ep_far}
    fin_recv[e] = fin_send[e]

    load_dd.wait()
    for k in reversed(ep_far):
        got_hid[k].wait_recv()
    got_dn = {}
    for dy in dy_far:
        rows = at(lax.rem(ey + dy, EY), RC)
        dn_send[rows, :] = dot(hid_all[rows, :], dd[...]).astype(BF16)
        for dx in dx_far:
            k = dy * EX + dx
            if k:
                got_dn[k] = ep_start(
                    8, k, dn_send.at[at(ep_peer(k), R), :], dn_recv.at[:, at(e, Dc)]
                )
    dn_recv[:, at(e, Dc)] = dn_send[at(e, R), :]

    for k in reversed(ep_far):
        got_fin[k].wait_recv()
    for k in reversed(ep_far):
        got_dn[k].wait_recv()
    got_tp = {}
    for k in tp_far + [0]:
        cols = at(tp_peer(k), Dt)
        back = fin_recv[:, :, cols].astype(F32).reshape(S8, Dt).astype(BF16)
        piece = dot(pick, back) + my_bshare * dn_recv[:, cols].astype(F32)
        tp_send[:, cols] = piece.astype(BF16)
        if k:
            got_tp[k] = tp_start(2, k, tp_send.at[:, cols], tp_recv.at[k])

    @pl.when(e != t)
    def _():
        cross(1, res_all.at[at(t, R), :], res_t).wait()

    last = res_t[...].astype(F32) + tp_send[:, at(t, Dt)].astype(F32)
    for k in reversed(tp_far):
        got_tp[k].wait_recv()
        last += tp_recv[k].astype(F32)
    out_all[:, at(t, Dt)] = last.astype(BF16)
    got_out = [
        tp_start(3, k, out_all.at[:, at(t, Dt)], out_all.at[:, at(t, Dt)]) for k in tp_far
    ]
    for k in ep_far:
        mix_copy(k).wait_send()

    @pl.when(e != t)
    def _():
        mix_copy(0).wait_send()

    for copy in got_out:
        copy.wait_recv()
    out_ref[...] = out_all[...]
    for copy in pending:
        copy.wait_send()


def on_device(
    n_ep,
    n_tp,
    tokens,
    state_matrix,
    state_norm,
    state_max,
    mixer_gain,
    w_query,
    w_key,
    w_value,
    w_outgate,
    w_ingate,
    w_forget,
    forget_bias,
    w_proj,
    ffn_gain,
    w_branch,
    routes,
    route_weight,
    expert_gate,
    expert_up,
    expert_down,
    dense_gate,
    dense_up,
    dense_down,
):
    R, D = tokens.shape
    hd = state_norm.shape[2]
    N, Dc, Dt, W = R * n_ep, D // n_ep, D // n_tp, hd
    F = dense_gate.shape[1]
    FE = expert_gate.shape[2]
    S, S8 = CAP * n_ep, PAD * n_ep
    vmem = pl.BlockSpec(memory_space=pltpu.VMEM)
    hbm = pl.BlockSpec(memory_space=pl.ANY)
    V = pltpu.VMEM
    scratch = [
        V(state_matrix.shape, F32),
        V((Dc, 4 * W), BF16),
        V((n_tp * W, Dc), BF16),
        V(expert_gate.shape, BF16),
        V(expert_up.shape, BF16),
        V(expert_down.shape, BF16),
        V((Dc, 2 * F), BF16),
        V(dense_down.shape, BF16),
        V((R, D), BF16),
        V((N, Dc), BF16),
        V((n_ep, LANES), F32),
        V((n_ep, n_ep, LANES), F32),
        V((N, 4 * W), BF16),
        V((n_ep, R, 4 * W), BF16),
        V((R, W), F32),
        V((R, W), BF16),
        V((R, n_tp * W), BF16),
        V((R, Dc), BF16),
        V((N, Dc), BF16),
        V((R, Dt), BF16),
        V((N, Dc), BF16),
        V((n_ep * S, N), BF16),
        V((8, LANES), F32),
        V((n_ep, 8, LANES), F32),
        V((N, 2 * F), BF16),
        V((n_ep, R, 2 * F), BF16),
        V((n_ep * S, Dc), BF16),
        V((S, D), BF16),
        V((N, F), BF16),
        V((n_ep, PAD, D), BF16),
        V((n_ep, PAD, D), BF16),
        V((N, Dc), BF16),
        V((R, D), BF16),
        V((R, D), BF16),
        V((n_tp, R, Dt), BF16),
        V((R, D), BF16),
        pltpu.SemaphoreType.DMA((12,)),
        pltpu.SemaphoreType.DMA((9, n_ep)),
        pltpu.SemaphoreType.DMA((9, n_ep)),
        pltpu.SemaphoreType.DMA((4, n_tp)),
        pltpu.SemaphoreType.DMA((4, n_tp)),
        pltpu.SemaphoreType.DMA((n_ep,)),
        pltpu.SemaphoreType.DMA((n_tp,)),
        pltpu.SemaphoreType.DMA((2,)),
        pltpu.SemaphoreType.DMA((2,)),
    ]
    Sh = jax.ShapeDtypeStruct
    layer_out, new_norm, new_max, key_w, value, keep = pl.pallas_call(
        functools.partial(layer_kernel, n_ep, n_tp),
        out_shape=(
            Sh((R, D), BF16),
            Sh((R, hd), F32),
            Sh((1, R), F32),
            Sh((R, hd), F32),
            Sh((R, hd), F32),
            Sh((R, hd), F32),
        ),
        in_specs=[vmem] * 11 + [hbm] * 12,
        out_specs=(vmem,) * 6,
        scratch_shapes=scratch,
        compiler_params=pltpu.CompilerParams(
            collective_id=0, has_side_effects=True, vmem_limit_bytes=66_000_000
        ),
    )(
        tokens,
        mixer_gain[None, :],
        w_ingate.T,
        w_forget.T,
        forget_bias[None, :],
        state_norm.reshape(R, hd),
        state_max.T,
        ffn_gain[None, :],
        w_branch.reshape(-1, LANES),
        routes.T,
        route_weight.T,
        state_matrix,
        w_query,
        w_key,
        w_value,
        w_outgate,
        w_proj,
        expert_gate,
        expert_up,
        expert_down,
        dense_gate,
        dense_up,
        dense_down,
    )
    new_matrix = (
        keep[:, None, None, :] * state_matrix + key_w[:, None, :, None] * value[:, None, None, :]
    )
    return (layer_out, new_matrix, new_norm.reshape(R, 1, hd), new_max.T)


def solution(mesh):
    in_specs = (
        P("ep", None),
        P("ep", "tp", None, None),
        P("ep", "tp", None),
        P("ep", "tp"),
        P(),
        P("ep", "tp"),
        P("ep", "tp"),
        P("ep", "tp"),
        P("ep", "tp"),
        P(),
        P(),
        P(),
        P("tp", "ep"),
        P(),
        P(),
        P("ep", None),
        P("ep", None),
        P("ep", None, "tp"),
        P("ep", None, "tp"),
        P("ep", "tp", None),
        P("ep", "tp"),
        P("ep", "tp"),
        P("tp", "ep"),
    )
    out_specs = (P("ep", None), P("ep", "tp", None, None), P("ep", "tp", None), P("ep", "tp"))
    return jax.shard_map(
        functools.partial(on_device, mesh.shape["ep"], mesh.shape["tp"]),
        mesh=mesh,
        in_specs=in_specs,
        out_specs=out_specs,
        check_vma=False,
    )
```

```python
import functools

import jax
import jax.numpy as jnp
from jax import lax
from jax.experimental import pallas as pl
from jax.experimental.pallas import tpu as pltpu
from jax.sharding import PartitionSpec as P

EPS = 1e-06
LANES = 128
CAP = 6
PAD = 8
F32 = jnp.float32
BF16 = jnp.bfloat16
MESH = pl.DeviceIdType.MESH


def dot(a, b):
    return jnp.dot(a, b, preferred_element_type=F32)


def dot_t(a, b):
    return lax.dot_general(a, b, (((1,), (1,)), ((), ())), preferred_element_type=F32)


def iota(shape, dim):
    return lax.broadcasted_iota(jnp.int32, shape, dim)


def layer_kernel(
    n_ep,
    n_tp,
    tokens_ref,
    gain_ref,
    win_ref,
    wfo_ref,
    bias_ref,
    norm_ref,
    smax_ref,
    fgain_ref,
    branch_ref,
    routes_ref,
    weight_ref,
    state_hbm,
    wq_hbm,
    wk_hbm,
    wv_hbm,
    wo_hbm,
    wproj_hbm,
    eg_hbm,
    eu_hbm,
    ed_hbm,
    dg_hbm,
    du_hbm,
    dd_hbm,
    out_ref,
    norm_out_ref,
    max_out_ref,
    keyw_ref,
    value_ref,
    keep_ref,
    state,
    wcat,
    wproj,
    eg,
    eu,
    edc,
    dgu,
    dd,
    nrm,
    x_all,
    info,
    info_recv,
    part_send,
    part_recv,
    numer,
    mix_send,
    mix_all,
    raw_blk,
    res_all,
    res_t,
    xg,
    gmat,
    stat,
    stat_recv,
    dense_send,
    dense_recv,
    disp_send,
    xrecv,
    hid_all,
    yo_send,
    yo_recv,
    fin_send,
    fin_recv,
    dno_send,
    dno_recv,
    dn_send,
    dn_recv,
    tp_send,
    tp_recv,
    out_all,
    load_sems,
    send_ep,
    recv_ep,
    send_tp,
    recv_tp,
    send_mx,
    recv_mx,
    send_tr,
    recv_tr,
    send_fw,
    recv_fw,
    send_sb,
    recv_sb,
):
    e = lax.axis_index("ep")
    t = lax.axis_index("tp")
    R, D = tokens_ref.shape
    N = R * n_ep
    Dc = D // n_ep
    HD = Dc // 2
    DH = D // 2
    W = mix_send.shape[1]
    F = dd.shape[0]
    EX = {16: 4, 4: 2}[n_ep]
    EY = n_ep // EX
    TZ = n_tp // 2
    S = CAP * n_ep
    S8 = PAD * n_ep
    Q = N // LANES
    PER = LANES // R
    RC = R * EX
    ey, ex = e // EX, lax.rem(e, EX)
    tz, tc = t // 2, lax.rem(t, 2)

    def at(index, size):
        return pl.ds(pl.multiple_of(index * size, size), size)

    def ring(d, n):
        return min(d, n - d)

    ep_far = sorted(range(1, n_ep), key=lambda k: -(ring(k // EX, EY) + ring(k % EX, EX)))
    dz_far = sorted(range(1, TZ), key=lambda d: -ring(d, TZ))
    dy_far = sorted(range(EY), key=lambda d: -ring(d, EY))
    dx_far = sorted(range(EX), key=lambda d: -ring(d, EX))

    def ep_peer(k):
        return lax.rem(ey + k // EX, EY) * EX + lax.rem(ex + k % EX, EX)

    def ep_from(k):
        return lax.rem(ey + EY - k // EX, EY) * EX + lax.rem(ex + EX - k % EX, EX)

    def tp_peer(k):
        return lax.rem(tz + k // 2, TZ) * 2 + lax.rem(tc + k % 2, 2)

    sibling = tz * 2 + 1 - tc

    loads = []

    def load(src, dst):
        copy = pltpu.make_async_copy(src, dst, load_sems.at[len(loads)])
        copy.start()
        loads.append(copy)
        return copy

    pending = []

    def ep_start(phase, k, src, dst):
        copy = pltpu.make_async_remote_copy(
            src_ref=src,
            dst_ref=dst,
            send_sem=send_ep.at[phase, k],
            recv_sem=recv_ep.at[phase, k],
            device_id={"ep": ep_peer(k)},
            device_id_type=MESH,
        )
        copy.start()
        pending.append(copy)
        return copy

    def tp_start(phase, k, src, dst):
        copy = pltpu.make_async_remote_copy(
            src_ref=src,
            dst_ref=dst,
            send_sem=send_tp.at[phase, k],
            recv_sem=recv_tp.at[phase, k],
            device_id={"tp": tp_peer(k)},
            device_id_type=MESH,
        )
        copy.start()
        pending.append(copy)
        return copy

    def side_start(send_sem, recv_sem, src, dst):
        copy = pltpu.make_async_remote_copy(
            src_ref=src,
            dst_ref=dst,
            send_sem=send_sem,
            recv_sem=recv_sem,
            device_id={"tp": sibling},
            device_id_type=MESH,
        )
        copy.start()
        pending.append(copy)
        return copy

    def spread_tp(phase, region):
        copies = {dz: tp_start(phase, 2 * dz, region(t), region(t)) for dz in dz_far}
        copies[0] = tp_start(phase, 1, region(t), region(t))
        return copies

    def gather_tp(phase, region, copies):
        passed = []
        for dz in reversed(dz_far):
            copies[dz].wait_recv()
            source = lax.rem(tz + TZ - dz, TZ) * 2 + tc
            odd = 2 * dz + 1
            passed.append(
                side_start(
                    send_tp.at[phase, odd], recv_tp.at[phase, odd], region(source), region(source)
                )
            )
        copies[0].wait_recv()
        for copy in passed:
            copy.wait_recv()

    def cross(phase, src, dst):
        return pltpu.make_async_remote_copy(
            src_ref=src,
            dst_ref=dst,
            send_sem=send_tr.at[phase],
            recv_sem=recv_tr.at[phase],
            device_id={"ep": t, "tp": e},
            device_id_type=MESH,
        )

    barrier = pltpu.get_barrier_semaphore()
    for k in ep_far:
        pl.semaphore_signal(barrier, inc=1, device_id={"ep": ep_peer(k)}, device_id_type=MESH)
    for k in range(1, n_tp):
        pl.semaphore_signal(barrier, inc=1, device_id={"tp": tp_peer(k)}, device_id_type=MESH)

    load_w = [
        load(src, wcat.at[:, pl.ds(i * W, W)])
        for i, src in enumerate((wq_hbm, wk_hbm, wv_hbm, wo_hbm))
    ]
    load_proj = load(wproj_hbm, wproj.at[at(t, W), :])
    load_state = load(state_hbm, state)
    load_dg, load_du = load(dg_hbm, dgu.at[:, pl.ds(0, F)]), load(du_hbm, dgu.at[:, pl.ds(F, F)])
    load_eg, load_eu = load(eg_hbm, eg), load(eu_hbm, eu)
    load_ed = [
        load(ed_hbm.at[0, :, at(2 * b + side, HD)], edc.at[i, :, pl.ds(b * HD, HD)])
        for i, side in enumerate((1 - tc, tc))
        for b in range(n_ep)
    ]
    load_dd = load(dd_hbm, dd)

    wide = tokens_ref[...].astype(F32)
    scale = lax.rsqrt(jnp.mean(wide * wide, axis=-1, keepdims=True) + EPS)
    nrm[...] = (wide * scale * gain_ref[...]).astype(BF16)

    r0, r1 = routes_ref[0:1, :], routes_ref[1:2, :]
    w0, w1 = weight_ref[0:1, :], weight_ref[1:2, :]
    total = w0 + w1
    which = iota((n_ep, R), 0)
    hit0, hit1 = which == r0, which == r1
    named = jnp.where(jnp.logical_or(hit0, hit1), 1.0, 0.0)
    earlier = jnp.where(iota((R, R), 0) < iota((R, R), 1), 1.0, 0.0).astype(BF16)
    slot = dot(named.astype(BF16), earlier)
    code = jnp.where(named > 0.0, slot + 1.0, 0.0)
    group_at = (e * CAP).astype(F32)
    rowcode = jnp.where(named > 0.0, slot + (1.0 + group_at), 0.0)
    shares = jnp.where(hit0, w0 / total, 0.0) + jnp.where(hit1, w1 / total, 0.0)
    info[:, 0:R] = rowcode
    info[:, R : 2 * R] = shares
    info[:, 2 * R : LANES] = jnp.zeros((n_ep, LANES - 2 * R), F32)

    pl.semaphore_wait(barrier, n_ep - 1 + n_tp - 1)
    got_x = {k: ep_start(0, k, nrm.at[:, at(ep_peer(k), Dc)], x_all.at[at(e, R), :]) for k in ep_far}
    x_all[at(e, R), :] = nrm[:, at(e, Dc)]
    load_proj.wait()

    def proj_rows(tt):
        return wproj.at[at(tt, W), :]

    got_wp = spread_tp(0, proj_rows)

    gate_in = dot_t(nrm[...], win_ref[...])
    gate_fo = dot_t(nrm[...], wfo_ref[...]) + bias_ref[...]
    mine = iota(gate_in.shape, 1) == t
    g_in = jnp.sum(jnp.where(mine, gate_in, 0.0), axis=1, keepdims=True)
    g_fo = jnp.sum(jnp.where(mine, gate_fo, 0.0), axis=1, keepdims=True)
    eye = iota((R, R), 0) == iota((R, R), 1)
    smax = jnp.sum(jnp.where(eye, smax_ref[...], 0.0), axis=1, keepdims=True)
    log_keep = jnp.minimum(g_fo, 0.0) - jnp.log(1.0 + jnp.exp(-jnp.abs(g_fo)))
    carried = log_keep + smax
    new_max = jnp.maximum(carried, g_in)
    keep = jnp.exp(carried - new_max)
    write = jnp.exp(g_in - new_max)
    max_out_ref[...] = jnp.sum(jnp.where(eye, new_max, 0.0), axis=0, keepdims=True)
    keep_ref[...] = jnp.broadcast_to(keep, keep_ref.shape)

    for copy in load_w:
        copy.wait()
    got_part = {}
    for dy in [(EY - d) % EY for d in range(EY)]:
        back = (EY - dy) % EY
        for dx in range(EX):
            k = dy * EX + dx
            if k:
                got_x[k].wait_recv()
        rows = at(lax.rem(ey + back, EY), RC)
        part_send[rows, :] = dot(x_all[rows, :], wcat[...]).astype(BF16)
        for dx in dx_far:
            k = back * EX + dx
            if k:
                got_part[k] = ep_start(1, k, part_send.at[at(ep_peer(k), R), :], part_recv.at[k])
    got_info = {k: ep_start(2, k, info, info_recv.at[k]) for k in ep_far}

    @pl.when(e != t)
    def _():
        cross(0, tokens_ref.at[:, at(t, Dc)], raw_blk).start()

    @pl.when(e == t)
    def _():
        raw_blk[...] = tokens_ref[:, at(t, Dc)]

    proj = part_send[at(e, R), :].astype(F32)
    for k in reversed(ep_far):
        got_part[k].wait_recv()
        proj += part_recv[k].astype(F32)

    load_state.wait()
    q = proj[:, 0:W]
    key = proj[:, W : 2 * W] * W ** (-0.5)
    val = proj[:, 2 * W : 3 * W]
    og = proj[:, 3 * W : 4 * W]
    key_w = write * key
    new_norm = keep * norm_ref[...] + key_w
    q_t = q.T
    for b in range(R):
        numer[b : b + 1, :] = jnp.sum(q_t[:, b : b + 1] * state[b, 0], axis=0, keepdims=True)
    top = keep * numer[...] + jnp.sum(q * key_w, axis=1, keepdims=True) * val
    denom = jnp.sum(q * new_norm, axis=1, keepdims=True)
    cell = top / jnp.maximum(jnp.abs(denom), 1.0)
    mix_send[...] = (cell / (1.0 + jnp.exp(-og))).astype(BF16)

    def mix_copy(k):
        return pltpu.make_async_remote_copy(
            src_ref=mix_send,
            dst_ref=mix_all.at[:, at(t, W)],
            send_sem=send_mx.at[k],
            recv_sem=recv_mx.at[t],
            device_id={"ep": ep_peer(k), "tp": e},
            device_id_type=MESH,
        )

    for k in ep_far:
        mix_copy(k).start()

    @pl.when(e != t)
    def _():
        mix_copy(0).start()

    @pl.when(e == t)
    def _():
        mix_all[:, at(t, W)] = mix_send[...]

    gather_tp(0, proj_rows, got_wp)
    norm_out_ref[...] = new_norm
    keyw_ref[...] = key_w
    value_ref[...] = val

    for k in ep_far:
        got_info[k].wait_recv()
    quarter = iota((n_ep, LANES), 1) // R
    codes, sharesl = [], []

    info_recv[0] = info[...]
    for qq in range(Q):
        ctile = jnp.zeros((n_ep, LANES), F32)
        stile = jnp.zeros((n_ep, LANES), F32)
        for j in range(PER):
            g = qq * PER + j
            gy, gx = g // EX, g % EX
            slot_k = lax.rem(ey + (EY - gy), EY) * EX + lax.rem(ex + (EX - gx), EX)
            tile = info_recv[slot_k]
            there = quarter == j
            ctile += jnp.where(there, tile if j == 0 else pltpu.roll(tile, j * R, 1), 0.0)
            back = (j - 1) % PER * R
            stile += jnp.where(there, tile if back == 0 else pltpu.roll(tile, back, 1), 0.0)
        codes.append(ctile)
        sharesl.append(stile)
    code_all = jnp.concatenate(codes, axis=1) if Q > 1 else codes[0]
    share_all = jnp.concatenate(sharesl, axis=1) if Q > 1 else sharesl[0]
    row_no = (iota((S, N), 0) + 1).astype(F32)
    for p in range(n_ep):
        gmat[p * S : (p + 1) * S, :] = jnp.where(row_no == code_all[p : p + 1, :], 1.0, 0.0).astype(
            BF16
        )
    is_mine = iota((n_ep, N), 0) == e
    my_code = jnp.sum(jnp.where(is_mine, code_all, 0.0), axis=0, keepdims=True)
    my_share = jnp.sum(jnp.where(is_mine, share_all, 0.0), axis=0, keepdims=True)
    my_code8 = jnp.where(
        my_code > 0.0, my_code + ((PAD - CAP) * (iota((1, N), 1) // R)).astype(F32), 0.0
    )
    row_share = jnp.sum(
        jnp.where((iota((S8, N), 0) + 1).astype(F32) == my_code8, my_share, 0.0),
        axis=1,
        keepdims=True,
    )
    spread = jnp.where(
        jnp.logical_and(
            iota((S8, S), 0) // PAD * CAP + iota((S8, S), 0) % PAD == iota((S8, S), 1),
            iota((S8, S), 0) % PAD < CAP,
        ),
        1.0,
        0.0,
    ).astype(BF16)
    repeat = jnp.where(iota((S8, n_ep), 0) // PAD == iota((S8, n_ep), 1), 1.0, 0.0).astype(BF16)
    code_rep = dot(repeat, code.astype(BF16))
    pick_t = jnp.where((iota((S8, R), 0) % PAD + 1).astype(F32) == code_rep, 1.0, 0.0)
    pick = pick_t.T.astype(BF16)

    @pl.when(e != t)
    def _():
        cross(0, tokens_ref.at[:, at(t, Dc)], raw_blk).wait()

    for tt in range(n_tp):

        @pl.when(jnp.logical_or(e != t, t != tt))
        def _():
            pltpu.make_async_remote_copy(
                src_ref=mix_send,
                dst_ref=mix_all.at[:, pl.ds(tt * W, W)],
                send_sem=send_mx.at[0],
                recv_sem=recv_mx.at[tt],
                device_id={"ep": t, "tp": e},
                device_id_type=MESH,
            ).wait_recv()

    mine_res = raw_blk[...].astype(F32) + dot(mix_all[...], wproj[...])
    res_all[at(t, R), :] = mine_res.astype(BF16)

    def res_rows(tt):
        return res_all.at[at(tt, R), :]

    got_res = spread_tp(1, res_rows)

    def half_copy(c):
        return pltpu.make_async_remote_copy(
            src_ref=res_all.at[at(t, R), pl.ds(c * HD, HD)],
            dst_ref=res_t.at[:, at(lax.rem(e, 2), HD)],
            send_sem=send_tr.at[1 + c],
            recv_sem=recv_tr.at[1 + lax.rem(e, 2)],
            device_id={"ep": t, "tp": e // 2 * 2 + c},
            device_id_type=MESH,
        )

    for c in range(2):
        away = jnp.logical_or(e != t, tc != c)

        @pl.when(away)
        def _():
            half_copy(c).start()

        @pl.when(jnp.logical_not(away))
        def _():
            res_t[:, pl.ds(c * HD, HD)] = res_all[at(t, R), pl.ds(c * HD, HD)]

    load_dg.wait()
    load_du.wait()
    my_fgain = fgain_ref[:, at(e, Dc)]
    wide_branch = branch_ref[...].astype(F32)
    pieces = Dc // LANES
    branch_rows = [
        jnp.sum(
            jnp.where(iota(wide_branch.shape, 0) == e * pieces + i, wide_branch, 0.0),
            axis=0,
            keepdims=True,
        )
        for i in range(pieces)
    ]
    my_branch = jnp.concatenate(branch_rows, axis=1) if pieces > 1 else branch_rows[0]
    my_branch = jnp.broadcast_to(my_branch, (8, Dc)).astype(BF16)
    ones = jnp.ones((8, Dc), BF16)

    gather_tp(1, res_rows, got_res)
    block = res_all[...].astype(F32)
    xg[...] = (block * my_fgain).astype(BF16)
    square = block * block
    high = square.astype(BF16)
    low = (square - high.astype(F32)).astype(BF16)
    sums = dot_t(ones, high) + dot_t(ones, low)
    branch = dot_t(my_branch, xg[...])
    row8 = iota((8, LANES), 0)
    tile = jnp.zeros((8, LANES), F32)
    for qq in range(Q):
        cols = slice(qq * LANES, (qq + 1) * LANES)
        tile += jnp.where(row8 == qq, sums[:, cols], 0.0)
        tile += jnp.where(row8 == 4 + qq, branch[:, cols], 0.0)
    stat[...] = tile
    got_stat = {k: ep_start(3, k, stat, stat_recv.at[k]) for k in ep_far}

    got_dense = {}
    for dy in dy_far:
        rows = at(lax.rem(ey + dy, EY), RC)
        dense_send[rows, :] = dot(xg[rows, :], dgu[...]).astype(BF16)
        for dx in dx_far:
            k = dy * EX + dx
            if k:
                got_dense[k] = ep_start(
                    4, k, dense_send.at[at(ep_peer(k), R), :], dense_recv.at[k]
                )
    got_disp = {}
    for dy in dy_far:
        rows = at(lax.rem(ey + dy, EY), S * EX)
        disp_send[rows, :] = dot(gmat[rows, :], xg[:, at(tc, HD)]).astype(BF16)
        for dx in dx_far:
            k = dy * EX + dx
            if k:
                got_disp[k] = ep_start(
                    5, k, disp_send.at[at(ep_peer(k), S), :], xrecv.at[:, at(2 * e + tc, HD)]
                )
    xrecv[:, at(2 * e + tc, HD)] = disp_send[at(e, S), :]

    def forward(k):
        region = xrecv.at[:, at(2 * ep_from(k) + tc, HD)]
        return side_start(send_fw.at[k], recv_fw.at[k], region, region)

    passed = [forward(0)]

    for k in reversed(ep_far):
        got_stat[k].wait_recv()
        tile += stat_recv[k]
    scale_l = lax.rsqrt(tile[0:Q, :] * (1.0 / D) + EPS)
    share_l = 1.0 / (1.0 + jnp.exp(-(scale_l * tile[4 : 4 + Q, :])))
    my_scale = jnp.zeros((R, 1), F32)
    my_bshare = jnp.zeros((R, 1), F32)
    for qq in range(Q):
        here = iota((R, LANES), 1) + qq * LANES == iota((R, LANES), 0) + e * R
        my_scale += jnp.sum(jnp.where(here, scale_l[qq : qq + 1, :], 0.0), axis=1, keepdims=True)
        my_bshare += jnp.sum(jnp.where(here, share_l[qq : qq + 1, :], 0.0), axis=1, keepdims=True)
    scale_row = (
        jnp.concatenate([scale_l[qq : qq + 1, :] for qq in range(Q)], axis=1) if Q > 1 else scale_l
    )
    row_scale = jnp.sum(jnp.where(row_no == my_code, scale_row, 0.0), axis=1, keepdims=True)

    both = dense_send[at(e, R), :].astype(F32)
    for k in reversed(ep_far):
        got_dense[k].wait_recv()
        both += dense_recv[k].astype(F32)
    both *= my_scale
    g, u = both[:, :F], both[:, F:]
    hid_all[at(e, R), :] = (g / (1.0 + jnp.exp(-g)) * u).astype(BF16)
    got_hid = {
        k: ep_start(6, k, hid_all.at[at(e, R), :], hid_all.at[at(e, R), :]) for k in ep_far
    }

    load_eg.wait()
    load_eu.wait()
    for k in reversed(ep_far):
        got_disp[k].wait_recv()
        passed.append(forward(k))
    for copy in passed:
        copy.wait_recv()
    gp = dot(xrecv[...], eg[0]) * row_scale
    up = dot(xrecv[...], eu[0]) * row_scale
    ehid = (gp / (1.0 + jnp.exp(-gp)) * up).astype(BF16)
    ehid8 = dot(spread, ehid).astype(BF16)
    for copy in load_ed:
        copy.wait()
    step = min(512, DH)
    strips = [slice(c * step, (c + 1) * step) for c in range(DH // step)]
    got_yo = []
    for i, cols in enumerate(strips):
        yo_send[:, cols] = (dot(ehid8, edc[0, :, cols]) * row_share).astype(BF16)
        got_yo.append(
            side_start(send_sb.at[i], recv_sb.at[i], yo_send.at[:, cols], yo_recv.at[:, cols])
        )
    for copy, cols in zip(got_yo, strips):
        y = dot(ehid8, edc[1, :, cols]) * row_share
        copy.wait_recv()
        y += yo_recv[:, cols].astype(F32)
        fin_send[:, :, cols] = y.reshape(n_ep, PAD, step).astype(BF16)
    got_fin = {k: ep_start(7, k, fin_send.at[ep_peer(k)], fin_recv.at[e]) for k in ep_far}
    fin_recv[e] = fin_send[e]

    load_dd.wait()
    for k in reversed(ep_far):
        got_hid[k].wait_recv()
    got_no = {}
    for dy in dy_far:
        rows = at(lax.rem(ey + dy, EY), RC)
        dno_send[rows, :] = dot(hid_all[rows, :], dd[:, at(1 - tc, HD)]).astype(BF16)
        got_no[dy] = side_start(
            send_sb.at[4 + dy], recv_sb.at[4 + dy], dno_send.at[rows, :], dno_recv.at[rows, :]
        )
    got_dn = {}
    for dy in dy_far:
        rows = at(lax.rem(ey + dy, EY), RC)
        down = dot(hid_all[rows, :], dd[:, at(tc, HD)])
        got_no[dy].wait_recv()
        dn_send[rows, :] = (down + dno_recv[rows, :].astype(F32)).astype(BF16)
        for dx in dx_far:
            k = dy * EX + dx
            if k:
                got_dn[k] = ep_start(
                    8, k, dn_send.at[at(ep_peer(k), R), :], dn_recv.at[:, at(e, HD)]
                )
    dn_recv[:, at(e, HD)] = dn_send[at(e, R), :]

    for k in reversed(ep_far):
        got_fin[k].wait_recv()
    for k in reversed(ep_far):
        got_dn[k].wait_recv()
    got_tp = {}
    for dz in dz_far + [0]:
        cols = at(lax.rem(tz + dz, TZ), Dc)
        back = fin_recv[:, :, cols].astype(F32).reshape(S8, Dc).astype(BF16)
        piece = dot(pick, back) + my_bshare * dn_recv[:, cols].astype(F32)
        tp_send[:, cols] = piece.astype(BF16)
        if dz:
            got_tp[dz] = tp_start(2, 2 * dz, tp_send.at[:, cols], tp_recv.at[dz])

    for i in range(2):

        @pl.when(jnp.logical_or(e != t, lax.rem(e, 2) != i))
        def _():
            pltpu.make_async_remote_copy(
                src_ref=res_all.at[at(t, R), pl.ds(0, HD)],
                dst_ref=res_t.at[:, pl.ds(i * HD, HD)],
                send_sem=send_tr.at[1 + i],
                recv_sem=recv_tr.at[1 + i],
                device_id={"ep": t, "tp": e},
                device_id_type=MESH,
            ).wait_recv()

    last = res_t[...].astype(F32) + tp_send[:, at(tz, Dc)].astype(F32)
    for dz in reversed(dz_far):
        got_tp[dz].wait_recv()
        last += tp_recv[dz].astype(F32)
    out_all[:, at(tc * TZ + tz, Dc)] = last.astype(BF16)

    def out_cols(tt):
        return out_all.at[:, at(lax.rem(tt, 2) * TZ + tt // 2, Dc)]

    got_out = spread_tp(3, out_cols)
    for k in ep_far:
        mix_copy(k).wait_send()

    @pl.when(e != t)
    def _():
        mix_copy(0).wait_send()

    for c in range(2):

        @pl.when(jnp.logical_or(e != t, tc != c))
        def _():
            half_copy(c).wait_send()

    gather_tp(3, out_cols, got_out)
    for b in range(n_ep):
        for c in range(2):
            out_ref[:, pl.ds((2 * b + c) * HD, HD)] = out_all[:, pl.ds(c * DH + b * HD, HD)]
    for copy in pending:
        copy.wait_send()


def on_device(
    n_ep,
    n_tp,
    tokens,
    state_matrix,
    state_norm,
    state_max,
    mixer_gain,
    w_query,
    w_key,
    w_value,
    w_outgate,
    w_ingate,
    w_forget,
    forget_bias,
    w_proj,
    ffn_gain,
    w_branch,
    routes,
    route_weight,
    expert_gate,
    expert_up,
    expert_down,
    dense_gate,
    dense_up,
    dense_down,
):
    R, D = tokens.shape
    hd = state_norm.shape[2]
    N, Dc, DH, W = R * n_ep, D // n_ep, D // 2, hd
    F = dense_gate.shape[1]
    FE = expert_gate.shape[2]
    S, S8 = CAP * n_ep, PAD * n_ep
    vmem = pl.BlockSpec(memory_space=pltpu.VMEM)
    hbm = pl.BlockSpec(memory_space=pl.ANY)
    V = pltpu.VMEM
    scratch = [
        V(state_matrix.shape, F32),
        V((Dc, 4 * W), BF16),
        V((n_tp * W, Dc), BF16),
        V(expert_gate.shape, BF16),
        V(expert_up.shape, BF16),
        V((2, FE, DH), BF16),
        V((Dc, 2 * F), BF16),
        V(dense_down.shape, BF16),
        V((R, D), BF16),
        V((N, Dc), BF16),
        V((n_ep, LANES), F32),
        V((n_ep, n_ep, LANES), F32),
        V((N, 4 * W), BF16),
        V((n_ep, R, 4 * W), BF16),
        V((R, W), F32),
        V((R, W), BF16),
        V((R, n_tp * W), BF16),
        V((R, Dc), BF16),
        V((N, Dc), BF16),
        V((R, Dc), BF16),
        V((N, Dc), BF16),
        V((n_ep * S, N), BF16),
        V((8, LANES), F32),
        V((n_ep, 8, LANES), F32),
        V((N, 2 * F), BF16),
        V((n_ep, R, 2 * F), BF16),
        V((n_ep * S, Dc // 2), BF16),
        V((S, D), BF16),
        V((N, F), BF16),
        V((S8, DH), BF16),
        V((S8, DH), BF16),
        V((n_ep, PAD, DH), BF16),
        V((n_ep, PAD, DH), BF16),
        V((N, Dc // 2), BF16),
        V((N, Dc // 2), BF16),
        V((N, Dc // 2), BF16),
        V((R, DH), BF16),
        V((R, DH), BF16),
        V((n_tp // 2, R, Dc), BF16),
        V((R, D), BF16),
        pltpu.SemaphoreType.DMA((11 + 2 * n_ep,)),
        pltpu.SemaphoreType.DMA((9, n_ep)),
        pltpu.SemaphoreType.DMA((9, n_ep)),
        pltpu.SemaphoreType.DMA((4, n_tp)),
        pltpu.SemaphoreType.DMA((4, n_tp)),
        pltpu.SemaphoreType.DMA((n_ep,)),
        pltpu.SemaphoreType.DMA((n_tp,)),
        pltpu.SemaphoreType.DMA((3,)),
        pltpu.SemaphoreType.DMA((3,)),
        pltpu.SemaphoreType.DMA((n_ep,)),
        pltpu.SemaphoreType.DMA((n_ep,)),
        pltpu.SemaphoreType.DMA((8,)),
        pltpu.SemaphoreType.DMA((8,)),
    ]
    Sh = jax.ShapeDtypeStruct
    layer_out, new_norm, new_max, key_w, value, keep = pl.pallas_call(
        functools.partial(layer_kernel, n_ep, n_tp),
        out_shape=(
            Sh((R, D), BF16),
            Sh((R, hd), F32),
            Sh((1, R), F32),
            Sh((R, hd), F32),
            Sh((R, hd), F32),
            Sh((R, hd), F32),
        ),
        in_specs=[vmem] * 11 + [hbm] * 12,
        out_specs=(vmem,) * 6,
        scratch_shapes=scratch,
        compiler_params=pltpu.CompilerParams(
            collective_id=0, has_side_effects=True, vmem_limit_bytes=66_000_000
        ),
    )(
        tokens,
        mixer_gain[None, :],
        w_ingate.T,
        w_forget.T,
        forget_bias[None, :],
        state_norm.reshape(R, hd),
        state_max.T,
        ffn_gain[None, :],
        w_branch.reshape(-1, LANES),
        routes.T,
        route_weight.T,
        state_matrix,
        w_query,
        w_key,
        w_value,
        w_outgate,
        w_proj,
        expert_gate,
        expert_up,
        expert_down,
        dense_gate,
        dense_up,
        dense_down,
    )
    new_matrix = (
        keep[:, None, None, :] * state_matrix + key_w[:, None, :, None] * value[:, None, None, :]
    )
    return (layer_out, new_matrix, new_norm.reshape(R, 1, hd), new_max.T)


def solution(mesh):
    in_specs = (
        P("ep", None),
        P("ep", "tp", None, None),
        P("ep", "tp", None),
        P("ep", "tp"),
        P(),
        P("ep", "tp"),
        P("ep", "tp"),
        P("ep", "tp"),
        P("ep", "tp"),
        P(),
        P(),
        P(),
        P("tp", "ep"),
        P(),
        P(),
        P("ep", None),
        P("ep", None),
        P("ep", None, "tp"),
        P("ep", None, "tp"),
        P("ep", "tp", None),
        P("ep", "tp"),
        P("ep", "tp"),
        P("tp", "ep"),
    )
    out_specs = (P("ep", None), P("ep", "tp", None, None), P("ep", "tp", None), P("ep", "tp"))
    return jax.shard_map(
        functools.partial(on_device, mesh.shape["ep"], mesh.shape["tp"]),
        mesh=mesh,
        in_specs=in_specs,
        out_specs=out_specs,
        check_vma=False,
    )
```

```python
import functools

import jax
import jax.numpy as jnp
from jax import lax
from jax.experimental import pallas as pl
from jax.experimental.pallas import tpu as pltpu
from jax.sharding import PartitionSpec as P

EPS = 1e-06
LANES = 128
CAP = 6
PAD = 8
F32 = jnp.float32
BF16 = jnp.bfloat16
MESH = pl.DeviceIdType.MESH


def dot(a, b):
    return jnp.dot(a, b, preferred_element_type=F32)


def dot_t(a, b):
    return lax.dot_general(a, b, (((1,), (1,)), ((), ())), preferred_element_type=F32)


def iota(shape, dim):
    return lax.broadcasted_iota(jnp.int32, shape, dim)


def layer_kernel(
    n_ep,
    n_tp,
    tokens_ref,
    gain_ref,
    win_ref,
    wfo_ref,
    bias_ref,
    norm_ref,
    smax_ref,
    fgain_ref,
    branch_ref,
    routes_ref,
    weight_ref,
    state_hbm,
    wq_hbm,
    wk_hbm,
    wv_hbm,
    wo_hbm,
    wproj_hbm,
    eg_hbm,
    eu_hbm,
    ed_hbm,
    dg_hbm,
    du_hbm,
    dd_hbm,
    out_ref,
    norm_out_ref,
    max_out_ref,
    keyw_ref,
    value_ref,
    keep_ref,
    state,
    wcat,
    wproj,
    eg,
    eu,
    edc,
    dgu,
    dd,
    nrm,
    x_all,
    info,
    info_recv,
    part_send,
    part_recv,
    numer,
    mix_send,
    mix_all,
    raw_blk,
    res_all,
    res_t,
    xg,
    gmat,
    stat,
    stat_recv,
    dense_send,
    da_recv,
    db_recv,
    a2_send,
    a2_recv,
    b2_send,
    b2_recv,
    disp_send,
    xrecv,
    hid_all,
    yo_send,
    yo_recv,
    fin_send,
    fin_recv,
    dno_send,
    dno_recv,
    dn_send,
    dn_recv,
    tp_send,
    tp_recv,
    out_all,
    load_sems,
    send_ep,
    recv_ep,
    send_tp,
    recv_tp,
    send_mx,
    recv_mx,
    send_tr,
    recv_tr,
    send_fw,
    recv_fw,
    send_sb,
    recv_sb,
    send_a,
    recv_a,
    send_b,
    recv_b,
):
    e = lax.axis_index("ep")
    t = lax.axis_index("tp")
    R, D = tokens_ref.shape
    N = R * n_ep
    Dc = D // n_ep
    HD = Dc // 2
    DH = D // 2
    W = mix_send.shape[1]
    F = dd.shape[0]
    EX = {16: 4, 4: 2}[n_ep]
    EY = n_ep // EX
    TZ = n_tp // 2
    S = CAP * n_ep
    S8 = PAD * n_ep
    Q = N // LANES
    PER = LANES // R
    RC = R * EX
    ey, ex = e // EX, lax.rem(e, EX)
    mine_group = lax.rem(t + e, n_ep)
    tz, tc = t // 2, lax.rem(t, 2)

    def at(index, size):
        return pl.ds(pl.multiple_of(index * size, size), size)

    def ring(d, n):
        return min(d, n - d)

    ep_far = sorted(range(1, n_ep), key=lambda k: -(ring(k // EX, EY) + ring(k % EX, EX)))
    dz_far = sorted(range(1, TZ), key=lambda d: -ring(d, TZ))
    dy_far = sorted(range(EY), key=lambda d: -ring(d, EY))
    dx_far = sorted(range(EX), key=lambda d: -ring(d, EX))

    def ep_peer(k):
        return lax.rem(ey + k // EX, EY) * EX + lax.rem(ex + k % EX, EX)

    def ep_from(k):
        return lax.rem(ey + EY - k // EX, EY) * EX + lax.rem(ex + EX - k % EX, EX)

    def tp_peer(k):
        return lax.rem(tz + k // 2, TZ) * 2 + lax.rem(tc + k % 2, 2)

    sibling = tz * 2 + 1 - tc

    loads = []

    def load(src, dst):
        copy = pltpu.make_async_copy(src, dst, load_sems.at[len(loads)])
        copy.start()
        loads.append(copy)
        return copy

    pending = []

    def ep_start(phase, k, src, dst):
        copy = pltpu.make_async_remote_copy(
            src_ref=src,
            dst_ref=dst,
            send_sem=send_ep.at[phase, k],
            recv_sem=recv_ep.at[phase, k],
            device_id={"ep": ep_peer(k)},
            device_id_type=MESH,
        )
        copy.start()
        pending.append(copy)
        return copy

    def tp_start(phase, k, src, dst):
        copy = pltpu.make_async_remote_copy(
            src_ref=src,
            dst_ref=dst,
            send_sem=send_tp.at[phase, k],
            recv_sem=recv_tp.at[phase, k],
            device_id={"tp": tp_peer(k)},
            device_id_type=MESH,
        )
        copy.start()
        pending.append(copy)
        return copy

    def side_start(send_sem, recv_sem, src, dst):
        copy = pltpu.make_async_remote_copy(
            src_ref=src,
            dst_ref=dst,
            send_sem=send_sem,
            recv_sem=recv_sem,
            device_id={"tp": sibling},
            device_id_type=MESH,
        )
        copy.start()
        pending.append(copy)
        return copy

    def spread_tp(phase, region):
        copies = {dz: tp_start(phase, 2 * dz, region(t), region(t)) for dz in dz_far}
        copies[0] = tp_start(phase, 1, region(t), region(t))
        return copies

    def gather_tp(phase, region, copies):
        passed = []
        for dz in reversed(dz_far):
            copies[dz].wait_recv()
            source = lax.rem(tz + TZ - dz, TZ) * 2 + tc
            odd = 2 * dz + 1
            passed.append(
                side_start(
                    send_tp.at[phase, odd], recv_tp.at[phase, odd], region(source), region(source)
                )
            )
        copies[0].wait_recv()
        for copy in passed:
            copy.wait_recv()

    def raw_copy():
        return pltpu.make_async_remote_copy(
            src_ref=tokens_ref.at[:, at(t, Dc)],
            dst_ref=raw_blk,
            send_sem=send_tr.at[0],
            recv_sem=recv_tr.at[0],
            device_id={"ep": t, "tp": lax.rem(e + n_ep - t, n_ep)},
            device_id_type=MESH,
        )

    raw_away = jnp.logical_or(e != 0, t != 0)
    fin_recv[...] = jnp.zeros_like(fin_recv)

    barrier = pltpu.get_barrier_semaphore()
    for k in ep_far:
        pl.semaphore_signal(barrier, inc=1, device_id={"ep": ep_peer(k)}, device_id_type=MESH)
    for k in range(1, n_tp):
        pl.semaphore_signal(barrier, inc=1, device_id={"tp": tp_peer(k)}, device_id_type=MESH)

    load_w = [
        load(src, wcat.at[:, pl.ds(i * W, W)])
        for i, src in enumerate((wq_hbm, wk_hbm, wv_hbm, wo_hbm))
    ]
    load_proj = load(wproj_hbm, wproj.at[at(t, W), :])
    load_state = load(state_hbm, state)
    load_dg, load_du = load(dg_hbm, dgu.at[:, pl.ds(0, F)]), load(du_hbm, dgu.at[:, pl.ds(F, F)])
    load_eg, load_eu = load(eg_hbm, eg), load(eu_hbm, eu)
    load_ed = [
        load(ed_hbm.at[0, :, at(2 * b + side, HD)], edc.at[i, :, pl.ds(b * HD, HD)])
        for i, side in enumerate((1 - tc, tc))
        for b in range(n_ep)
    ]
    load_dd = load(dd_hbm, dd)

    wide = tokens_ref[...].astype(F32)
    scale = lax.rsqrt(jnp.mean(wide * wide, axis=-1, keepdims=True) + EPS)
    nrm[...] = (wide * scale * gain_ref[...]).astype(BF16)

    r0, r1 = routes_ref[0:1, :], routes_ref[1:2, :]
    w0, w1 = weight_ref[0:1, :], weight_ref[1:2, :]
    total = w0 + w1
    which = iota((n_ep, R), 0)
    hit0, hit1 = which == r0, which == r1
    named = jnp.where(jnp.logical_or(hit0, hit1), 1.0, 0.0)
    earlier = jnp.where(iota((R, R), 0) < iota((R, R), 1), 1.0, 0.0).astype(BF16)
    slot = dot(named.astype(BF16), earlier)
    code = jnp.where(named > 0.0, slot + 1.0, 0.0)
    group_at = (e * CAP).astype(F32)
    rowcode = jnp.where(named > 0.0, slot + (1.0 + group_at), 0.0)
    shares = jnp.where(hit0, w0 / total, 0.0) + jnp.where(hit1, w1 / total, 0.0)
    info[:, 0:R] = rowcode
    info[:, R : 2 * R] = shares
    info[:, 2 * R : LANES] = jnp.zeros((n_ep, LANES - 2 * R), F32)

    pl.semaphore_wait(barrier, n_ep - 1 + n_tp - 1)
    got_x = {k: ep_start(0, k, nrm.at[:, at(ep_peer(k), Dc)], x_all.at[at(e, R), :]) for k in ep_far}
    x_all[at(e, R), :] = nrm[:, at(e, Dc)]
    load_proj.wait()

    def proj_rows(tt):
        return wproj.at[at(tt, W), :]

    got_wp = spread_tp(0, proj_rows)

    gate_in = dot_t(nrm[...], win_ref[...])
    gate_fo = dot_t(nrm[...], wfo_ref[...]) + bias_ref[...]
    mine = iota(gate_in.shape, 1) == t
    g_in = jnp.sum(jnp.where(mine, gate_in, 0.0), axis=1, keepdims=True)
    g_fo = jnp.sum(jnp.where(mine, gate_fo, 0.0), axis=1, keepdims=True)
    eye = iota((R, R), 0) == iota((R, R), 1)
    smax = jnp.sum(jnp.where(eye, smax_ref[...], 0.0), axis=1, keepdims=True)
    log_keep = jnp.minimum(g_fo, 0.0) - jnp.log(1.0 + jnp.exp(-jnp.abs(g_fo)))
    carried = log_keep + smax
    new_max = jnp.maximum(carried, g_in)
    keep = jnp.exp(carried - new_max)
    write = jnp.exp(g_in - new_max)
    max_out_ref[...] = jnp.sum(jnp.where(eye, new_max, 0.0), axis=0, keepdims=True)
    keep_ref[...] = jnp.broadcast_to(keep, keep_ref.shape)

    for copy in load_w:
        copy.wait()
    got_part = {}
    for dy in [(EY - d) % EY for d in range(EY)]:
        back = (EY - dy) % EY
        for dx in range(EX):
            k = dy * EX + dx
            if k:
                got_x[k].wait_recv()
        rows = at(lax.rem(ey + back, EY), RC)
        part_send[rows, :] = dot(x_all[rows, :], wcat[...]).astype(BF16)
        for dx in dx_far:
            k = back * EX + dx
            if k:
                got_part[k] = ep_start(1, k, part_send.at[at(ep_peer(k), R), :], part_recv.at[k])
    got_info = {k: ep_start(2, k, info, info_recv.at[k]) for k in ep_far}

    @pl.when(raw_away)
    def _():
        raw_copy().start()

    @pl.when(jnp.logical_not(raw_away))
    def _():
        raw_blk[...] = tokens_ref[:, at(t, Dc)]

    proj = part_send[at(e, R), :].astype(F32)
    for k in reversed(ep_far):
        got_part[k].wait_recv()
        proj += part_recv[k].astype(F32)

    load_state.wait()
    q = proj[:, 0:W]
    key = proj[:, W : 2 * W] * W ** (-0.5)
    val = proj[:, 2 * W : 3 * W]
    og = proj[:, 3 * W : 4 * W]
    key_w = write * key
    new_norm = keep * norm_ref[...] + key_w
    q_t = q.T
    for b in range(R):
        numer[b : b + 1, :] = jnp.sum(q_t[:, b : b + 1] * state[b, 0], axis=0, keepdims=True)
    top = keep * numer[...] + jnp.sum(q * key_w, axis=1, keepdims=True) * val
    denom = jnp.sum(q * new_norm, axis=1, keepdims=True)
    cell = top / jnp.maximum(jnp.abs(denom), 1.0)
    mix_send[...] = (cell / (1.0 + jnp.exp(-og))).astype(BF16)

    def mix_copy(k):
        return pltpu.make_async_remote_copy(
            src_ref=mix_send,
            dst_ref=mix_all.at[:, at(t, W)],
            send_sem=send_mx.at[k],
            recv_sem=recv_mx.at[t],
            device_id={"ep": ep_peer(k), "tp": lax.rem(e + n_ep - ep_peer(k), n_ep)},
            device_id_type=MESH,
        )

    for k in ep_far:
        mix_copy(k).start()

    @pl.when(t != 0)
    def _():
        mix_copy(0).start()

    @pl.when(t == 0)
    def _():
        mix_all[:, at(t, W)] = mix_send[...]

    gather_tp(0, proj_rows, got_wp)
    norm_out_ref[...] = new_norm
    keyw_ref[...] = key_w
    value_ref[...] = val

    for k in ep_far:
        got_info[k].wait_recv()
    quarter = iota((n_ep, LANES), 1) // R
    codes, sharesl = [], []

    info_recv[0] = info[...]
    for qq in range(Q):
        ctile = jnp.zeros((n_ep, LANES), F32)
        stile = jnp.zeros((n_ep, LANES), F32)
        for j in range(PER):
            g = qq * PER + j
            gy, gx = g // EX, g % EX
            slot_k = lax.rem(ey + (EY - gy), EY) * EX + lax.rem(ex + (EX - gx), EX)
            tile = info_recv[slot_k]
            there = quarter == j
            ctile += jnp.where(there, tile if j == 0 else pltpu.roll(tile, j * R, 1), 0.0)
            back = (j - 1) % PER * R
            stile += jnp.where(there, tile if back == 0 else pltpu.roll(tile, back, 1), 0.0)
        codes.append(ctile)
        sharesl.append(stile)
    code_all = jnp.concatenate(codes, axis=1) if Q > 1 else codes[0]
    share_all = jnp.concatenate(sharesl, axis=1) if Q > 1 else sharesl[0]
    row_no = (iota((S, N), 0) + 1).astype(F32)
    for p in range(n_ep):
        gmat[p * S : (p + 1) * S, :] = jnp.where(row_no == code_all[p : p + 1, :], 1.0, 0.0).astype(
            BF16
        )
    is_mine = iota((n_ep, N), 0) == e
    my_code = jnp.sum(jnp.where(is_mine, code_all, 0.0), axis=0, keepdims=True)
    my_share = jnp.sum(jnp.where(is_mine, share_all, 0.0), axis=0, keepdims=True)
    my_code8 = jnp.where(
        my_code > 0.0, my_code + ((PAD - CAP) * (iota((1, N), 1) // R)).astype(F32), 0.0
    )
    row_share = jnp.sum(
        jnp.where((iota((S8, N), 0) + 1).astype(F32) == my_code8, my_share, 0.0),
        axis=1,
        keepdims=True,
    )
    spread = jnp.where(
        jnp.logical_and(
            iota((S8, S), 0) // PAD * CAP + iota((S8, S), 0) % PAD == iota((S8, S), 1),
            iota((S8, S), 0) % PAD < CAP,
        ),
        1.0,
        0.0,
    ).astype(BF16)
    repeat = jnp.where(iota((S8, n_ep), 0) // PAD == iota((S8, n_ep), 1), 1.0, 0.0).astype(BF16)
    code_rep = dot(repeat, code.astype(BF16))
    pick_t = jnp.where((iota((S8, R), 0) % PAD + 1).astype(F32) == code_rep, 1.0, 0.0)
    pick = pick_t.T.astype(BF16)

    @pl.when(raw_away)
    def _():
        raw_copy().wait()

    for tt in range(n_tp):

        def arrive_mix(tt=tt):
            pltpu.make_async_remote_copy(
                src_ref=mix_send,
                dst_ref=mix_all.at[:, pl.ds(tt * W, W)],
                send_sem=send_mx.at[0],
                recv_sem=recv_mx.at[tt],
                device_id={"tp": sibling},
                device_id_type=MESH,
            ).wait_recv()

        if tt:
            arrive_mix()
        else:
            pl.when(t != 0)(arrive_mix)

    mine_res = raw_blk[...].astype(F32) + dot(mix_all[...], wproj[...])
    my_rows = at(mine_group, R)
    res_all[my_rows, :] = mine_res.astype(BF16)

    def res_rows(tt):
        return res_all.at[at(lax.rem(tt + e, n_ep), R), :]

    got_res = spread_tp(1, res_rows)

    def half_copy(c):
        return pltpu.make_async_remote_copy(
            src_ref=res_all.at[my_rows, pl.ds(c * HD, HD)],
            dst_ref=res_t.at[:, at(lax.rem(e, 2), HD)],
            send_sem=send_tr.at[1 + c],
            recv_sem=recv_tr.at[1 + lax.rem(e, 2)],
            device_id={"ep": mine_group, "tp": e // 2 * 2 + c},
            device_id_type=MESH,
        )

    stays = jnp.logical_and(t == 0, e < 2)

    @pl.when(jnp.logical_not(stays))
    def _():
        half_copy(0).start()

    @pl.when(stays)
    def _():
        res_t[:, at(lax.rem(e, 2), HD)] = res_all[my_rows, 0:HD]

    half_copy(1).start()

    load_dg.wait()
    load_du.wait()
    my_fgain = fgain_ref[:, at(e, Dc)]

    def stage_a(g):
        gy, gx = g // EX, lax.rem(g, EX)
        dx = lax.rem(gx + EX - ex, EX)
        return pltpu.make_async_remote_copy(
            src_ref=dense_send.at[at(g, R), pl.ds(0, F)],
            dst_ref=da_recv.at[dx, gy],
            send_sem=send_a.at[g],
            recv_sem=recv_a.at[dx * EY + gy],
            device_id={"ep": ey * EX + gx},
            device_id_type=MESH,
        )

    def stage_b(g):
        gy, gx = g // EX, lax.rem(g, EX)
        dy = lax.rem(gy + EY - ey, EY)
        return pltpu.make_async_remote_copy(
            src_ref=dense_send.at[at(g, R), pl.ds(F, F)],
            dst_ref=db_recv.at[dy, gx],
            send_sem=send_b.at[g],
            recv_sem=recv_b.at[dy * EX + gx],
            device_id={"ep": gy * EX + ex},
            device_id_type=MESH,
        )

    def dense_part(tt):
        g = lax.rem(tt + e, n_ep)
        rows = at(g, R)
        xg[rows, :] = (res_all[rows, :].astype(F32) * my_fgain).astype(BF16)
        dense_send[rows, :] = dot(xg[rows, :], dgu[...]).astype(BF16)

        @pl.when(lax.rem(g, EX) != ex)
        def _():
            stage_a(g).start()

        @pl.when(g // EX != ey)
        def _():
            stage_b(g).start()

    dense_part(t)
    got_res[0].wait_recv()
    dense_part(sibling)
    late = None
    for dz in reversed(dz_far):
        got_res[dz].wait_recv()
        there = lax.rem(tz + TZ - dz, TZ) * 2
        odd = 2 * dz + 1
        passing = side_start(
            send_tp.at[1, odd], recv_tp.at[1, odd], res_rows(there + tc), res_rows(there + tc)
        )
        dense_part(there + tc)
        if late is not None:
            late[0].wait_recv()
            dense_part(late[1])
        late = (passing, there + 1 - tc)
    late[0].wait_recv()
    dense_part(late[1])

    wide_branch = branch_ref[...].astype(F32)
    pieces = Dc // LANES
    branch_rows = [
        jnp.sum(
            jnp.where(iota(wide_branch.shape, 0) == e * pieces + i, wide_branch, 0.0),
            axis=0,
            keepdims=True,
        )
        for i in range(pieces)
    ]
    my_branch = jnp.concatenate(branch_rows, axis=1) if pieces > 1 else branch_rows[0]
    my_branch = jnp.broadcast_to(my_branch, (8, Dc)).astype(BF16)
    ones = jnp.ones((8, Dc), BF16)
    block = res_all[...].astype(F32)
    square = block * block
    high = square.astype(BF16)
    low = (square - high.astype(F32)).astype(BF16)
    sums = dot_t(ones, high) + dot_t(ones, low)
    branch = dot_t(my_branch, xg[...])
    row8 = iota((8, LANES), 0)
    tile = jnp.zeros((8, LANES), F32)
    for qq in range(Q):
        cols = slice(qq * LANES, (qq + 1) * LANES)
        tile += jnp.where(row8 == qq, sums[:, cols], 0.0)
        tile += jnp.where(row8 == 4 + qq, branch[:, cols], 0.0)
    stat[...] = tile
    got_stat = {k: ep_start(3, k, stat, stat_recv.at[k]) for k in ep_far}

    got_disp = {}

    def dispatch(dy):
        rows = at(lax.rem(ey + dy, EY), S * EX)
        disp_send[rows, :] = dot(gmat[rows, :], xg[:, at(tc, HD)]).astype(BF16)
        for dx in dx_far:
            k = dy * EX + dx
            if k:
                got_disp[k] = ep_start(
                    5, k, disp_send.at[at(ep_peer(k), S), :], xrecv.at[:, at(2 * e + tc, HD)]
                )

    for dy in dy_far[: EY // 2]:
        dispatch(dy)

    got_a, got_b = {}, {}
    for d in dy_far:
        gy = lax.rem(ey + d, EY)
        term = dense_send[at(gy * EX + ex, R), 0:F].astype(F32)
        for dx in range(1, EX):
            pltpu.make_async_remote_copy(
                src_ref=dense_send.at[pl.ds(0, R), pl.ds(0, F)],
                dst_ref=da_recv.at[dx, gy],
                send_sem=send_a.at[0],
                recv_sem=recv_a.at[dx * EY + gy],
                device_id={"ep": e},
                device_id_type=MESH,
            ).wait_recv()
            term += da_recv[dx, gy].astype(F32)
        if d:
            a2_send[d] = term.astype(BF16)
            got_a[d] = ep_start(4, d * EX, a2_send.at[d], a2_recv.at[d])
        else:
            g = term
    for d in dx_far:
        gx = lax.rem(ex + d, EX)
        term = dense_send[at(ey * EX + gx, R), F : 2 * F].astype(F32)
        for dy in range(1, EY):
            pltpu.make_async_remote_copy(
                src_ref=dense_send.at[pl.ds(0, R), pl.ds(F, F)],
                dst_ref=db_recv.at[dy, gx],
                send_sem=send_b.at[0],
                recv_sem=recv_b.at[dy * EX + gx],
                device_id={"ep": e},
                device_id_type=MESH,
            ).wait_recv()
            term += db_recv[dy, gx].astype(F32)
        if d:
            b2_send[d] = term.astype(BF16)
            got_b[d] = ep_start(4, d, b2_send.at[d], b2_recv.at[d])
        else:
            u = term

    for dy in dy_far[EY // 2 :]:
        dispatch(dy)
    xrecv[:, at(2 * e + tc, HD)] = disp_send[at(e, S), :]

    def forward(k):
        region = xrecv.at[:, at(2 * ep_from(k) + tc, HD)]
        return side_start(send_fw.at[k], recv_fw.at[k], region, region)

    passed = [forward(0)]

    for k in reversed(ep_far):
        got_stat[k].wait_recv()
        tile += stat_recv[k]
    scale_l = lax.rsqrt(tile[0:Q, :] * (1.0 / D) + EPS)
    share_l = 1.0 / (1.0 + jnp.exp(-(scale_l * tile[4 : 4 + Q, :])))
    my_scale = jnp.zeros((R, 1), F32)
    my_bshare = jnp.zeros((R, 1), F32)
    for qq in range(Q):
        here = iota((R, LANES), 1) + qq * LANES == iota((R, LANES), 0) + e * R
        my_scale += jnp.sum(jnp.where(here, scale_l[qq : qq + 1, :], 0.0), axis=1, keepdims=True)
        my_bshare += jnp.sum(jnp.where(here, share_l[qq : qq + 1, :], 0.0), axis=1, keepdims=True)
    scale_row = (
        jnp.concatenate([scale_l[qq : qq + 1, :] for qq in range(Q)], axis=1) if Q > 1 else scale_l
    )
    row_scale = jnp.sum(jnp.where(row_no == my_code, scale_row, 0.0), axis=1, keepdims=True)

    for d in reversed(dy_far):
        if d:
            got_a[d].wait_recv()
            g += a2_recv[d].astype(F32)
    for d in reversed(dx_far):
        if d:
            got_b[d].wait_recv()
            u += b2_recv[d].astype(F32)
    g, u = g * my_scale, u * my_scale
    hid_all[at(e, R), :] = (g / (1.0 + jnp.exp(-g)) * u).astype(BF16)
    got_hid = {
        k: ep_start(6, k, hid_all.at[at(e, R), :], hid_all.at[at(e, R), :]) for k in ep_far
    }

    load_eg.wait()
    load_eu.wait()
    for k in reversed(ep_far):
        got_disp[k].wait_recv()
        passed.append(forward(k))
    for copy in passed:
        copy.wait_recv()
    gp = dot(xrecv[...], eg[0]) * row_scale
    up = dot(xrecv[...], eu[0]) * row_scale
    ehid = (gp / (1.0 + jnp.exp(-gp)) * up).astype(BF16)
    ehid8 = dot(spread, ehid).astype(BF16)
    for copy in load_ed:
        copy.wait()
    step = min(512, DH)
    strips = [slice(c * step, (c + 1) * step) for c in range(DH // step)]
    got_yo = []
    for i, cols in enumerate(strips):
        yo_send[:, cols] = (dot(ehid8, edc[0, :, cols]) * row_share).astype(BF16)
        got_yo.append(
            side_start(send_sb.at[i], recv_sb.at[i], yo_send.at[:, cols], yo_recv.at[:, cols])
        )
    got_fin = {}
    wide = DH // 2
    per_strip = max(1, wide // step)
    for i, (copy, cols) in enumerate(zip(got_yo, strips)):
        y = dot(ehid8, edc[1, :, cols]) * row_share
        copy.wait_recv()
        y += yo_recv[:, cols].astype(F32)
        fin_send[:, :, cols] = y.reshape(n_ep, PAD, step).astype(BF16)
        if i % per_strip == per_strip - 1:
            j = i // per_strip
            part = pl.ds(j * per_strip * step, per_strip * step)
            for k in ep_far:
                got_fin[j, k] = ep_start(
                    7 + j,
                    k,
                    fin_send.at[ep_peer(k), pl.ds(0, CAP), part],
                    fin_recv.at[e, pl.ds(0, CAP), part],
                )
    fin_recv[e] = fin_send[e]

    load_dd.wait()
    got_no = {}
    for dy in reversed(dy_far):
        for dx in range(EX):
            k = (EY - dy) % EY * EX + dx
            if k:
                got_hid[k].wait_recv()
        rows = at(lax.rem(ey + dy, EY), RC)
        dno_send[rows, :] = dot(hid_all[rows, :], dd[:, at(1 - tc, HD)]).astype(BF16)
        got_no[dy] = side_start(
            send_sb.at[4 + dy], recv_sb.at[4 + dy], dno_send.at[rows, :], dno_recv.at[rows, :]
        )
    got_dn = {}
    for dy in reversed(dy_far):
        rows = at(lax.rem(ey + dy, EY), RC)
        down = dot(hid_all[rows, :], dd[:, at(tc, HD)])
        got_no[dy].wait_recv()
        dn_send[rows, :] = (down + dno_recv[rows, :].astype(F32)).astype(BF16)
        for dx in dx_far:
            k = dy * EX + dx
            if k:
                got_dn[k] = ep_start(
                    9, k, dn_send.at[at(ep_peer(k), R), :], dn_recv.at[:, at(e, HD)]
                )
    dn_recv[:, at(e, HD)] = dn_send[at(e, R), :]

    for copy in got_fin.values():
        copy.wait_recv()
    for k in reversed(ep_far):
        got_dn[k].wait_recv()
    got_tp = {}
    for dz in dz_far + [0]:
        cols = at(lax.rem(tz + dz, TZ), Dc)
        back = fin_recv[:, :, cols].astype(F32).reshape(S8, Dc).astype(BF16)
        piece = dot(pick, back) + my_bshare * dn_recv[:, cols].astype(F32)
        tp_send[:, cols] = piece.astype(BF16)
        if dz:
            got_tp[dz] = tp_start(2, 2 * dz, tp_send.at[:, cols], tp_recv.at[dz])

    for i in range(2):

        @pl.when(jnp.logical_not(jnp.logical_and(t == 0, e == i)))
        def _():
            pltpu.make_async_remote_copy(
                src_ref=res_all.at[pl.ds(0, R), pl.ds(0, HD)],
                dst_ref=res_t.at[:, pl.ds(i * HD, HD)],
                send_sem=send_tr.at[1 + i],
                recv_sem=recv_tr.at[1 + i],
                device_id={"tp": sibling},
                device_id_type=MESH,
            ).wait_recv()

    last = res_t[...].astype(F32) + tp_send[:, at(tz, Dc)].astype(F32)
    for dz in reversed(dz_far):
        got_tp[dz].wait_recv()
        last += tp_recv[dz].astype(F32)
    out_all[:, at(tc * TZ + tz, Dc)] = last.astype(BF16)

    def out_cols(tt):
        return out_all.at[:, at(lax.rem(tt, 2) * TZ + tt // 2, Dc)]

    got_out = spread_tp(3, out_cols)
    for k in ep_far:
        mix_copy(k).wait_send()

    @pl.when(t != 0)
    def _():
        mix_copy(0).wait_send()

    @pl.when(jnp.logical_not(stays))
    def _():
        half_copy(0).wait_send()

    half_copy(1).wait_send()
    for g in range(n_ep):

        @pl.when(g % EX != ex)
        def _():
            stage_a(g).wait_send()

        @pl.when(g // EX != ey)
        def _():
            stage_b(g).wait_send()

    gather_tp(3, out_cols, got_out)
    for b in range(n_ep):
        for c in range(2):
            out_ref[:, pl.ds((2 * b + c) * HD, HD)] = out_all[:, pl.ds(c * DH + b * HD, HD)]
    for copy in pending:
        copy.wait_send()


def on_device(
    n_ep,
    n_tp,
    tokens,
    state_matrix,
    state_norm,
    state_max,
    mixer_gain,
    w_query,
    w_key,
    w_value,
    w_outgate,
    w_ingate,
    w_forget,
    forget_bias,
    w_proj,
    ffn_gain,
    w_branch,
    routes,
    route_weight,
    expert_gate,
    expert_up,
    expert_down,
    dense_gate,
    dense_up,
    dense_down,
):
    R, D = tokens.shape
    hd = state_norm.shape[2]
    N, Dc, DH, W = R * n_ep, D // n_ep, D // 2, hd
    F = dense_gate.shape[1]
    FE = expert_gate.shape[2]
    S, S8 = CAP * n_ep, PAD * n_ep
    EX = {16: 4, 4: 2}[n_ep]
    EY = n_ep // EX
    vmem = pl.BlockSpec(memory_space=pltpu.VMEM)
    hbm = pl.BlockSpec(memory_space=pl.ANY)
    V = pltpu.VMEM
    scratch = [
        V(state_matrix.shape, F32),
        V((Dc, 4 * W), BF16),
        V((n_tp * W, Dc), BF16),
        V(expert_gate.shape, BF16),
        V(expert_up.shape, BF16),
        V((2, FE, DH), BF16),
        V((Dc, 2 * F), BF16),
        V(dense_down.shape, BF16),
        V((R, D), BF16),
        V((N, Dc), BF16),
        V((n_ep, LANES), F32),
        V((n_ep, n_ep, LANES), F32),
        V((N, 4 * W), BF16),
        V((n_ep, R, 4 * W), BF16),
        V((R, W), F32),
        V((R, W), BF16),
        V((R, n_tp * W), BF16),
        V((R, Dc), BF16),
        V((N, Dc), BF16),
        V((R, Dc), BF16),
        V((N, Dc), BF16),
        V((n_ep * S, N), BF16),
        V((8, LANES), F32),
        V((n_ep, 8, LANES), F32),
        V((N, 2 * F), BF16),
        V((EX, EY, R, F), BF16),
        V((EY, EX, R, F), BF16),
        V((EY, R, F), BF16),
        V((EY, R, F), BF16),
        V((EX, R, F), BF16),
        V((EX, R, F), BF16),
        V((n_ep * S, Dc // 2), BF16),
        V((S, D), BF16),
        V((N, F), BF16),
        V((S8, DH), BF16),
        V((S8, DH), BF16),
        V((n_ep, PAD, DH), BF16),
        V((n_ep, PAD, DH), BF16),
        V((N, Dc // 2), BF16),
        V((N, Dc // 2), BF16),
        V((N, Dc // 2), BF16),
        V((R, DH), BF16),
        V((R, DH), BF16),
        V((n_tp // 2, R, Dc), BF16),
        V((R, D), BF16),
        pltpu.SemaphoreType.DMA((11 + 2 * n_ep,)),
        pltpu.SemaphoreType.DMA((10, n_ep)),
        pltpu.SemaphoreType.DMA((10, n_ep)),
        pltpu.SemaphoreType.DMA((4, n_tp)),
        pltpu.SemaphoreType.DMA((4, n_tp)),
        pltpu.SemaphoreType.DMA((n_ep,)),
        pltpu.SemaphoreType.DMA((n_tp,)),
        pltpu.SemaphoreType.DMA((3,)),
        pltpu.SemaphoreType.DMA((3,)),
        pltpu.SemaphoreType.DMA((n_ep,)),
        pltpu.SemaphoreType.DMA((n_ep,)),
        pltpu.SemaphoreType.DMA((8,)),
        pltpu.SemaphoreType.DMA((8,)),
        pltpu.SemaphoreType.DMA((n_ep,)),
        pltpu.SemaphoreType.DMA((n_ep,)),
        pltpu.SemaphoreType.DMA((n_ep,)),
        pltpu.SemaphoreType.DMA((n_ep,)),
    ]
    Sh = jax.ShapeDtypeStruct
    layer_out, new_norm, new_max, key_w, value, keep = pl.pallas_call(
        functools.partial(layer_kernel, n_ep, n_tp),
        out_shape=(
            Sh((R, D), BF16),
            Sh((R, hd), F32),
            Sh((1, R), F32),
            Sh((R, hd), F32),
            Sh((R, hd), F32),
            Sh((R, hd), F32),
        ),
        in_specs=[vmem] * 11 + [hbm] * 12,
        out_specs=(vmem,) * 6,
        scratch_shapes=scratch,
        compiler_params=pltpu.CompilerParams(
            collective_id=0, has_side_effects=True, vmem_limit_bytes=66_000_000
        ),
    )(
        tokens,
        mixer_gain[None, :],
        w_ingate.T,
        w_forget.T,
        forget_bias[None, :],
        state_norm.reshape(R, hd),
        state_max.T,
        ffn_gain[None, :],
        w_branch.reshape(-1, LANES),
        routes.T,
        route_weight.T,
        state_matrix,
        w_query,
        w_key,
        w_value,
        w_outgate,
        w_proj,
        expert_gate,
        expert_up,
        expert_down,
        dense_gate,
        dense_up,
        dense_down,
    )
    new_matrix = (
        keep[:, None, None, :] * state_matrix + key_w[:, None, :, None] * value[:, None, None, :]
    )
    return (layer_out, new_matrix, new_norm.reshape(R, 1, hd), new_max.T)


def solution(mesh):
    in_specs = (
        P("ep", None),
        P("ep", "tp", None, None),
        P("ep", "tp", None),
        P("ep", "tp"),
        P(),
        P("ep", "tp"),
        P("ep", "tp"),
        P("ep", "tp"),
        P("ep", "tp"),
        P(),
        P(),
        P(),
        P("tp", "ep"),
        P(),
        P(),
        P("ep", None),
        P("ep", None),
        P("ep", None, "tp"),
        P("ep", None, "tp"),
        P("ep", "tp", None),
        P("ep", "tp"),
        P("ep", "tp"),
        P("tp", "ep"),
    )
    out_specs = (P("ep", None), P("ep", "tp", None, None), P("ep", "tp", None), P("ep", "tp"))
    return jax.shard_map(
        functools.partial(on_device, mesh.shape["ep"], mesh.shape["tp"]),
        mesh=mesh,
        in_specs=in_specs,
        out_specs=out_specs,
        check_vma=False,
    )
```

```python
import functools

import jax
import jax.numpy as jnp
from jax import lax
from jax.experimental import pallas as pl
from jax.experimental.pallas import tpu as pltpu
from jax.sharding import PartitionSpec as P

EPS = 1e-06
LANES = 128
CAP = 6
PAD = 8
F32 = jnp.float32
BF16 = jnp.bfloat16
MESH = pl.DeviceIdType.MESH


def dot(a, b):
    return jnp.dot(a, b, preferred_element_type=F32)


def dot_t(a, b):
    return lax.dot_general(a, b, (((1,), (1,)), ((), ())), preferred_element_type=F32)


def iota(shape, dim):
    return lax.broadcasted_iota(jnp.int32, shape, dim)


def layer_kernel(
    n_ep,
    n_tp,
    tokens_ref,
    gain_ref,
    win_ref,
    wfo_ref,
    bias_ref,
    norm_ref,
    smax_ref,
    fgain_ref,
    branch_ref,
    routes_ref,
    weight_ref,
    state_hbm,
    wq_hbm,
    wk_hbm,
    wv_hbm,
    wo_hbm,
    wproj_hbm,
    eg_hbm,
    eu_hbm,
    ed_hbm,
    dg_hbm,
    du_hbm,
    dd_hbm,
    out_ref,
    norm_out_ref,
    max_out_ref,
    mat_ref,
    state,
    wcat,
    wproj,
    eg,
    eu,
    edc,
    dgu,
    dd,
    nrm,
    x_all,
    info,
    info_recv,
    part_send,
    part_recv,
    numer,
    mix_send,
    mix_all,
    raw_blk,
    res_all,
    res_t,
    xg,
    gmat,
    stat,
    stat_recv,
    dense_send,
    da_recv,
    db_recv,
    a2_send,
    a2_recv,
    b2_send,
    b2_recv,
    disp_send,
    xrecv,
    hid_all,
    yo_send,
    yo_recv,
    fin_send,
    fin_recv,
    dno_send,
    dno_recv,
    dn_send,
    dn_recv,
    comb,
    tp_send,
    tp_recv,
    out_all,
    load_sems,
    send_ep,
    recv_ep,
    send_tp,
    recv_tp,
    send_mx,
    recv_mx,
    send_tr,
    recv_tr,
    send_fw,
    recv_fw,
    send_sb,
    recv_sb,
    send_a,
    recv_a,
    send_b,
    recv_b,
):
    e = lax.axis_index("ep")
    t = lax.axis_index("tp")
    R, D = tokens_ref.shape
    N = R * n_ep
    Dc = D // n_ep
    HD = Dc // 2
    DH = D // 2
    W = mix_send.shape[1]
    F = dd.shape[0]
    EX = {16: 4, 4: 2}[n_ep]
    EY = n_ep // EX
    TZ = n_tp // 2
    S = CAP * n_ep
    S8 = PAD * n_ep
    Q = N // LANES
    PER = LANES // R
    RC = R * EX
    ey, ex = e // EX, lax.rem(e, EX)
    mine_group = lax.rem(t + e, n_ep)
    tz, tc = t // 2, lax.rem(t, 2)

    def at(index, size):
        return pl.ds(pl.multiple_of(index * size, size), size)

    def ring(d, n):
        return min(d, n - d)

    ep_far = sorted(range(1, n_ep), key=lambda k: -(ring(k // EX, EY) + ring(k % EX, EX)))
    dz_far = sorted(range(1, TZ), key=lambda d: -ring(d, TZ))
    dy_far = sorted(range(EY), key=lambda d: -ring(d, EY))
    dx_far = sorted(range(EX), key=lambda d: -ring(d, EX))

    def ep_peer(k):
        return lax.rem(ey + k // EX, EY) * EX + lax.rem(ex + k % EX, EX)

    def ep_from(k):
        return lax.rem(ey + EY - k // EX, EY) * EX + lax.rem(ex + EX - k % EX, EX)

    def tp_peer(k):
        return lax.rem(tz + k // 2, TZ) * 2 + lax.rem(tc + k % 2, 2)

    sibling = tz * 2 + 1 - tc

    loads = []

    def load(src, dst):
        copy = pltpu.make_async_copy(src, dst, load_sems.at[len(loads)])
        copy.start()
        loads.append(copy)
        return copy

    pending = []

    def ep_start(phase, k, src, dst):
        copy = pltpu.make_async_remote_copy(
            src_ref=src,
            dst_ref=dst,
            send_sem=send_ep.at[phase, k],
            recv_sem=recv_ep.at[phase, k],
            device_id={"ep": ep_peer(k)},
            device_id_type=MESH,
        )
        copy.start()
        pending.append(copy)
        return copy

    def tp_start(phase, k, src, dst):
        copy = pltpu.make_async_remote_copy(
            src_ref=src,
            dst_ref=dst,
            send_sem=send_tp.at[phase, k],
            recv_sem=recv_tp.at[phase, k],
            device_id={"tp": tp_peer(k)},
            device_id_type=MESH,
        )
        copy.start()
        pending.append(copy)
        return copy

    def side_start(send_sem, recv_sem, src, dst):
        copy = pltpu.make_async_remote_copy(
            src_ref=src,
            dst_ref=dst,
            send_sem=send_sem,
            recv_sem=recv_sem,
            device_id={"tp": sibling},
            device_id_type=MESH,
        )
        copy.start()
        pending.append(copy)
        return copy

    def spread_tp(phase, region):
        copies = {dz: tp_start(phase, 2 * dz, region(t), region(t)) for dz in dz_far}
        copies[0] = tp_start(phase, 1, region(t), region(t))
        return copies

    def gather_tp(phase, region, copies):
        passed = []
        for dz in reversed(dz_far):
            copies[dz].wait_recv()
            source = lax.rem(tz + TZ - dz, TZ) * 2 + tc
            odd = 2 * dz + 1
            passed.append(
                side_start(
                    send_tp.at[phase, odd], recv_tp.at[phase, odd], region(source), region(source)
                )
            )
        copies[0].wait_recv()
        for copy in passed:
            copy.wait_recv()

    def raw_copy():
        return pltpu.make_async_remote_copy(
            src_ref=tokens_ref.at[:, at(t, Dc)],
            dst_ref=raw_blk,
            send_sem=send_tr.at[0],
            recv_sem=recv_tr.at[0],
            device_id={"ep": t, "tp": lax.rem(e + n_ep - t, n_ep)},
            device_id_type=MESH,
        )

    raw_away = jnp.logical_or(e != 0, t != 0)
    fin_recv[...] = jnp.zeros_like(fin_recv)

    barrier = pltpu.get_barrier_semaphore()
    for k in ep_far:
        pl.semaphore_signal(barrier, inc=1, device_id={"ep": ep_peer(k)}, device_id_type=MESH)
    for k in range(1, n_tp):
        pl.semaphore_signal(barrier, inc=1, device_id={"tp": tp_peer(k)}, device_id_type=MESH)

    load_w = [
        load(src, wcat.at[:, pl.ds(i * W, W)])
        for i, src in enumerate((wq_hbm, wk_hbm, wv_hbm, wo_hbm))
    ]
    load_proj = load(wproj_hbm, wproj.at[at(t, W), :])
    load_state = load(state_hbm, state)
    load_dg, load_du = load(dg_hbm, dgu.at[:, pl.ds(0, F)]), load(du_hbm, dgu.at[:, pl.ds(F, F)])
    load_eg, load_eu = load(eg_hbm, eg), load(eu_hbm, eu)
    load_ed = [
        load(ed_hbm.at[0, :, at(2 * b + side, HD)], edc.at[i, :, pl.ds(b * HD, HD)])
        for i, side in enumerate((1 - tc, tc))
        for b in range(n_ep)
    ]
    load_dd = load(dd_hbm, dd)

    wide = tokens_ref[...].astype(F32)
    scale = lax.rsqrt(jnp.mean(wide * wide, axis=-1, keepdims=True) + EPS)
    nrm[...] = (wide * scale * gain_ref[...]).astype(BF16)

    r0, r1 = routes_ref[0:1, :], routes_ref[1:2, :]
    w0, w1 = weight_ref[0:1, :], weight_ref[1:2, :]
    total = w0 + w1
    which = iota((n_ep, R), 0)
    hit0, hit1 = which == r0, which == r1
    named = jnp.where(jnp.logical_or(hit0, hit1), 1.0, 0.0)
    earlier = jnp.where(iota((R, R), 0) < iota((R, R), 1), 1.0, 0.0).astype(BF16)
    slot = dot(named.astype(BF16), earlier)
    code = jnp.where(named > 0.0, slot + 1.0, 0.0)
    group_at = (e * CAP).astype(F32)
    rowcode = jnp.where(named > 0.0, slot + (1.0 + group_at), 0.0)
    shares = jnp.where(hit0, w0 / total, 0.0) + jnp.where(hit1, w1 / total, 0.0)
    info[:, 0:R] = rowcode
    info[:, R : 2 * R] = shares
    info[:, 2 * R : LANES] = jnp.zeros((n_ep, LANES - 2 * R), F32)

    pl.semaphore_wait(barrier, n_ep - 1 + n_tp - 1)
    got_x = {k: ep_start(0, k, nrm.at[:, at(ep_peer(k), Dc)], x_all.at[at(e, R), :]) for k in ep_far}
    x_all[at(e, R), :] = nrm[:, at(e, Dc)]
    load_proj.wait()

    def proj_rows(tt):
        return wproj.at[at(tt, W), :]

    got_wp = spread_tp(0, proj_rows)

    gate_in = dot_t(nrm[...], win_ref[...])
    gate_fo = dot_t(nrm[...], wfo_ref[...]) + bias_ref[...]
    mine = iota(gate_in.shape, 1) == t
    g_in = jnp.sum(jnp.where(mine, gate_in, 0.0), axis=1, keepdims=True)
    g_fo = jnp.sum(jnp.where(mine, gate_fo, 0.0), axis=1, keepdims=True)
    eye = iota((R, R), 0) == iota((R, R), 1)
    smax = jnp.sum(jnp.where(eye, smax_ref[...], 0.0), axis=1, keepdims=True)
    log_keep = jnp.minimum(g_fo, 0.0) - jnp.log(1.0 + jnp.exp(-jnp.abs(g_fo)))
    carried = log_keep + smax
    new_max = jnp.maximum(carried, g_in)
    keep = jnp.exp(carried - new_max)
    write = jnp.exp(g_in - new_max)
    max_out_ref[...] = jnp.sum(jnp.where(eye, new_max, 0.0), axis=0, keepdims=True)

    for copy in load_w:
        copy.wait()
    got_part = {}
    for dy in [(EY - d) % EY for d in range(EY)]:
        back = (EY - dy) % EY
        for dx in range(EX):
            k = dy * EX + dx
            if k:
                got_x[k].wait_recv()
        rows = at(lax.rem(ey + back, EY), RC)
        part_send[rows, :] = dot(x_all[rows, :], wcat[...]).astype(BF16)
        for dx in dx_far:
            k = back * EX + dx
            if k:
                got_part[k] = ep_start(1, k, part_send.at[at(ep_peer(k), R), :], part_recv.at[k])
    got_info = {k: ep_start(2, k, info, info_recv.at[k]) for k in ep_far}

    @pl.when(raw_away)
    def _():
        raw_copy().start()

    @pl.when(jnp.logical_not(raw_away))
    def _():
        raw_blk[...] = tokens_ref[:, at(t, Dc)]

    proj = part_send[at(e, R), :].astype(F32)
    for k in reversed(ep_far):
        got_part[k].wait_recv()
        proj += part_recv[k].astype(F32)

    load_state.wait()
    q = proj[:, 0:W]
    key = proj[:, W : 2 * W] * W ** (-0.5)
    val = proj[:, 2 * W : 3 * W]
    og = proj[:, 3 * W : 4 * W]
    key_w = write * key
    new_norm = keep * norm_ref[...] + key_w
    q_t = q.T
    for b in range(R):
        numer[b : b + 1, :] = jnp.sum(q_t[:, b : b + 1] * state[b, 0], axis=0, keepdims=True)
    top = keep * numer[...] + jnp.sum(q * key_w, axis=1, keepdims=True) * val
    denom = jnp.sum(q * new_norm, axis=1, keepdims=True)
    cell = top / jnp.maximum(jnp.abs(denom), 1.0)
    mix_send[...] = (cell / (1.0 + jnp.exp(-og))).astype(BF16)

    def mix_copy(k):
        return pltpu.make_async_remote_copy(
            src_ref=mix_send,
            dst_ref=mix_all.at[:, at(t, W)],
            send_sem=send_mx.at[k],
            recv_sem=recv_mx.at[t],
            device_id={"ep": ep_peer(k), "tp": lax.rem(e + n_ep - ep_peer(k), n_ep)},
            device_id_type=MESH,
        )

    for k in ep_far:
        mix_copy(k).start()

    @pl.when(t != 0)
    def _():
        mix_copy(0).start()

    @pl.when(t == 0)
    def _():
        mix_all[:, at(t, W)] = mix_send[...]

    key_t = key_w.T
    for b in range(R):
        state[b, 0] = keep[b : b + 1, :] * state[b, 0] + key_t[:, b : b + 1] * val[b : b + 1, :]
    store_mat = load(state, mat_ref)
    gather_tp(0, proj_rows, got_wp)
    norm_out_ref[...] = new_norm

    for k in ep_far:
        got_info[k].wait_recv()
    quarter = iota((n_ep, LANES), 1) // R
    codes, sharesl = [], []

    info_recv[0] = info[...]
    for qq in range(Q):
        ctile = jnp.zeros((n_ep, LANES), F32)
        stile = jnp.zeros((n_ep, LANES), F32)
        for j in range(PER):
            g = qq * PER + j
            gy, gx = g // EX, g % EX
            slot_k = lax.rem(ey + (EY - gy), EY) * EX + lax.rem(ex + (EX - gx), EX)
            tile = info_recv[slot_k]
            there = quarter == j
            ctile += jnp.where(there, tile if j == 0 else pltpu.roll(tile, j * R, 1), 0.0)
            back = (j - 1) % PER * R
            stile += jnp.where(there, tile if back == 0 else pltpu.roll(tile, back, 1), 0.0)
        codes.append(ctile)
        sharesl.append(stile)
    code_all = jnp.concatenate(codes, axis=1) if Q > 1 else codes[0]
    share_all = jnp.concatenate(sharesl, axis=1) if Q > 1 else sharesl[0]
    row_no = (iota((S, N), 0) + 1).astype(F32)
    for p in range(n_ep):
        gmat[p * S : (p + 1) * S, :] = jnp.where(row_no == code_all[p : p + 1, :], 1.0, 0.0).astype(
            BF16
        )
    is_mine = iota((n_ep, N), 0) == e
    my_code = jnp.sum(jnp.where(is_mine, code_all, 0.0), axis=0, keepdims=True)
    my_share = jnp.sum(jnp.where(is_mine, share_all, 0.0), axis=0, keepdims=True)
    my_code8 = jnp.where(
        my_code > 0.0, my_code + ((PAD - CAP) * (iota((1, N), 1) // R)).astype(F32), 0.0
    )
    row_share = jnp.sum(
        jnp.where((iota((S8, N), 0) + 1).astype(F32) == my_code8, my_share, 0.0),
        axis=1,
        keepdims=True,
    )
    spread = jnp.where(
        jnp.logical_and(
            iota((S8, S), 0) // PAD * CAP + iota((S8, S), 0) % PAD == iota((S8, S), 1),
            iota((S8, S), 0) % PAD < CAP,
        ),
        1.0,
        0.0,
    ).astype(BF16)
    repeat = jnp.where(iota((S8, n_ep), 0) // PAD == iota((S8, n_ep), 1), 1.0, 0.0).astype(BF16)
    code_rep = dot(repeat, code.astype(BF16))
    pick_t = jnp.where((iota((S8, R), 0) % PAD + 1).astype(F32) == code_rep, 1.0, 0.0)
    pick = pick_t.T.astype(BF16)

    @pl.when(raw_away)
    def _():
        raw_copy().wait()

    for tt in range(n_tp):

        def arrive_mix(tt=tt):
            pltpu.make_async_remote_copy(
                src_ref=mix_send,
                dst_ref=mix_all.at[:, pl.ds(tt * W, W)],
                send_sem=send_mx.at[0],
                recv_sem=recv_mx.at[tt],
                device_id={"tp": sibling},
                device_id_type=MESH,
            ).wait_recv()

        if tt:
            arrive_mix()
        else:
            pl.when(t != 0)(arrive_mix)

    mine_res = raw_blk[...].astype(F32) + dot(mix_all[...], wproj[...])
    my_rows = at(mine_group, R)
    res_all[my_rows, :] = mine_res.astype(BF16)

    def res_rows(tt):
        return res_all.at[at(lax.rem(tt + e, n_ep), R), :]

    got_res = spread_tp(1, res_rows)

    def half_copy(c):
        return pltpu.make_async_remote_copy(
            src_ref=res_all.at[my_rows, pl.ds(c * HD, HD)],
            dst_ref=res_t.at[:, at(lax.rem(e, 2), HD)],
            send_sem=send_tr.at[1 + c],
            recv_sem=recv_tr.at[1 + lax.rem(e, 2)],
            device_id={"ep": mine_group, "tp": e // 2 * 2 + c},
            device_id_type=MESH,
        )

    stays = jnp.logical_and(t == 0, e < 2)

    @pl.when(jnp.logical_not(stays))
    def _():
        half_copy(0).start()

    @pl.when(stays)
    def _():
        res_t[:, at(lax.rem(e, 2), HD)] = res_all[my_rows, 0:HD]

    half_copy(1).start()

    load_dg.wait()
    load_du.wait()
    my_fgain = fgain_ref[:, at(e, Dc)]

    def stage_a(g):
        gy, gx = g // EX, lax.rem(g, EX)
        dx = lax.rem(gx + EX - ex, EX)
        return pltpu.make_async_remote_copy(
            src_ref=dense_send.at[at(g, R), pl.ds(0, F)],
            dst_ref=da_recv.at[dx, gy],
            send_sem=send_a.at[g],
            recv_sem=recv_a.at[dx * EY + gy],
            device_id={"ep": ey * EX + gx},
            device_id_type=MESH,
        )

    def stage_b(g):
        gy, gx = g // EX, lax.rem(g, EX)
        dy = lax.rem(gy + EY - ey, EY)
        return pltpu.make_async_remote_copy(
            src_ref=dense_send.at[at(g, R), pl.ds(F, F)],
            dst_ref=db_recv.at[dy, gx],
            send_sem=send_b.at[g],
            recv_sem=recv_b.at[dy * EX + gx],
            device_id={"ep": gy * EX + ex},
            device_id_type=MESH,
        )

    def dense_part(tt):
        g = lax.rem(tt + e, n_ep)
        rows = at(g, R)
        xg[rows, :] = (res_all[rows, :].astype(F32) * my_fgain).astype(BF16)
        dense_send[rows, :] = dot(xg[rows, :], dgu[...]).astype(BF16)

        @pl.when(lax.rem(g, EX) != ex)
        def _():
            stage_a(g).start()

        @pl.when(g // EX != ey)
        def _():
            stage_b(g).start()

    dense_part(t)
    got_res[0].wait_recv()
    dense_part(sibling)
    late = None
    for dz in reversed(dz_far):
        got_res[dz].wait_recv()
        there = lax.rem(tz + TZ - dz, TZ) * 2
        odd = 2 * dz + 1
        passing = side_start(
            send_tp.at[1, odd], recv_tp.at[1, odd], res_rows(there + tc), res_rows(there + tc)
        )
        dense_part(there + tc)
        if late is not None:
            late[0].wait_recv()
            dense_part(late[1])
        late = (passing, there + 1 - tc)
    late[0].wait_recv()
    dense_part(late[1])

    wide_branch = branch_ref[...].astype(F32)
    pieces = Dc // LANES
    branch_rows = [
        jnp.sum(
            jnp.where(iota(wide_branch.shape, 0) == e * pieces + i, wide_branch, 0.0),
            axis=0,
            keepdims=True,
        )
        for i in range(pieces)
    ]
    my_branch = jnp.concatenate(branch_rows, axis=1) if pieces > 1 else branch_rows[0]
    my_branch = jnp.broadcast_to(my_branch, (8, Dc)).astype(BF16)
    ones = jnp.ones((8, Dc), BF16)
    block = res_all[...].astype(F32)
    square = block * block
    high = square.astype(BF16)
    low = (square - high.astype(F32)).astype(BF16)
    sums = dot_t(ones, high) + dot_t(ones, low)
    branch = dot_t(my_branch, xg[...])
    row8 = iota((8, LANES), 0)
    tile = jnp.zeros((8, LANES), F32)
    for qq in range(Q):
        cols = slice(qq * LANES, (qq + 1) * LANES)
        tile += jnp.where(row8 == qq, sums[:, cols], 0.0)
        tile += jnp.where(row8 == 4 + qq, branch[:, cols], 0.0)
    stat[...] = tile
    got_stat = {k: ep_start(3, k, stat, stat_recv.at[k]) for k in ep_far}

    got_disp = {}

    def dispatch(dy):
        rows = at(lax.rem(ey + dy, EY), S * EX)
        disp_send[rows, :] = dot(gmat[rows, :], xg[:, at(tc, HD)]).astype(BF16)
        for dx in dx_far:
            k = dy * EX + dx
            if k:
                got_disp[k] = ep_start(
                    5, k, disp_send.at[at(ep_peer(k), S), :], xrecv.at[:, at(2 * e + tc, HD)]
                )

    for dy in dy_far:
        dispatch(dy)

    got_a, got_b = {}, {}
    for d in dy_far:
        gy = lax.rem(ey + d, EY)
        term = dense_send[at(gy * EX + ex, R), 0:F].astype(F32)
        for dx in range(1, EX):
            pltpu.make_async_remote_copy(
                src_ref=dense_send.at[pl.ds(0, R), pl.ds(0, F)],
                dst_ref=da_recv.at[dx, gy],
                send_sem=send_a.at[0],
                recv_sem=recv_a.at[dx * EY + gy],
                device_id={"ep": e},
                device_id_type=MESH,
            ).wait_recv()
            term += da_recv[dx, gy].astype(F32)
        if d:
            a2_send[d] = term.astype(BF16)
            got_a[d] = ep_start(4, d * EX, a2_send.at[d], a2_recv.at[d])
        else:
            g = term
    for d in dx_far:
        gx = lax.rem(ex + d, EX)
        term = dense_send[at(ey * EX + gx, R), F : 2 * F].astype(F32)
        for dy in range(1, EY):
            pltpu.make_async_remote_copy(
                src_ref=dense_send.at[pl.ds(0, R), pl.ds(F, F)],
                dst_ref=db_recv.at[dy, gx],
                send_sem=send_b.at[0],
                recv_sem=recv_b.at[dy * EX + gx],
                device_id={"ep": e},
                device_id_type=MESH,
            ).wait_recv()
            term += db_recv[dy, gx].astype(F32)
        if d:
            b2_send[d] = term.astype(BF16)
            got_b[d] = ep_start(4, d, b2_send.at[d], b2_recv.at[d])
        else:
            u = term

    xrecv[:, at(2 * e + tc, HD)] = disp_send[at(e, S), :]

    def forward(k):
        region = xrecv.at[:, at(2 * ep_from(k) + tc, HD)]
        return side_start(send_fw.at[k], recv_fw.at[k], region, region)

    passed = [forward(0)]

    for k in reversed(ep_far):
        got_stat[k].wait_recv()
        tile += stat_recv[k]
    scale_l = lax.rsqrt(tile[0:Q, :] * (1.0 / D) + EPS)
    share_l = 1.0 / (1.0 + jnp.exp(-(scale_l * tile[4 : 4 + Q, :])))
    my_scale = jnp.zeros((R, 1), F32)
    my_bshare = jnp.zeros((R, 1), F32)
    for qq in range(Q):
        here = iota((R, LANES), 1) + qq * LANES == iota((R, LANES), 0) + e * R
        my_scale += jnp.sum(jnp.where(here, scale_l[qq : qq + 1, :], 0.0), axis=1, keepdims=True)
        my_bshare += jnp.sum(jnp.where(here, share_l[qq : qq + 1, :], 0.0), axis=1, keepdims=True)
    scale_row = (
        jnp.concatenate([scale_l[qq : qq + 1, :] for qq in range(Q)], axis=1) if Q > 1 else scale_l
    )
    row_scale = jnp.sum(jnp.where(row_no == my_code, scale_row, 0.0), axis=1, keepdims=True)

    for d in reversed(dy_far):
        if d:
            got_a[d].wait_recv()
            g += a2_recv[d].astype(F32)
    for d in reversed(dx_far):
        if d:
            got_b[d].wait_recv()
            u += b2_recv[d].astype(F32)
    g, u = g * my_scale, u * my_scale
    hid_all[at(e, R), :] = (g / (1.0 + jnp.exp(-g)) * u).astype(BF16)
    got_hid = {
        k: ep_start(6, k, hid_all.at[at(e, R), :], hid_all.at[at(e, R), :]) for k in ep_far
    }

    load_eg.wait()
    load_eu.wait()
    for k in reversed(ep_far):
        got_disp[k].wait_recv()
        passed.append(forward(k))
    for copy in passed:
        copy.wait_recv()
    gp = dot(xrecv[...], eg[0]) * row_scale
    up = dot(xrecv[...], eu[0]) * row_scale
    ehid = (gp / (1.0 + jnp.exp(-gp)) * up).astype(BF16)
    ehid8 = dot(spread, ehid).astype(BF16)
    for copy in load_ed:
        copy.wait()
    step = min(512, DH)
    strips = [slice(c * step, (c + 1) * step) for c in range(DH // step)]
    got_yo = []
    for i, cols in enumerate(strips):
        yo_send[:, cols] = (dot(ehid8, edc[0, :, cols]) * row_share).astype(BF16)
        got_yo.append(
            side_start(send_sb.at[i], recv_sb.at[i], yo_send.at[:, cols], yo_recv.at[:, cols])
        )
    got_fin = {}
    wide = DH // 2
    per_strip = max(1, wide // step)
    for i, (copy, cols) in enumerate(zip(got_yo, strips)):
        y = dot(ehid8, edc[1, :, cols]) * row_share
        copy.wait_recv()
        y += yo_recv[:, cols].astype(F32)
        fin_send[:, :, cols] = y.reshape(n_ep, PAD, step).astype(BF16)
        if i % per_strip == per_strip - 1:
            j = i // per_strip
            part = pl.ds(j * per_strip * step, per_strip * step)
            for k in ep_far:
                got_fin[j, k] = ep_start(
                    7 + j,
                    k,
                    fin_send.at[ep_peer(k), pl.ds(0, CAP), part],
                    fin_recv.at[e, pl.ds(0, CAP), part],
                )
    fin_recv[e] = fin_send[e]

    load_dd.wait()
    got_no = {}
    for dy in reversed(dy_far):
        for dx in range(EX):
            k = (EY - dy) % EY * EX + dx
            if k:
                got_hid[k].wait_recv()
        rows = at(lax.rem(ey + dy, EY), RC)
        dno_send[rows, :] = dot(hid_all[rows, :], dd[:, at(1 - tc, HD)]).astype(BF16)
        got_no[dy] = side_start(
            send_sb.at[4 + dy], recv_sb.at[4 + dy], dno_send.at[rows, :], dno_recv.at[rows, :]
        )
    got_dn = {}
    for dy in reversed(dy_far):
        rows = at(lax.rem(ey + dy, EY), RC)
        down = dot(hid_all[rows, :], dd[:, at(tc, HD)])
        got_no[dy].wait_recv()
        dn_send[rows, :] = (down + dno_recv[rows, :].astype(F32)).astype(BF16)
        for dx in dx_far:
            k = dy * EX + dx
            if k:
                got_dn[k] = ep_start(
                    9, k, dn_send.at[at(ep_peer(k), R), :], dn_recv.at[:, at(e, HD)]
                )
    dn_recv[:, at(e, HD)] = dn_send[at(e, R), :]

    for copy in got_fin.values():
        copy.wait_recv()
    for z in range(TZ):
        cols = slice(z * Dc, (z + 1) * Dc)
        back = fin_recv[:, :, cols].astype(F32).reshape(S8, Dc).astype(BF16)
        comb[:, cols] = dot(pick, back)
    for k in reversed(ep_far):
        got_dn[k].wait_recv()
    got_tp = {}
    for dz in dz_far + [0]:
        cols = at(lax.rem(tz + dz, TZ), Dc)
        piece = comb[:, cols] + my_bshare * dn_recv[:, cols].astype(F32)
        tp_send[:, cols] = piece.astype(BF16)
        if dz:
            got_tp[dz] = tp_start(2, 2 * dz, tp_send.at[:, cols], tp_recv.at[dz])

    for i in range(2):

        @pl.when(jnp.logical_not(jnp.logical_and(t == 0, e == i)))
        def _():
            pltpu.make_async_remote_copy(
                src_ref=res_all.at[pl.ds(0, R), pl.ds(0, HD)],
                dst_ref=res_t.at[:, pl.ds(i * HD, HD)],
                send_sem=send_tr.at[1 + i],
                recv_sem=recv_tr.at[1 + i],
                device_id={"tp": sibling},
                device_id_type=MESH,
            ).wait_recv()

    last = res_t[...].astype(F32) + tp_send[:, at(tz, Dc)].astype(F32)
    for dz in reversed(dz_far):
        got_tp[dz].wait_recv()
        last += tp_recv[dz].astype(F32)
    out_all[:, at(tc * TZ + tz, Dc)] = last.astype(BF16)

    def out_cols(tt):
        return out_all.at[:, at(lax.rem(tt, 2) * TZ + tt // 2, Dc)]

    got_out = spread_tp(3, out_cols)
    for k in ep_far:
        mix_copy(k).wait_send()

    @pl.when(t != 0)
    def _():
        mix_copy(0).wait_send()

    @pl.when(jnp.logical_not(stays))
    def _():
        half_copy(0).wait_send()

    half_copy(1).wait_send()
    for g in range(n_ep):

        @pl.when(g % EX != ex)
        def _():
            stage_a(g).wait_send()

        @pl.when(g // EX != ey)
        def _():
            stage_b(g).wait_send()

    gather_tp(3, out_cols, got_out)
    for b in range(n_ep):
        for c in range(2):
            out_ref[:, pl.ds((2 * b + c) * HD, HD)] = out_all[:, pl.ds(c * DH + b * HD, HD)]
    for copy in pending:
        copy.wait_send()
    store_mat.wait()


def store_kernel(chunks, *refs):
    bufs, sems = refs[8:12], refs[12]
    rows = refs[3].shape[0] // chunks
    moves = [(refs[i], bufs[i], refs[4 + i]) for i in range(3)]
    for c in range(chunks):
        part = pl.ds(c * rows, rows)
        moves.append((refs[3].at[part], bufs[3].at[part], refs[7].at[part]))
    inward = [pltpu.make_async_copy(m[0], m[1], sems.at[0, i]) for i, m in enumerate(moves)]
    outward = [pltpu.make_async_copy(m[1], m[2], sems.at[1, i]) for i, m in enumerate(moves)]
    for copy in inward:
        copy.start()
    for came, goes in zip(inward, outward):
        came.wait()
        goes.start()
    for copy in outward:
        copy.wait()


def on_device(
    n_ep,
    n_tp,
    tokens,
    state_matrix,
    state_norm,
    state_max,
    mixer_gain,
    w_query,
    w_key,
    w_value,
    w_outgate,
    w_ingate,
    w_forget,
    forget_bias,
    w_proj,
    ffn_gain,
    w_branch,
    routes,
    route_weight,
    expert_gate,
    expert_up,
    expert_down,
    dense_gate,
    dense_up,
    dense_down,
):
    R, D = tokens.shape
    hd = state_norm.shape[2]
    N, Dc, DH, W = R * n_ep, D // n_ep, D // 2, hd
    F = dense_gate.shape[1]
    FE = expert_gate.shape[2]
    S, S8 = CAP * n_ep, PAD * n_ep
    EX = {16: 4, 4: 2}[n_ep]
    EY = n_ep // EX
    vmem = pl.BlockSpec(memory_space=pltpu.VMEM)
    hbm = pl.BlockSpec(memory_space=pltpu.HBM)
    V = pltpu.VMEM
    scratch = [
        V(state_matrix.shape, F32),
        V((Dc, 4 * W), BF16),
        V((n_tp * W, Dc), BF16),
        V(expert_gate.shape, BF16),
        V(expert_up.shape, BF16),
        V((2, FE, DH), BF16),
        V((Dc, 2 * F), BF16),
        V(dense_down.shape, BF16),
        V((R, D), BF16),
        V((N, Dc), BF16),
        V((n_ep, LANES), F32),
        V((n_ep, n_ep, LANES), F32),
        V((N, 4 * W), BF16),
        V((n_ep, R, 4 * W), BF16),
        V((R, W), F32),
        V((R, W), BF16),
        V((R, n_tp * W), BF16),
        V((R, Dc), BF16),
        V((N, Dc), BF16),
        V((R, Dc), BF16),
        V((N, Dc), BF16),
        V((n_ep * S, N), BF16),
        V((8, LANES), F32),
        V((n_ep, 8, LANES), F32),
        V((N, 2 * F), BF16),
        V((EX, EY, R, F), BF16),
        V((EY, EX, R, F), BF16),
        V((EY, R, F), BF16),
        V((EY, R, F), BF16),
        V((EX, R, F), BF16),
        V((EX, R, F), BF16),
        V((n_ep * S, Dc // 2), BF16),
        V((S, D), BF16),
        V((N, F), BF16),
        V((S8, DH), BF16),
        V((S8, DH), BF16),
        V((n_ep, PAD, DH), BF16),
        V((n_ep, PAD, DH), BF16),
        V((N, Dc // 2), BF16),
        V((N, Dc // 2), BF16),
        V((N, Dc // 2), BF16),
        V((R, DH), BF16),
        V((R, DH), F32),
        V((R, DH), BF16),
        V((n_tp // 2, R, Dc), BF16),
        V((R, D), BF16),
        pltpu.SemaphoreType.DMA((12 + 2 * n_ep,)),
        pltpu.SemaphoreType.DMA((10, n_ep)),
        pltpu.SemaphoreType.DMA((10, n_ep)),
        pltpu.SemaphoreType.DMA((4, n_tp)),
        pltpu.SemaphoreType.DMA((4, n_tp)),
        pltpu.SemaphoreType.DMA((n_ep,)),
        pltpu.SemaphoreType.DMA((n_tp,)),
        pltpu.SemaphoreType.DMA((3,)),
        pltpu.SemaphoreType.DMA((3,)),
        pltpu.SemaphoreType.DMA((n_ep,)),
        pltpu.SemaphoreType.DMA((n_ep,)),
        pltpu.SemaphoreType.DMA((8,)),
        pltpu.SemaphoreType.DMA((8,)),
        pltpu.SemaphoreType.DMA((n_ep,)),
        pltpu.SemaphoreType.DMA((n_ep,)),
        pltpu.SemaphoreType.DMA((n_ep,)),
        pltpu.SemaphoreType.DMA((n_ep,)),
    ]
    Sh = jax.ShapeDtypeStruct
    results = pl.pallas_call(
        functools.partial(layer_kernel, n_ep, n_tp),
        out_shape=(
            Sh((R, D), BF16),
            Sh((R, hd), F32),
            Sh((1, R), F32),
            Sh(state_matrix.shape, F32),
        ),
        in_specs=[vmem] * 11 + [hbm] * 12,
        out_specs=(vmem,) * 3 + (hbm,),
        scratch_shapes=scratch,
        compiler_params=pltpu.CompilerParams(
            collective_id=0, has_side_effects=True, vmem_limit_bytes=66_000_000
        ),
    )(
        tokens,
        mixer_gain[None, :],
        w_ingate.T,
        w_forget.T,
        forget_bias[None, :],
        state_norm.reshape(R, hd),
        state_max.T,
        ffn_gain[None, :],
        w_branch.reshape(-1, LANES),
        routes.T,
        route_weight.T,
        state_matrix,
        w_query,
        w_key,
        w_value,
        w_outgate,
        w_proj,
        expert_gate,
        expert_up,
        expert_down,
        dense_gate,
        dense_up,
        dense_down,
    )
    layer_out, new_norm, new_max, new_matrix = pl.pallas_call(
        functools.partial(store_kernel, 8),
        out_shape=tuple(Sh(r.shape, r.dtype) for r in results),
        in_specs=[hbm] * 4,
        out_specs=(hbm,) * 4,
        scratch_shapes=[V(r.shape, r.dtype) for r in results] + [pltpu.SemaphoreType.DMA((2, 11))],
        compiler_params=pltpu.CompilerParams(vmem_limit_bytes=66_000_000),
    )(*results)
    return (layer_out, new_matrix, new_norm.reshape(R, 1, hd), new_max.T)


def solution(mesh):
    in_specs = (
        P("ep", None),
        P("ep", "tp", None, None),
        P("ep", "tp", None),
        P("ep", "tp"),
        P(),
        P("ep", "tp"),
        P("ep", "tp"),
        P("ep", "tp"),
        P("ep", "tp"),
        P(),
        P(),
        P(),
        P("tp", "ep"),
        P(),
        P(),
        P("ep", None),
        P("ep", None),
        P("ep", None, "tp"),
        P("ep", None, "tp"),
        P("ep", "tp", None),
        P("ep", "tp"),
        P("ep", "tp"),
        P("tp", "ep"),
    )
    out_specs = (P("ep", None), P("ep", "tp", None, None), P("ep", "tp", None), P("ep", "tp"))
    return jax.shard_map(
        functools.partial(on_device, mesh.shape["ep"], mesh.shape["tp"]),
        mesh=mesh,
        in_specs=in_specs,
        out_specs=out_specs,
        check_vma=False,
    )
```

```python
import functools

import jax
import jax.numpy as jnp
from jax import lax
from jax.experimental import pallas as pl
from jax.experimental.pallas import tpu as pltpu
from jax.sharding import PartitionSpec as P

EPS = 1e-06
LANES = 128
CAP = 6
PAD = 8
F32 = jnp.float32
BF16 = jnp.bfloat16
MESH = pl.DeviceIdType.MESH


def dot(a, b):
    return jnp.dot(a, b, preferred_element_type=F32)


def dot_t(a, b):
    return lax.dot_general(a, b, (((1,), (1,)), ((), ())), preferred_element_type=F32)


def iota(shape, dim):
    return lax.broadcasted_iota(jnp.int32, shape, dim)


def layer_kernel(
    n_ep,
    n_tp,
    tokens_ref,
    gain_ref,
    win_ref,
    wfo_ref,
    bias_ref,
    norm_ref,
    smax_ref,
    fgain_ref,
    branch_ref,
    routes_ref,
    weight_ref,
    state_hbm,
    wq_hbm,
    wk_hbm,
    wv_hbm,
    wo_hbm,
    wproj_hbm,
    eg_hbm,
    eu_hbm,
    ed_hbm,
    dg_hbm,
    du_hbm,
    dd_hbm,
    out_ref,
    norm_out_ref,
    max_out_ref,
    mat_ref,
    state,
    wcat,
    wproj,
    eg,
    eu,
    edc,
    dgu,
    dd,
    nrm,
    x_all,
    info,
    info_recv,
    part_send,
    part_recv,
    numer,
    mix_send,
    mix_all,
    raw_blk,
    res_all,
    res_t,
    xg,
    gmat,
    stat,
    stat_recv,
    dense_send,
    da_recv,
    db_recv,
    a2_send,
    a2_recv,
    b2_send,
    b2_recv,
    disp_send,
    xrecv,
    hid_all,
    yo_send,
    yo_recv,
    fin_send,
    fin_recv,
    dno_send,
    dno_recv,
    dn_send,
    dn_recv,
    comb,
    tp_send,
    tp_recv,
    out_all,
    load_sems,
    send_ep,
    recv_ep,
    send_tp,
    recv_tp,
    send_mx,
    recv_mx,
    send_tr,
    recv_tr,
    send_fw,
    recv_fw,
    send_sb,
    recv_sb,
    send_a,
    recv_a,
    send_b,
    recv_b,
):
    e = lax.axis_index("ep")
    t = lax.axis_index("tp")
    R, D = tokens_ref.shape
    N = R * n_ep
    Dc = D // n_ep
    HD = Dc // 2
    DH = D // 2
    W = mix_send.shape[1]
    F = dd.shape[0]
    EX = {16: 4, 4: 2}[n_ep]
    EY = n_ep // EX
    TZ = n_tp // 2
    S = CAP * n_ep
    S8 = PAD * n_ep
    Q = N // LANES
    PER = LANES // R
    RC = R * EX
    ey, ex = e // EX, lax.rem(e, EX)
    mine_group = lax.rem(t + e, n_ep)
    tz, tc = t // 2, lax.rem(t, 2)

    def at(index, size):
        return pl.ds(pl.multiple_of(index * size, size), size)

    def ring(d, n):
        return min(d, n - d)

    ep_far = sorted(range(1, n_ep), key=lambda k: -(ring(k // EX, EY) + ring(k % EX, EX)))
    dz_far = sorted(range(1, TZ), key=lambda d: -ring(d, TZ))
    dy_far = sorted(range(EY), key=lambda d: -ring(d, EY))
    dx_far = sorted(range(EX), key=lambda d: -ring(d, EX))

    def ep_peer(k):
        return lax.rem(ey + k // EX, EY) * EX + lax.rem(ex + k % EX, EX)

    def ep_from(k):
        return lax.rem(ey + EY - k // EX, EY) * EX + lax.rem(ex + EX - k % EX, EX)

    def tp_peer(k):
        return lax.rem(tz + k // 2, TZ) * 2 + lax.rem(tc + k % 2, 2)

    sibling = tz * 2 + 1 - tc

    loads = []

    def load(src, dst):
        copy = pltpu.make_async_copy(src, dst, load_sems.at[len(loads)])
        copy.start()
        loads.append(copy)
        return copy

    pending = []
    scopes = []

    def phase(name):
        if scopes:
            scopes.pop().__exit__(None, None, None)
        if name:
            scopes.append(jax.named_scope(name))
            scopes[0].__enter__()

    def ep_start(phase, k, src, dst):
        copy = pltpu.make_async_remote_copy(
            src_ref=src,
            dst_ref=dst,
            send_sem=send_ep.at[phase, k],
            recv_sem=recv_ep.at[phase, k],
            device_id={"ep": ep_peer(k)},
            device_id_type=MESH,
        )
        copy.start()
        pending.append(copy)
        return copy

    def tp_start(phase, k, src, dst, to=None):
        copy = pltpu.make_async_remote_copy(
            src_ref=src,
            dst_ref=dst,
            send_sem=send_tp.at[phase, k],
            recv_sem=recv_tp.at[phase, k],
            device_id={"tp": tp_peer(k if to is None else to)},
            device_id_type=MESH,
        )
        copy.start()
        pending.append(copy)
        return copy

    def side_start(send_sem, recv_sem, src, dst):
        copy = pltpu.make_async_remote_copy(
            src_ref=src,
            dst_ref=dst,
            send_sem=send_sem,
            recv_sem=recv_sem,
            device_id={"tp": sibling},
            device_id_type=MESH,
        )
        copy.start()
        pending.append(copy)
        return copy

    def spread_tp(phase, region, order):
        copies = {0: tp_start(phase, 1, region(t), region(t))}
        for dz in order:
            copies[dz] = tp_start(phase, 2 * dz, region(t), region(t))
        return copies

    def gather_tp(phase, region, copies, here=()):
        passed = []
        for dz in reversed(dz_far):
            if dz not in here:
                copies[dz].wait_recv()
            source = lax.rem(tz + TZ - dz, TZ) * 2 + tc
            odd = 2 * dz + 1
            passed.append(
                side_start(
                    send_tp.at[phase, odd], recv_tp.at[phase, odd], region(source), region(source)
                )
            )
        copies[0].wait_recv()
        for copy in passed:
            copy.wait_recv()

    def raw_copy():
        return pltpu.make_async_remote_copy(
            src_ref=tokens_ref.at[:, at(t, Dc)],
            dst_ref=raw_blk,
            send_sem=send_tr.at[0],
            recv_sem=recv_tr.at[0],
            device_id={"ep": t, "tp": lax.rem(e + n_ep - t, n_ep)},
            device_id_type=MESH,
        )

    raw_away = jnp.logical_or(e != 0, t != 0)
    fin_recv[...] = jnp.zeros_like(fin_recv)

    phase('greet')
    barrier = pltpu.get_barrier_semaphore()
    for k in ep_far:
        pl.semaphore_signal(barrier, inc=1, device_id={"ep": ep_peer(k)}, device_id_type=MESH)
    for k in range(1, n_tp):
        pl.semaphore_signal(barrier, inc=1, device_id={"tp": tp_peer(k)}, device_id_type=MESH)

    load_w = [
        load(src, wcat.at[:, pl.ds(i * W, W)])
        for i, src in enumerate((wq_hbm, wk_hbm, wv_hbm, wo_hbm))
    ]
    load_proj = load(wproj_hbm, wproj.at[at(t, W), :])
    load_state = load(state_hbm, state)
    load_dg, load_du = load(dg_hbm, dgu.at[:, pl.ds(0, F)]), load(du_hbm, dgu.at[:, pl.ds(F, F)])
    load_eg, load_eu = load(eg_hbm, eg), load(eu_hbm, eu)
    load_ed = [
        load(ed_hbm.at[0, :, at(2 * b + side, HD)], edc.at[i, :, pl.ds(b * HD, HD)])
        for i, side in enumerate((1 - tc, tc))
        for b in range(n_ep)
    ]
    load_dd = load(dd_hbm, dd)

    wide = tokens_ref[...].astype(F32)
    scale = lax.rsqrt(jnp.mean(wide * wide, axis=-1, keepdims=True) + EPS)
    nrm[...] = (wide * scale * gain_ref[...]).astype(BF16)

    r0, r1 = routes_ref[0:1, :], routes_ref[1:2, :]
    w0, w1 = weight_ref[0:1, :], weight_ref[1:2, :]
    total = w0 + w1
    which = iota((n_ep, R), 0)
    hit0, hit1 = which == r0, which == r1
    named = jnp.where(jnp.logical_or(hit0, hit1), 1.0, 0.0)
    earlier = jnp.where(iota((R, R), 0) < iota((R, R), 1), 1.0, 0.0).astype(BF16)
    slot = dot(named.astype(BF16), earlier)
    code = jnp.where(named > 0.0, slot + 1.0, 0.0)
    group_at = (e * CAP).astype(F32)
    rowcode = jnp.where(named > 0.0, slot + (1.0 + group_at), 0.0)
    shares = jnp.where(hit0, w0 / total, 0.0) + jnp.where(hit1, w1 / total, 0.0)
    info[:, 0:R] = rowcode
    info[:, R : 2 * R] = shares
    info[:, 2 * R : LANES] = jnp.zeros((n_ep, LANES - 2 * R), F32)

    phase('greeted')
    pl.semaphore_wait(barrier, n_ep - 1 + n_tp - 1)
    phase('send_x')
    got_x = {k: ep_start(0, k, nrm.at[:, at(ep_peer(k), Dc)], x_all.at[at(e, R), :]) for k in ep_far}
    x_all[at(e, R), :] = nrm[:, at(e, Dc)]
    load_proj.wait()

    def proj_rows(tt):
        return wproj.at[at(tt, W), :]

    relays = {2: (1, 2), 6: (7,)} if TZ == 8 else {}
    direct = [dz for dz in dz_far if TZ != 8 or ring(dz, TZ) <= 2]
    got_wp = spread_tp(0, proj_rows, direct)

    phase('gates')
    gate_in = dot_t(nrm[...], win_ref[...])
    gate_fo = dot_t(nrm[...], wfo_ref[...]) + bias_ref[...]
    mine = iota(gate_in.shape, 1) == t
    g_in = jnp.sum(jnp.where(mine, gate_in, 0.0), axis=1, keepdims=True)
    g_fo = jnp.sum(jnp.where(mine, gate_fo, 0.0), axis=1, keepdims=True)
    eye = iota((R, R), 0) == iota((R, R), 1)
    smax = jnp.sum(jnp.where(eye, smax_ref[...], 0.0), axis=1, keepdims=True)
    log_keep = jnp.minimum(g_fo, 0.0) - jnp.log(1.0 + jnp.exp(-jnp.abs(g_fo)))
    carried = log_keep + smax
    new_max = jnp.maximum(carried, g_in)
    keep = jnp.exp(carried - new_max)
    write = jnp.exp(g_in - new_max)
    max_out_ref[...] = jnp.sum(jnp.where(eye, new_max, 0.0), axis=0, keepdims=True)

    phase('project')
    for copy in load_w:
        copy.wait()
    got_part = {}
    for dy in [(EY - d) % EY for d in range(EY)]:
        back = (EY - dy) % EY
        for dx in range(EX):
            k = dy * EX + dx
            if k:
                got_x[k].wait_recv()
        rows = at(lax.rem(ey + back, EY), RC)
        part_send[rows, :] = dot(x_all[rows, :], wcat[...]).astype(BF16)
        for dx in dx_far:
            k = back * EX + dx
            if k:
                got_part[k] = ep_start(1, k, part_send.at[at(ep_peer(k), R), :], part_recv.at[k])
    for first, onward in relays.items():
        got_wp[first].wait_recv()
        block = proj_rows(lax.rem(tz + TZ - first, TZ) * 2 + tc)
        for then in onward:
            dz = (first + then) % TZ
            got_wp[dz] = tp_start(0, 2 * dz, block, block, 2 * then)
    phase('send_info')
    got_info = {k: ep_start(2, k, info, info_recv.at[k]) for k in ep_far}

    @pl.when(raw_away)
    def _():
        raw_copy().start()

    @pl.when(jnp.logical_not(raw_away))
    def _():
        raw_blk[...] = tokens_ref[:, at(t, Dc)]

    phase('sum_parts')
    proj = part_send[at(e, R), :].astype(F32)
    for k in reversed(ep_far):
        got_part[k].wait_recv()
        proj += part_recv[k].astype(F32)

    phase('cell')
    load_state.wait()
    q = proj[:, 0:W]
    key = proj[:, W : 2 * W] * W ** (-0.5)
    val = proj[:, 2 * W : 3 * W]
    og = proj[:, 3 * W : 4 * W]
    key_w = write * key
    new_norm = keep * norm_ref[...] + key_w
    q_t = q.T
    for b in range(R):
        numer[b : b + 1, :] = jnp.sum(q_t[:, b : b + 1] * state[b, 0], axis=0, keepdims=True)
    top = keep * numer[...] + jnp.sum(q * key_w, axis=1, keepdims=True) * val
    denom = jnp.sum(q * new_norm, axis=1, keepdims=True)
    cell = top / jnp.maximum(jnp.abs(denom), 1.0)
    mix_send[...] = (cell / (1.0 + jnp.exp(-og))).astype(BF16)

    phase('send_cell')
    def mix_copy(k):
        return pltpu.make_async_remote_copy(
            src_ref=mix_send,
            dst_ref=mix_all.at[:, at(t, W)],
            send_sem=send_mx.at[k],
            recv_sem=recv_mx.at[t],
            device_id={"ep": ep_peer(k), "tp": lax.rem(e + n_ep - ep_peer(k), n_ep)},
            device_id_type=MESH,
        )

    for k in ep_far:
        mix_copy(k).start()

    @pl.when(t != 0)
    def _():
        mix_copy(0).start()

    @pl.when(t == 0)
    def _():
        mix_all[:, at(t, W)] = mix_send[...]

    key_t = key_w.T
    for b in range(R):
        state[b, 0] = keep[b : b + 1, :] * state[b, 0] + key_t[:, b : b + 1] * val[b : b + 1, :]
    store_mat = load(state, mat_ref)
    phase('pass_proj')
    gather_tp(0, proj_rows, got_wp, relays)
    phase('info')
    norm_out_ref[...] = new_norm

    for k in ep_far:
        got_info[k].wait_recv()
    phase('maps')
    quarter = iota((n_ep, LANES), 1) // R
    codes, sharesl = [], []

    info_recv[0] = info[...]
    for qq in range(Q):
        ctile = jnp.zeros((n_ep, LANES), F32)
        stile = jnp.zeros((n_ep, LANES), F32)
        for j in range(PER):
            g = qq * PER + j
            gy, gx = g // EX, g % EX
            slot_k = lax.rem(ey + (EY - gy), EY) * EX + lax.rem(ex + (EX - gx), EX)
            tile = info_recv[slot_k]
            there = quarter == j
            ctile += jnp.where(there, tile if j == 0 else pltpu.roll(tile, j * R, 1), 0.0)
            back = (j - 1) % PER * R
            stile += jnp.where(there, tile if back == 0 else pltpu.roll(tile, back, 1), 0.0)
        codes.append(ctile)
        sharesl.append(stile)
    code_all = jnp.concatenate(codes, axis=1) if Q > 1 else codes[0]
    share_all = jnp.concatenate(sharesl, axis=1) if Q > 1 else sharesl[0]
    row_no = (iota((S, N), 0) + 1).astype(F32)
    for p in range(n_ep):
        gmat[p * S : (p + 1) * S, :] = jnp.where(row_no == code_all[p : p + 1, :], 1.0, 0.0).astype(
            BF16
        )
    is_mine = iota((n_ep, N), 0) == e
    my_code = jnp.sum(jnp.where(is_mine, code_all, 0.0), axis=0, keepdims=True)
    my_share = jnp.sum(jnp.where(is_mine, share_all, 0.0), axis=0, keepdims=True)
    my_code8 = jnp.where(
        my_code > 0.0, my_code + ((PAD - CAP) * (iota((1, N), 1) // R)).astype(F32), 0.0
    )
    row_share = jnp.sum(
        jnp.where((iota((S8, N), 0) + 1).astype(F32) == my_code8, my_share, 0.0),
        axis=1,
        keepdims=True,
    )
    spread = jnp.where(
        jnp.logical_and(
            iota((S8, S), 0) // PAD * CAP + iota((S8, S), 0) % PAD == iota((S8, S), 1),
            iota((S8, S), 0) % PAD < CAP,
        ),
        1.0,
        0.0,
    ).astype(BF16)
    repeat = jnp.where(iota((S8, n_ep), 0) // PAD == iota((S8, n_ep), 1), 1.0, 0.0).astype(BF16)
    code_rep = dot(repeat, code.astype(BF16))
    pick_t = jnp.where((iota((S8, R), 0) % PAD + 1).astype(F32) == code_rep, 1.0, 0.0)
    pick = pick_t.T.astype(BF16)

    @pl.when(raw_away)
    def _():
        raw_copy().wait()

    phase('wait_cell')
    for tt in range(n_tp):

        def arrive_mix(tt=tt):
            pltpu.make_async_remote_copy(
                src_ref=mix_send,
                dst_ref=mix_all.at[:, pl.ds(tt * W, W)],
                send_sem=send_mx.at[0],
                recv_sem=recv_mx.at[tt],
                device_id={"tp": sibling},
                device_id_type=MESH,
            ).wait_recv()

        if tt:
            arrive_mix()
        else:
            pl.when(t != 0)(arrive_mix)

    phase('residual')
    mine_res = raw_blk[...].astype(F32) + dot(mix_all[...], wproj[...])
    my_rows = at(mine_group, R)
    res_all[my_rows, :] = mine_res.astype(BF16)

    def res_rows(tt):
        return res_all.at[at(lax.rem(tt + e, n_ep), R), :]

    got_res = spread_tp(1, res_rows, dz_far[::-1])

    def half_copy(c):
        return pltpu.make_async_remote_copy(
            src_ref=res_all.at[my_rows, pl.ds(c * HD, HD)],
            dst_ref=res_t.at[:, at(lax.rem(e, 2), HD)],
            send_sem=send_tr.at[1 + c],
            recv_sem=recv_tr.at[1 + lax.rem(e, 2)],
            device_id={"ep": mine_group, "tp": e // 2 * 2 + c},
            device_id_type=MESH,
        )

    stays = jnp.logical_and(t == 0, e < 2)

    @pl.when(jnp.logical_not(stays))
    def _():
        half_copy(0).start()

    @pl.when(stays)
    def _():
        res_t[:, at(lax.rem(e, 2), HD)] = res_all[my_rows, 0:HD]

    half_copy(1).start()

    load_dg.wait()
    load_du.wait()
    my_fgain = fgain_ref[:, at(e, Dc)]

    def stage_a(g):
        gy, gx = g // EX, lax.rem(g, EX)
        dx = lax.rem(gx + EX - ex, EX)
        return pltpu.make_async_remote_copy(
            src_ref=dense_send.at[at(g, R), pl.ds(0, F)],
            dst_ref=da_recv.at[dx, gy],
            send_sem=send_a.at[g],
            recv_sem=recv_a.at[dx * EY + gy],
            device_id={"ep": ey * EX + gx},
            device_id_type=MESH,
        )

    def stage_b(g):
        gy, gx = g // EX, lax.rem(g, EX)
        dy = lax.rem(gy + EY - ey, EY)
        return pltpu.make_async_remote_copy(
            src_ref=dense_send.at[at(g, R), pl.ds(F, F)],
            dst_ref=db_recv.at[dy, gx],
            send_sem=send_b.at[g],
            recv_sem=recv_b.at[dy * EX + gx],
            device_id={"ep": gy * EX + ex},
            device_id_type=MESH,
        )

    def dense_part(tt):
        g = lax.rem(tt + e, n_ep)
        rows = at(g, R)
        xg[rows, :] = (res_all[rows, :].astype(F32) * my_fgain).astype(BF16)
        dense_send[rows, :] = dot(xg[rows, :], dgu[...]).astype(BF16)

        @pl.when(lax.rem(g, EX) != ex)
        def _():
            stage_a(g).start()

        @pl.when(g // EX != ey)
        def _():
            stage_b(g).start()

    phase(None)
    dense_part(t)
    got_res[0].wait_recv()
    dense_part(sibling)
    late = None
    for dz in reversed(dz_far):
        got_res[dz].wait_recv()
        there = lax.rem(tz + TZ - dz, TZ) * 2
        odd = 2 * dz + 1
        passing = side_start(
            send_tp.at[1, odd], recv_tp.at[1, odd], res_rows(there + tc), res_rows(there + tc)
        )
        dense_part(there + tc)
        if late is not None:
            late[0].wait_recv()
            dense_part(late[1])
        late = (passing, there + 1 - tc)
    late[0].wait_recv()
    dense_part(late[1])

    wide_branch = branch_ref[...].astype(F32)
    pieces = Dc // LANES
    branch_rows = [
        jnp.sum(
            jnp.where(iota(wide_branch.shape, 0) == e * pieces + i, wide_branch, 0.0),
            axis=0,
            keepdims=True,
        )
        for i in range(pieces)
    ]
    my_branch = jnp.concatenate(branch_rows, axis=1) if pieces > 1 else branch_rows[0]
    my_branch = jnp.broadcast_to(my_branch, (8, Dc)).astype(BF16)
    ones = jnp.ones((8, Dc), BF16)
    block = res_all[...].astype(F32)
    square = block * block
    high = square.astype(BF16)
    low = (square - high.astype(F32)).astype(BF16)
    sums = dot_t(ones, high) + dot_t(ones, low)
    branch = dot_t(my_branch, xg[...])
    row8 = iota((8, LANES), 0)
    tile = jnp.zeros((8, LANES), F32)
    for qq in range(Q):
        cols = slice(qq * LANES, (qq + 1) * LANES)
        tile += jnp.where(row8 == qq, sums[:, cols], 0.0)
        tile += jnp.where(row8 == 4 + qq, branch[:, cols], 0.0)
    stat[...] = tile
    got_stat = {k: ep_start(3, k, stat, stat_recv.at[k]) for k in ep_far}

    got_disp = {}

    def dispatch(dy):
        rows = at(lax.rem(ey + dy, EY), S * EX)
        disp_send[rows, :] = dot(gmat[rows, :], xg[:, at(tc, HD)]).astype(BF16)
        for dx in dx_far:
            k = dy * EX + dx
            if k:
                got_disp[k] = ep_start(
                    5, k, disp_send.at[at(ep_peer(k), S), :], xrecv.at[:, at(2 * e + tc, HD)]
                )

    for dy in dy_far:
        dispatch(dy)

    got_a, got_b = {}, {}
    for d in dy_far:
        gy = lax.rem(ey + d, EY)
        term = dense_send[at(gy * EX + ex, R), 0:F].astype(F32)
        for dx in range(1, EX):
            pltpu.make_async_remote_copy(
                src_ref=dense_send.at[pl.ds(0, R), pl.ds(0, F)],
                dst_ref=da_recv.at[dx, gy],
                send_sem=send_a.at[0],
                recv_sem=recv_a.at[dx * EY + gy],
                device_id={"ep": e},
                device_id_type=MESH,
            ).wait_recv()
            term += da_recv[dx, gy].astype(F32)
        if d:
            a2_send[d] = term.astype(BF16)
            got_a[d] = ep_start(4, d * EX, a2_send.at[d], a2_recv.at[d])
        else:
            g = term
    for d in dx_far:
        gx = lax.rem(ex + d, EX)
        term = dense_send[at(ey * EX + gx, R), F : 2 * F].astype(F32)
        for dy in range(1, EY):
            pltpu.make_async_remote_copy(
                src_ref=dense_send.at[pl.ds(0, R), pl.ds(F, F)],
                dst_ref=db_recv.at[dy, gx],
                send_sem=send_b.at[0],
                recv_sem=recv_b.at[dy * EX + gx],
                device_id={"ep": e},
                device_id_type=MESH,
            ).wait_recv()
            term += db_recv[dy, gx].astype(F32)
        if d:
            b2_send[d] = term.astype(BF16)
            got_b[d] = ep_start(4, d, b2_send.at[d], b2_recv.at[d])
        else:
            u = term

    xrecv[:, at(2 * e + tc, HD)] = disp_send[at(e, S), :]

    def forward(k):
        region = xrecv.at[:, at(2 * ep_from(k) + tc, HD)]
        return side_start(send_fw.at[k], recv_fw.at[k], region, region)

    passed = [forward(0)]

    for k in reversed(ep_far):
        got_stat[k].wait_recv()
        tile += stat_recv[k]
    scale_l = lax.rsqrt(tile[0:Q, :] * (1.0 / D) + EPS)
    share_l = 1.0 / (1.0 + jnp.exp(-(scale_l * tile[4 : 4 + Q, :])))
    my_scale = jnp.zeros((R, 1), F32)
    my_bshare = jnp.zeros((R, 1), F32)
    for qq in range(Q):
        here = iota((R, LANES), 1) + qq * LANES == iota((R, LANES), 0) + e * R
        my_scale += jnp.sum(jnp.where(here, scale_l[qq : qq + 1, :], 0.0), axis=1, keepdims=True)
        my_bshare += jnp.sum(jnp.where(here, share_l[qq : qq + 1, :], 0.0), axis=1, keepdims=True)
    scale_row = (
        jnp.concatenate([scale_l[qq : qq + 1, :] for qq in range(Q)], axis=1) if Q > 1 else scale_l
    )
    row_scale = jnp.sum(jnp.where(row_no == my_code, scale_row, 0.0), axis=1, keepdims=True)

    for d in reversed(dy_far):
        if d:
            got_a[d].wait_recv()
            g += a2_recv[d].astype(F32)
    for d in reversed(dx_far):
        if d:
            got_b[d].wait_recv()
            u += b2_recv[d].astype(F32)
    g, u = g * my_scale, u * my_scale
    hid_all[at(e, R), :] = (g / (1.0 + jnp.exp(-g)) * u).astype(BF16)
    got_hid = {
        k: ep_start(6, k, hid_all.at[at(e, R), :], hid_all.at[at(e, R), :]) for k in ep_far
    }

    load_eg.wait()
    load_eu.wait()
    for k in reversed(ep_far):
        got_disp[k].wait_recv()
        passed.append(forward(k))
    for copy in passed:
        copy.wait_recv()
    gp = dot(xrecv[...], eg[0]) * row_scale
    up = dot(xrecv[...], eu[0]) * row_scale
    ehid = (gp / (1.0 + jnp.exp(-gp)) * up).astype(BF16)
    ehid8 = dot(spread, ehid).astype(BF16)
    for copy in load_ed:
        copy.wait()
    step = min(512, DH)
    strips = [slice(c * step, (c + 1) * step) for c in range(DH // step)]
    got_yo = []
    for i, cols in enumerate(strips):
        yo_send[:, cols] = (dot(ehid8, edc[0, :, cols]) * row_share).astype(BF16)
        got_yo.append(
            side_start(send_sb.at[i], recv_sb.at[i], yo_send.at[:, cols], yo_recv.at[:, cols])
        )
    got_fin = {}
    wide = DH // 2
    per_strip = max(1, wide // step)
    for i, (copy, cols) in enumerate(zip(got_yo, strips)):
        y = dot(ehid8, edc[1, :, cols]) * row_share
        copy.wait_recv()
        y += yo_recv[:, cols].astype(F32)
        fin_send[:, :, cols] = y.reshape(n_ep, PAD, step).astype(BF16)
        if i % per_strip == per_strip - 1:
            j = i // per_strip
            part = pl.ds(j * per_strip * step, per_strip * step)
            for k in ep_far:
                got_fin[j, k] = ep_start(
                    7 + j,
                    k,
                    fin_send.at[ep_peer(k), pl.ds(0, CAP), part],
                    fin_recv.at[e, pl.ds(0, CAP), part],
                )
    fin_recv[e] = fin_send[e]

    load_dd.wait()
    got_no = {}
    for dy in reversed(dy_far):
        for dx in range(EX):
            k = (EY - dy) % EY * EX + dx
            if k:
                got_hid[k].wait_recv()
        rows = at(lax.rem(ey + dy, EY), RC)
        dno_send[rows, :] = dot(hid_all[rows, :], dd[:, at(1 - tc, HD)]).astype(BF16)
        got_no[dy] = side_start(
            send_sb.at[4 + dy], recv_sb.at[4 + dy], dno_send.at[rows, :], dno_recv.at[rows, :]
        )
    got_dn = {}
    for dy in reversed(dy_far):
        rows = at(lax.rem(ey + dy, EY), RC)
        down = dot(hid_all[rows, :], dd[:, at(tc, HD)])
        got_no[dy].wait_recv()
        dn_send[rows, :] = (down + dno_recv[rows, :].astype(F32)).astype(BF16)
        for dx in dx_far:
            k = dy * EX + dx
            if k:
                got_dn[k] = ep_start(
                    9, k, dn_send.at[at(ep_peer(k), R), :], dn_recv.at[:, at(e, HD)]
                )
    dn_recv[:, at(e, HD)] = dn_send[at(e, R), :]

    for copy in got_fin.values():
        copy.wait_recv()
    for z in range(TZ):
        cols = slice(z * Dc, (z + 1) * Dc)
        back = fin_recv[:, :, cols].astype(F32).reshape(S8, Dc).astype(BF16)
        comb[:, cols] = dot(pick, back)
    for k in reversed(ep_far):
        got_dn[k].wait_recv()
    got_tp = {}
    for dz in dz_far + [0]:
        cols = at(lax.rem(tz + dz, TZ), Dc)
        piece = comb[:, cols] + my_bshare * dn_recv[:, cols].astype(F32)
        tp_send[:, cols] = piece.astype(BF16)
        if dz:
            got_tp[dz] = tp_start(2, 2 * dz, tp_send.at[:, cols], tp_recv.at[dz])

    for i in range(2):

        @pl.when(jnp.logical_not(jnp.logical_and(t == 0, e == i)))
        def _():
            pltpu.make_async_remote_copy(
                src_ref=res_all.at[pl.ds(0, R), pl.ds(0, HD)],
                dst_ref=res_t.at[:, pl.ds(i * HD, HD)],
                send_sem=send_tr.at[1 + i],
                recv_sem=recv_tr.at[1 + i],
                device_id={"tp": sibling},
                device_id_type=MESH,
            ).wait_recv()

    last = res_t[...].astype(F32) + tp_send[:, at(tz, Dc)].astype(F32)
    for dz in reversed(dz_far):
        got_tp[dz].wait_recv()
        last += tp_recv[dz].astype(F32)
    out_all[:, at(tc * TZ + tz, Dc)] = last.astype(BF16)

    def out_cols(tt):
        return out_all.at[:, at(lax.rem(tt, 2) * TZ + tt // 2, Dc)]

    got_out = spread_tp(3, out_cols, dz_far)
    for k in ep_far:
        mix_copy(k).wait_send()

    @pl.when(t != 0)
    def _():
        mix_copy(0).wait_send()

    @pl.when(jnp.logical_not(stays))
    def _():
        half_copy(0).wait_send()

    half_copy(1).wait_send()
    for g in range(n_ep):

        @pl.when(g % EX != ex)
        def _():
            stage_a(g).wait_send()

        @pl.when(g // EX != ey)
        def _():
            stage_b(g).wait_send()

    gather_tp(3, out_cols, got_out)
    for b in range(n_ep):
        for c in range(2):
            out_ref[:, pl.ds((2 * b + c) * HD, HD)] = out_all[:, pl.ds(c * DH + b * HD, HD)]
    for copy in pending:
        copy.wait_send()
    store_mat.wait()


def store_kernel(chunks, *refs):
    bufs, sems = refs[8:12], refs[12]
    rows = refs[3].shape[0] // chunks
    moves = [(refs[i], bufs[i], refs[4 + i]) for i in range(3)]
    for c in range(chunks):
        part = pl.ds(c * rows, rows)
        moves.append((refs[3].at[part], bufs[3].at[part], refs[7].at[part]))
    inward = [pltpu.make_async_copy(m[0], m[1], sems.at[0, i]) for i, m in enumerate(moves)]
    outward = [pltpu.make_async_copy(m[1], m[2], sems.at[1, i]) for i, m in enumerate(moves)]
    for copy in inward:
        copy.start()
    for came, goes in zip(inward, outward):
        came.wait()
        goes.start()
    for copy in outward:
        copy.wait()


def on_device(
    n_ep,
    n_tp,
    tokens,
    state_matrix,
    state_norm,
    state_max,
    mixer_gain,
    w_query,
    w_key,
    w_value,
    w_outgate,
    w_ingate,
    w_forget,
    forget_bias,
    w_proj,
    ffn_gain,
    w_branch,
    routes,
    route_weight,
    expert_gate,
    expert_up,
    expert_down,
    dense_gate,
    dense_up,
    dense_down,
):
    R, D = tokens.shape
    hd = state_norm.shape[2]
    N, Dc, DH, W = R * n_ep, D // n_ep, D // 2, hd
    F = dense_gate.shape[1]
    FE = expert_gate.shape[2]
    S, S8 = CAP * n_ep, PAD * n_ep
    EX = {16: 4, 4: 2}[n_ep]
    EY = n_ep // EX
    vmem = pl.BlockSpec(memory_space=pltpu.VMEM)
    hbm = pl.BlockSpec(memory_space=pltpu.HBM)
    V = pltpu.VMEM
    scratch = [
        V(state_matrix.shape, F32),
        V((Dc, 4 * W), BF16),
        V((n_tp * W, Dc), BF16),
        V(expert_gate.shape, BF16),
        V(expert_up.shape, BF16),
        V((2, FE, DH), BF16),
        V((Dc, 2 * F), BF16),
        V(dense_down.shape, BF16),
        V((R, D), BF16),
        V((N, Dc), BF16),
        V((n_ep, LANES), F32),
        V((n_ep, n_ep, LANES), F32),
        V((N, 4 * W), BF16),
        V((n_ep, R, 4 * W), BF16),
        V((R, W), F32),
        V((R, W), BF16),
        V((R, n_tp * W), BF16),
        V((R, Dc), BF16),
        V((N, Dc), BF16),
        V((R, Dc), BF16),
        V((N, Dc), BF16),
        V((n_ep * S, N), BF16),
        V((8, LANES), F32),
        V((n_ep, 8, LANES), F32),
        V((N, 2 * F), BF16),
        V((EX, EY, R, F), BF16),
        V((EY, EX, R, F), BF16),
        V((EY, R, F), BF16),
        V((EY, R, F), BF16),
        V((EX, R, F), BF16),
        V((EX, R, F), BF16),
        V((n_ep * S, Dc // 2), BF16),
        V((S, D), BF16),
        V((N, F), BF16),
        V((S8, DH), BF16),
        V((S8, DH), BF16),
        V((n_ep, PAD, DH), BF16),
        V((n_ep, PAD, DH), BF16),
        V((N, Dc // 2), BF16),
        V((N, Dc // 2), BF16),
        V((N, Dc // 2), BF16),
        V((R, DH), BF16),
        V((R, DH), F32),
        V((R, DH), BF16),
        V((n_tp // 2, R, Dc), BF16),
        V((R, D), BF16),
        pltpu.SemaphoreType.DMA((12 + 2 * n_ep,)),
        pltpu.SemaphoreType.DMA((10, n_ep)),
        pltpu.SemaphoreType.DMA((10, n_ep)),
        pltpu.SemaphoreType.DMA((4, n_tp)),
        pltpu.SemaphoreType.DMA((4, n_tp)),
        pltpu.SemaphoreType.DMA((n_ep,)),
        pltpu.SemaphoreType.DMA((n_tp,)),
        pltpu.SemaphoreType.DMA((3,)),
        pltpu.SemaphoreType.DMA((3,)),
        pltpu.SemaphoreType.DMA((n_ep,)),
        pltpu.SemaphoreType.DMA((n_ep,)),
        pltpu.SemaphoreType.DMA((8,)),
        pltpu.SemaphoreType.DMA((8,)),
        pltpu.SemaphoreType.DMA((n_ep,)),
        pltpu.SemaphoreType.DMA((n_ep,)),
        pltpu.SemaphoreType.DMA((n_ep,)),
        pltpu.SemaphoreType.DMA((n_ep,)),
    ]
    Sh = jax.ShapeDtypeStruct
    results = pl.pallas_call(
        functools.partial(layer_kernel, n_ep, n_tp),
        out_shape=(
            Sh((R, D), BF16),
            Sh((R, hd), F32),
            Sh((1, R), F32),
            Sh(state_matrix.shape, F32),
        ),
        in_specs=[vmem] * 11 + [hbm] * 12,
        out_specs=(vmem,) * 3 + (hbm,),
        scratch_shapes=scratch,
        compiler_params=pltpu.CompilerParams(
            collective_id=0, has_side_effects=True, vmem_limit_bytes=66_000_000
        ),
    )(
        tokens,
        mixer_gain[None, :],
        w_ingate.T,
        w_forget.T,
        forget_bias[None, :],
        state_norm.reshape(R, hd),
        state_max.T,
        ffn_gain[None, :],
        w_branch.reshape(-1, LANES),
        routes.T,
        route_weight.T,
        state_matrix,
        w_query,
        w_key,
        w_value,
        w_outgate,
        w_proj,
        expert_gate,
        expert_up,
        expert_down,
        dense_gate,
        dense_up,
        dense_down,
    )
    layer_out, new_norm, new_max, new_matrix = pl.pallas_call(
        functools.partial(store_kernel, 8),
        out_shape=tuple(Sh(r.shape, r.dtype) for r in results),
        in_specs=[hbm] * 4,
        out_specs=(hbm,) * 4,
        scratch_shapes=[V(r.shape, r.dtype) for r in results] + [pltpu.SemaphoreType.DMA((2, 11))],
        compiler_params=pltpu.CompilerParams(vmem_limit_bytes=66_000_000),
    )(*results)
    return (layer_out, new_matrix, new_norm.reshape(R, 1, hd), new_max.T)


def solution(mesh):
    in_specs = (
        P("ep", None),
        P("ep", "tp", None, None),
        P("ep", "tp", None),
        P("ep", "tp"),
        P(),
        P("ep", "tp"),
        P("ep", "tp"),
        P("ep", "tp"),
        P("ep", "tp"),
        P(),
        P(),
        P(),
        P("tp", "ep"),
        P(),
        P(),
        P("ep", None),
        P("ep", None),
        P("ep", None, "tp"),
        P("ep", None, "tp"),
        P("ep", "tp", None),
        P("ep", "tp"),
        P("ep", "tp"),
        P("tp", "ep"),
    )
    out_specs = (P("ep", None), P("ep", "tp", None, None), P("ep", "tp", None), P("ep", "tp"))
    return jax.shard_map(
        functools.partial(on_device, mesh.shape["ep"], mesh.shape["tp"]),
        mesh=mesh,
        in_specs=in_specs,
        out_specs=out_specs,
        check_vma=False,
    )
```

```python
import functools

import jax
import jax.numpy as jnp
from jax import lax
from jax.experimental import pallas as pl
from jax.experimental.pallas import tpu as pltpu
from jax.sharding import PartitionSpec as P

EPS = 1e-06
LANES = 128
CAP = 6
PAD = 8
F32 = jnp.float32
BF16 = jnp.bfloat16
MESH = pl.DeviceIdType.MESH


def dot(a, b):
    return jnp.dot(a, b, preferred_element_type=F32)


def dot_t(a, b):
    return lax.dot_general(a, b, (((1,), (1,)), ((), ())), preferred_element_type=F32)


def iota(shape, dim):
    return lax.broadcasted_iota(jnp.int32, shape, dim)


def layer_kernel(
    n_ep,
    n_tp,
    tokens_ref,
    gain_ref,
    win_ref,
    wfo_ref,
    bias_ref,
    norm_ref,
    smax_ref,
    fgain_ref,
    branch_ref,
    routes_ref,
    weight_ref,
    state_hbm,
    wq_hbm,
    wk_hbm,
    wv_hbm,
    wo_hbm,
    wproj_hbm,
    eg_hbm,
    eu_hbm,
    ed_hbm,
    dg_hbm,
    du_hbm,
    dd_hbm,
    out_ref,
    norm_out_ref,
    max_out_ref,
    mat_ref,
    state,
    wcat,
    wproj,
    eg,
    eu,
    edc,
    dgu,
    dd,
    nrm,
    x_all,
    info,
    info_recv,
    part_send,
    part_recv,
    numer,
    mix_send,
    mix_all,
    raw_blk,
    res_all,
    res_t,
    xg,
    gmat,
    stat,
    stat_recv,
    dense_send,
    da_recv,
    db_recv,
    a2_send,
    a2_recv,
    b2_send,
    b2_recv,
    disp_send,
    xrecv,
    hid_all,
    yo_send,
    yo_recv,
    fin_send,
    fin_recv,
    dno_send,
    dno_recv,
    dn_send,
    dn_recv,
    comb,
    tp_send,
    tp_recv,
    out_all,
    load_sems,
    send_ep,
    recv_ep,
    send_tp,
    recv_tp,
    send_mx,
    recv_mx,
    send_tr,
    recv_tr,
    send_fw,
    recv_fw,
    send_sb,
    recv_sb,
    send_a,
    recv_a,
    send_b,
    recv_b,
):
    e = lax.axis_index("ep")
    t = lax.axis_index("tp")
    R, D = tokens_ref.shape
    N = R * n_ep
    Dc = D // n_ep
    HD = Dc // 2
    DH = D // 2
    W = mix_send.shape[1]
    F = dd.shape[0]
    EX = {16: 4, 4: 2}[n_ep]
    EY = n_ep // EX
    TZ = n_tp // 2
    S = CAP * n_ep
    S8 = PAD * n_ep
    Q = N // LANES
    PER = LANES // R
    RC = R * EX
    ey, ex = e // EX, lax.rem(e, EX)
    mine_group = lax.rem(t + e, n_ep)
    tz, tc = t // 2, lax.rem(t, 2)

    def at(index, size):
        return pl.ds(pl.multiple_of(index * size, size), size)

    def ring(d, n):
        return min(d, n - d)

    ep_far = sorted(range(1, n_ep), key=lambda k: -(ring(k // EX, EY) + ring(k % EX, EX)))
    dz_far = sorted(range(1, TZ), key=lambda d: -ring(d, TZ))
    dy_far = sorted(range(EY), key=lambda d: -ring(d, EY))
    dx_far = sorted(range(EX), key=lambda d: -ring(d, EX))

    def ep_peer(k):
        return lax.rem(ey + k // EX, EY) * EX + lax.rem(ex + k % EX, EX)

    def ep_from(k):
        return lax.rem(ey + EY - k // EX, EY) * EX + lax.rem(ex + EX - k % EX, EX)

    def tp_peer(k):
        return lax.rem(tz + k // 2, TZ) * 2 + lax.rem(tc + k % 2, 2)

    sibling = tz * 2 + 1 - tc

    loads = []

    def load(src, dst):
        copy = pltpu.make_async_copy(src, dst, load_sems.at[len(loads)])
        copy.start()
        loads.append(copy)
        return copy

    pending = []
    scopes = []

    def phase(name):
        if scopes:
            scopes.pop().__exit__(None, None, None)
        if name:
            scopes.append(jax.named_scope(name))
            scopes[0].__enter__()

    def ep_start(phase, k, src, dst):
        copy = pltpu.make_async_remote_copy(
            src_ref=src,
            dst_ref=dst,
            send_sem=send_ep.at[phase, k],
            recv_sem=recv_ep.at[phase, k],
            device_id={"ep": ep_peer(k)},
            device_id_type=MESH,
        )
        copy.start()
        pending.append(copy)
        return copy

    def tp_start(phase, k, src, dst, to=None):
        copy = pltpu.make_async_remote_copy(
            src_ref=src,
            dst_ref=dst,
            send_sem=send_tp.at[phase, k],
            recv_sem=recv_tp.at[phase, k],
            device_id={"tp": tp_peer(k if to is None else to)},
            device_id_type=MESH,
        )
        copy.start()
        pending.append(copy)
        return copy

    def side_start(send_sem, recv_sem, src, dst):
        copy = pltpu.make_async_remote_copy(
            src_ref=src,
            dst_ref=dst,
            send_sem=send_sem,
            recv_sem=recv_sem,
            device_id={"tp": sibling},
            device_id_type=MESH,
        )
        copy.start()
        pending.append(copy)
        return copy

    def spread_tp(phase, region, order):
        copies = {0: tp_start(phase, 1, region(t), region(t))}
        for dz in order:
            copies[dz] = tp_start(phase, 2 * dz, region(t), region(t))
        return copies

    def gather_tp(phase, region, copies, here=()):
        passed = []
        for dz in reversed(dz_far):
            if dz not in here:
                copies[dz].wait_recv()
            source = lax.rem(tz + TZ - dz, TZ) * 2 + tc
            odd = 2 * dz + 1
            passed.append(
                side_start(
                    send_tp.at[phase, odd], recv_tp.at[phase, odd], region(source), region(source)
                )
            )
        copies[0].wait_recv()
        for copy in passed:
            copy.wait_recv()

    def raw_copy():
        return pltpu.make_async_remote_copy(
            src_ref=tokens_ref.at[:, at(t, Dc)],
            dst_ref=raw_blk,
            send_sem=send_tr.at[0],
            recv_sem=recv_tr.at[0],
            device_id={"ep": t, "tp": lax.rem(e + n_ep - t, n_ep)},
            device_id_type=MESH,
        )

    raw_away = jnp.logical_or(e != 0, t != 0)

    phase('greet')
    barrier = pltpu.get_barrier_semaphore()
    for k in ep_far:
        pl.semaphore_signal(barrier, inc=1, device_id={"ep": ep_peer(k)}, device_id_type=MESH)
    for k in range(1, n_tp):
        pl.semaphore_signal(barrier, inc=1, device_id={"tp": tp_peer(k)}, device_id_type=MESH)

    load_w = [
        load(src, wcat.at[:, pl.ds(i * W, W)])
        for i, src in enumerate((wq_hbm, wk_hbm, wv_hbm, wo_hbm))
    ]
    load_proj = load(wproj_hbm, wproj.at[at(t, W), :])
    load_state = load(state_hbm, state)
    load_dg, load_du = load(dg_hbm, dgu.at[:, pl.ds(0, F)]), load(du_hbm, dgu.at[:, pl.ds(F, F)])
    load_eg, load_eu = load(eg_hbm, eg), load(eu_hbm, eu)
    load_ed = [
        load(ed_hbm.at[0, :, at(2 * b + side, HD)], edc.at[i, :, pl.ds(b * HD, HD)])
        for i, side in enumerate((1 - tc, tc))
        for b in range(n_ep)
    ]
    load_dd = load(dd_hbm, dd)

    fin_recv[...] = jnp.zeros_like(fin_recv)
    wide = tokens_ref[...].astype(F32)
    scale = lax.rsqrt(jnp.mean(wide * wide, axis=-1, keepdims=True) + EPS)
    nrm[...] = (wide * scale * gain_ref[...]).astype(BF16)

    r0, r1 = routes_ref[0:1, :], routes_ref[1:2, :]
    w0, w1 = weight_ref[0:1, :], weight_ref[1:2, :]
    total = w0 + w1
    which = iota((n_ep, R), 0)
    hit0, hit1 = which == r0, which == r1
    named = jnp.where(jnp.logical_or(hit0, hit1), 1.0, 0.0)
    earlier = jnp.where(iota((R, R), 0) < iota((R, R), 1), 1.0, 0.0).astype(BF16)
    slot = dot(named.astype(BF16), earlier)
    code = jnp.where(named > 0.0, slot + 1.0, 0.0)
    group_at = (e * CAP).astype(F32)
    rowcode = jnp.where(named > 0.0, slot + (1.0 + group_at), 0.0)
    shares = jnp.where(hit0, w0 / total, 0.0) + jnp.where(hit1, w1 / total, 0.0)
    info[:, 0:R] = rowcode
    info[:, R : 2 * R] = shares
    info[:, 2 * R : LANES] = jnp.zeros((n_ep, LANES - 2 * R), F32)

    phase('greeted')
    pl.semaphore_wait(barrier, n_ep - 1 + n_tp - 1)
    phase('send_x')
    got_x = {k: ep_start(0, k, nrm.at[:, at(ep_peer(k), Dc)], x_all.at[at(e, R), :]) for k in ep_far}
    x_all[at(e, R), :] = nrm[:, at(e, Dc)]
    load_proj.wait()

    def proj_rows(tt):
        return wproj.at[at(tt, W), :]

    relays = {2: (1, 2), 6: (7,)} if TZ == 8 else {}
    direct = [dz for dz in dz_far if TZ != 8 or ring(dz, TZ) <= 2]
    got_wp = spread_tp(0, proj_rows, direct)

    phase('gates')
    gate_in = dot_t(nrm[...], win_ref[...])
    gate_fo = dot_t(nrm[...], wfo_ref[...]) + bias_ref[...]
    mine = iota(gate_in.shape, 1) == t
    g_in = jnp.sum(jnp.where(mine, gate_in, 0.0), axis=1, keepdims=True)
    g_fo = jnp.sum(jnp.where(mine, gate_fo, 0.0), axis=1, keepdims=True)
    eye = iota((R, R), 0) == iota((R, R), 1)
    smax = jnp.sum(jnp.where(eye, smax_ref[...], 0.0), axis=1, keepdims=True)
    log_keep = jnp.minimum(g_fo, 0.0) - jnp.log(1.0 + jnp.exp(-jnp.abs(g_fo)))
    carried = log_keep + smax
    new_max = jnp.maximum(carried, g_in)
    keep = jnp.exp(carried - new_max)
    write = jnp.exp(g_in - new_max)
    max_out_ref[...] = jnp.sum(jnp.where(eye, new_max, 0.0), axis=0, keepdims=True)

    phase('project')
    for copy in load_w:
        copy.wait()
    got_part = {}
    for dy in [(EY - d) % EY for d in range(EY)]:
        back = (EY - dy) % EY
        for dx in range(EX):
            k = dy * EX + dx
            if k:
                got_x[k].wait_recv()
        rows = at(lax.rem(ey + back, EY), RC)
        part_send[rows, :] = dot(x_all[rows, :], wcat[...]).astype(BF16)
        for dx in dx_far:
            k = back * EX + dx
            if k:
                got_part[k] = ep_start(1, k, part_send.at[at(ep_peer(k), R), :], part_recv.at[k])
    for first, onward in relays.items():
        got_wp[first].wait_recv()
        block = proj_rows(lax.rem(tz + TZ - first, TZ) * 2 + tc)
        for then in onward:
            dz = (first + then) % TZ
            got_wp[dz] = tp_start(0, 2 * dz, block, block, 2 * then)
    phase('send_info')
    got_info = {k: ep_start(2, k, info, info_recv.at[k]) for k in ep_far}

    @pl.when(raw_away)
    def _():
        raw_copy().start()

    @pl.when(jnp.logical_not(raw_away))
    def _():
        raw_blk[...] = tokens_ref[:, at(t, Dc)]

    phase('sum_parts')
    proj = part_send[at(e, R), :].astype(F32)
    for k in reversed(ep_far):
        got_part[k].wait_recv()
        proj += part_recv[k].astype(F32)

    phase('cell')
    load_state.wait()
    q = proj[:, 0:W]
    key = proj[:, W : 2 * W] * W ** (-0.5)
    val = proj[:, 2 * W : 3 * W]
    og = proj[:, 3 * W : 4 * W]
    key_w = write * key
    new_norm = keep * norm_ref[...] + key_w
    q_t = q.T
    for b in range(R):
        numer[b : b + 1, :] = jnp.sum(q_t[:, b : b + 1] * state[b, 0], axis=0, keepdims=True)
    top = keep * numer[...] + jnp.sum(q * key_w, axis=1, keepdims=True) * val
    denom = jnp.sum(q * new_norm, axis=1, keepdims=True)
    cell = top / jnp.maximum(jnp.abs(denom), 1.0)
    mix_send[...] = (cell / (1.0 + jnp.exp(-og))).astype(BF16)

    phase('send_cell')
    def mix_copy(k):
        return pltpu.make_async_remote_copy(
            src_ref=mix_send,
            dst_ref=mix_all.at[:, at(t, W)],
            send_sem=send_mx.at[k],
            recv_sem=recv_mx.at[t],
            device_id={"ep": ep_peer(k), "tp": lax.rem(e + n_ep - ep_peer(k), n_ep)},
            device_id_type=MESH,
        )

    for k in ep_far:
        mix_copy(k).start()

    @pl.when(t != 0)
    def _():
        mix_copy(0).start()

    @pl.when(t == 0)
    def _():
        mix_all[:, at(t, W)] = mix_send[...]

    key_t = key_w.T
    for b in range(R):
        state[b, 0] = keep[b : b + 1, :] * state[b, 0] + key_t[:, b : b + 1] * val[b : b + 1, :]
    store_mat = load(state, mat_ref)
    phase('pass_proj')
    gather_tp(0, proj_rows, got_wp, relays)
    phase('info')
    norm_out_ref[...] = new_norm

    for k in ep_far:
        got_info[k].wait_recv()
    phase('maps')
    quarter = iota((n_ep, LANES), 1) // R
    codes, sharesl = [], []

    info_recv[0] = info[...]
    for qq in range(Q):
        ctile = jnp.zeros((n_ep, LANES), F32)
        stile = jnp.zeros((n_ep, LANES), F32)
        for j in range(PER):
            g = qq * PER + j
            gy, gx = g // EX, g % EX
            slot_k = lax.rem(ey + (EY - gy), EY) * EX + lax.rem(ex + (EX - gx), EX)
            tile = info_recv[slot_k]
            there = quarter == j
            ctile += jnp.where(there, tile if j == 0 else pltpu.roll(tile, j * R, 1), 0.0)
            back = (j - 1) % PER * R
            stile += jnp.where(there, tile if back == 0 else pltpu.roll(tile, back, 1), 0.0)
        codes.append(ctile)
        sharesl.append(stile)
    code_all = jnp.concatenate(codes, axis=1) if Q > 1 else codes[0]
    share_all = jnp.concatenate(sharesl, axis=1) if Q > 1 else sharesl[0]
    row_no = (iota((S, N), 0) + 1).astype(F32)
    for p in range(n_ep):
        gmat[p * S : (p + 1) * S, :] = jnp.where(row_no == code_all[p : p + 1, :], 1.0, 0.0).astype(
            BF16
        )
    is_mine = iota((n_ep, N), 0) == e
    my_code = jnp.sum(jnp.where(is_mine, code_all, 0.0), axis=0, keepdims=True)
    my_share = jnp.sum(jnp.where(is_mine, share_all, 0.0), axis=0, keepdims=True)
    my_code8 = jnp.where(
        my_code > 0.0, my_code + ((PAD - CAP) * (iota((1, N), 1) // R)).astype(F32), 0.0
    )
    row_share = jnp.sum(
        jnp.where((iota((S8, N), 0) + 1).astype(F32) == my_code8, my_share, 0.0),
        axis=1,
        keepdims=True,
    )
    spread = jnp.where(
        jnp.logical_and(
            iota((S8, S), 0) // PAD * CAP + iota((S8, S), 0) % PAD == iota((S8, S), 1),
            iota((S8, S), 0) % PAD < CAP,
        ),
        1.0,
        0.0,
    ).astype(BF16)
    repeat = jnp.where(iota((S8, n_ep), 0) // PAD == iota((S8, n_ep), 1), 1.0, 0.0).astype(BF16)
    code_rep = dot(repeat, code.astype(BF16))
    pick_t = jnp.where((iota((S8, R), 0) % PAD + 1).astype(F32) == code_rep, 1.0, 0.0)
    pick = pick_t.T.astype(BF16)

    @pl.when(raw_away)
    def _():
        raw_copy().wait()

    phase('wait_cell')
    heads = n_tp // 4
    mine_res = raw_blk[...].astype(F32)
    for tt in range(n_tp):

        def arrive_mix(tt=tt):
            pltpu.make_async_remote_copy(
                src_ref=mix_send,
                dst_ref=mix_all.at[:, pl.ds(tt * W, W)],
                send_sem=send_mx.at[0],
                recv_sem=recv_mx.at[tt],
                device_id={"tp": sibling},
                device_id_type=MESH,
            ).wait_recv()

        if tt:
            arrive_mix()
        else:
            pl.when(t != 0)(arrive_mix)
        if tt % heads == heads - 1:
            part = pl.ds((tt + 1 - heads) * W, heads * W)
            mine_res += dot(mix_all[:, part], wproj[part, :])

    phase('residual')
    my_rows = at(mine_group, R)
    res_all[my_rows, :] = mine_res.astype(BF16)

    def res_rows(tt):
        return res_all.at[at(lax.rem(tt + e, n_ep), R), :]

    got_res = spread_tp(1, res_rows, dz_far[::-1])

    def half_copy(c):
        return pltpu.make_async_remote_copy(
            src_ref=res_all.at[my_rows, pl.ds(c * HD, HD)],
            dst_ref=res_t.at[:, at(lax.rem(e, 2), HD)],
            send_sem=send_tr.at[1 + c],
            recv_sem=recv_tr.at[1 + lax.rem(e, 2)],
            device_id={"ep": mine_group, "tp": e // 2 * 2 + c},
            device_id_type=MESH,
        )

    stays = jnp.logical_and(t == 0, e < 2)

    @pl.when(jnp.logical_not(stays))
    def _():
        half_copy(0).start()

    @pl.when(stays)
    def _():
        res_t[:, at(lax.rem(e, 2), HD)] = res_all[my_rows, 0:HD]

    half_copy(1).start()

    load_dg.wait()
    load_du.wait()
    my_fgain = fgain_ref[:, at(e, Dc)]

    def stage_a(g):
        gy, gx = g // EX, lax.rem(g, EX)
        dx = lax.rem(gx + EX - ex, EX)
        return pltpu.make_async_remote_copy(
            src_ref=dense_send.at[at(g, R), pl.ds(0, F)],
            dst_ref=da_recv.at[dx, gy],
            send_sem=send_a.at[g],
            recv_sem=recv_a.at[dx * EY + gy],
            device_id={"ep": ey * EX + gx},
            device_id_type=MESH,
        )

    def stage_b(g):
        gy, gx = g // EX, lax.rem(g, EX)
        dy = lax.rem(gy + EY - ey, EY)
        return pltpu.make_async_remote_copy(
            src_ref=dense_send.at[at(g, R), pl.ds(F, F)],
            dst_ref=db_recv.at[dy, gx],
            send_sem=send_b.at[g],
            recv_sem=recv_b.at[dy * EX + gx],
            device_id={"ep": gy * EX + ex},
            device_id_type=MESH,
        )

    def dense_part(tt):
        g = lax.rem(tt + e, n_ep)
        rows = at(g, R)
        xg[rows, :] = (res_all[rows, :].astype(F32) * my_fgain).astype(BF16)
        dense_send[rows, :] = dot(xg[rows, :], dgu[...]).astype(BF16)

        @pl.when(lax.rem(g, EX) != ex)
        def _():
            stage_a(g).start()

        @pl.when(g // EX != ey)
        def _():
            stage_b(g).start()

    phase(None)
    dense_part(t)
    got_res[0].wait_recv()
    dense_part(sibling)
    late = None
    for dz in reversed(dz_far):
        got_res[dz].wait_recv()
        there = lax.rem(tz + TZ - dz, TZ) * 2
        odd = 2 * dz + 1
        passing = side_start(
            send_tp.at[1, odd], recv_tp.at[1, odd], res_rows(there + tc), res_rows(there + tc)
        )
        dense_part(there + tc)
        if late is not None:
            late[0].wait_recv()
            dense_part(late[1])
        late = (passing, there + 1 - tc)
    late[0].wait_recv()
    dense_part(late[1])

    wide_branch = branch_ref[...].astype(F32)
    pieces = Dc // LANES
    branch_rows = [
        jnp.sum(
            jnp.where(iota(wide_branch.shape, 0) == e * pieces + i, wide_branch, 0.0),
            axis=0,
            keepdims=True,
        )
        for i in range(pieces)
    ]
    my_branch = jnp.concatenate(branch_rows, axis=1) if pieces > 1 else branch_rows[0]
    my_branch = jnp.broadcast_to(my_branch, (8, Dc)).astype(BF16)
    ones = jnp.ones((8, Dc), BF16)
    block = res_all[...].astype(F32)
    square = block * block
    high = square.astype(BF16)
    low = (square - high.astype(F32)).astype(BF16)
    sums = dot_t(ones, high) + dot_t(ones, low)
    branch = dot_t(my_branch, xg[...])
    row8 = iota((8, LANES), 0)
    tile = jnp.zeros((8, LANES), F32)
    for qq in range(Q):
        cols = slice(qq * LANES, (qq + 1) * LANES)
        tile += jnp.where(row8 == qq, sums[:, cols], 0.0)
        tile += jnp.where(row8 == 4 + qq, branch[:, cols], 0.0)
    stat[...] = tile
    got_stat = {k: ep_start(3, k, stat, stat_recv.at[k]) for k in ep_far}

    got_disp = {}

    def dispatch(dy):
        rows = at(lax.rem(ey + dy, EY), S * EX)
        disp_send[rows, :] = dot(gmat[rows, :], xg[:, at(tc, HD)]).astype(BF16)
        for dx in dx_far:
            k = dy * EX + dx
            if k:
                got_disp[k] = ep_start(
                    5, k, disp_send.at[at(ep_peer(k), S), :], xrecv.at[:, at(2 * e + tc, HD)]
                )

    for dy in dy_far:
        dispatch(dy)

    got_a, got_b = {}, {}
    for d in dy_far:
        gy = lax.rem(ey + d, EY)
        term = dense_send[at(gy * EX + ex, R), 0:F].astype(F32)
        for dx in range(1, EX):
            pltpu.make_async_remote_copy(
                src_ref=dense_send.at[pl.ds(0, R), pl.ds(0, F)],
                dst_ref=da_recv.at[dx, gy],
                send_sem=send_a.at[0],
                recv_sem=recv_a.at[dx * EY + gy],
                device_id={"ep": e},
                device_id_type=MESH,
            ).wait_recv()
            term += da_recv[dx, gy].astype(F32)
        if d:
            a2_send[d] = term.astype(BF16)
            got_a[d] = ep_start(4, d * EX, a2_send.at[d], a2_recv.at[d])
        else:
            g = term
    for d in dx_far:
        gx = lax.rem(ex + d, EX)
        term = dense_send[at(ey * EX + gx, R), F : 2 * F].astype(F32)
        for dy in range(1, EY):
            pltpu.make_async_remote_copy(
                src_ref=dense_send.at[pl.ds(0, R), pl.ds(F, F)],
                dst_ref=db_recv.at[dy, gx],
                send_sem=send_b.at[0],
                recv_sem=recv_b.at[dy * EX + gx],
                device_id={"ep": e},
                device_id_type=MESH,
            ).wait_recv()
            term += db_recv[dy, gx].astype(F32)
        if d:
            b2_send[d] = term.astype(BF16)
            got_b[d] = ep_start(4, d, b2_send.at[d], b2_recv.at[d])
        else:
            u = term

    xrecv[:, at(2 * e + tc, HD)] = disp_send[at(e, S), :]

    def forward(k):
        region = xrecv.at[:, at(2 * ep_from(k) + tc, HD)]
        return side_start(send_fw.at[k], recv_fw.at[k], region, region)

    passed = [forward(0)]

    for k in reversed(ep_far):
        got_stat[k].wait_recv()
        tile += stat_recv[k]
    scale_l = lax.rsqrt(tile[0:Q, :] * (1.0 / D) + EPS)
    share_l = 1.0 / (1.0 + jnp.exp(-(scale_l * tile[4 : 4 + Q, :])))
    my_scale = jnp.zeros((R, 1), F32)
    my_bshare = jnp.zeros((R, 1), F32)
    for qq in range(Q):
        here = iota((R, LANES), 1) + qq * LANES == iota((R, LANES), 0) + e * R
        my_scale += jnp.sum(jnp.where(here, scale_l[qq : qq + 1, :], 0.0), axis=1, keepdims=True)
        my_bshare += jnp.sum(jnp.where(here, share_l[qq : qq + 1, :], 0.0), axis=1, keepdims=True)
    scale_row = (
        jnp.concatenate([scale_l[qq : qq + 1, :] for qq in range(Q)], axis=1) if Q > 1 else scale_l
    )
    row_scale = jnp.sum(jnp.where(row_no == my_code, scale_row, 0.0), axis=1, keepdims=True)

    for d in reversed(dy_far):
        if d:
            got_a[d].wait_recv()
            g += a2_recv[d].astype(F32)
    for d in reversed(dx_far):
        if d:
            got_b[d].wait_recv()
            u += b2_recv[d].astype(F32)
    g, u = g * my_scale, u * my_scale
    hid_all[at(e, R), :] = (g / (1.0 + jnp.exp(-g)) * u).astype(BF16)
    got_hid = {
        k: ep_start(6, k, hid_all.at[at(e, R), :], hid_all.at[at(e, R), :]) for k in ep_far
    }

    load_eg.wait()
    load_eu.wait()
    for k in reversed(ep_far):
        got_disp[k].wait_recv()
        passed.append(forward(k))
    for copy in passed:
        copy.wait_recv()
    gp = dot(xrecv[...], eg[0]) * row_scale
    up = dot(xrecv[...], eu[0]) * row_scale
    ehid = (gp / (1.0 + jnp.exp(-gp)) * up).astype(BF16)
    ehid8 = dot(spread, ehid).astype(BF16)
    for copy in load_ed:
        copy.wait()
    step = min(512, DH)
    strips = [slice(c * step, (c + 1) * step) for c in range(DH // step)]
    got_yo = []
    for i, cols in enumerate(strips):
        yo_send[:, cols] = (dot(ehid8, edc[0, :, cols]) * row_share).astype(BF16)
        got_yo.append(
            side_start(send_sb.at[i], recv_sb.at[i], yo_send.at[:, cols], yo_recv.at[:, cols])
        )
    got_fin = {}
    wide = DH // 2
    per_strip = max(1, wide // step)
    for i, (copy, cols) in enumerate(zip(got_yo, strips)):
        y = dot(ehid8, edc[1, :, cols]) * row_share
        copy.wait_recv()
        y += yo_recv[:, cols].astype(F32)
        fin_send[:, :, cols] = y.reshape(n_ep, PAD, step).astype(BF16)
        if i % per_strip == per_strip - 1:
            j = i // per_strip
            part = pl.ds(j * per_strip * step, per_strip * step)
            for k in ep_far:
                got_fin[j, k] = ep_start(
                    7 + j,
                    k,
                    fin_send.at[ep_peer(k), pl.ds(0, CAP), part],
                    fin_recv.at[e, pl.ds(0, CAP), part],
                )
    fin_recv[e] = fin_send[e]

    load_dd.wait()
    got_no = {}
    for dy in reversed(dy_far):
        for dx in range(EX):
            k = (EY - dy) % EY * EX + dx
            if k:
                got_hid[k].wait_recv()
        rows = at(lax.rem(ey + dy, EY), RC)
        dno_send[rows, :] = dot(hid_all[rows, :], dd[:, at(1 - tc, HD)]).astype(BF16)
        got_no[dy] = side_start(
            send_sb.at[4 + dy], recv_sb.at[4 + dy], dno_send.at[rows, :], dno_recv.at[rows, :]
        )
    got_dn = {}
    for dy in reversed(dy_far):
        rows = at(lax.rem(ey + dy, EY), RC)
        down = dot(hid_all[rows, :], dd[:, at(tc, HD)])
        got_no[dy].wait_recv()
        dn_send[rows, :] = (down + dno_recv[rows, :].astype(F32)).astype(BF16)
        for dx in dx_far:
            k = dy * EX + dx
            if k:
                got_dn[k] = ep_start(
                    9, k, dn_send.at[at(ep_peer(k), R), :], dn_recv.at[:, at(e, HD)]
                )
    dn_recv[:, at(e, HD)] = dn_send[at(e, R), :]

    for copy in got_fin.values():
        copy.wait_recv()
    for z in range(TZ):
        cols = slice(z * Dc, (z + 1) * Dc)
        back = fin_recv[:, :, cols].astype(F32).reshape(S8, Dc).astype(BF16)
        comb[:, cols] = dot(pick, back)
    for k in reversed(ep_far):
        got_dn[k].wait_recv()
    got_tp = {}
    for dz in dz_far + [0]:
        cols = at(lax.rem(tz + dz, TZ), Dc)
        piece = comb[:, cols] + my_bshare * dn_recv[:, cols].astype(F32)
        tp_send[:, cols] = piece.astype(BF16)
        if dz:
            got_tp[dz] = tp_start(2, 2 * dz, tp_send.at[:, cols], tp_recv.at[dz])

    for i in range(2):

        @pl.when(jnp.logical_not(jnp.logical_and(t == 0, e == i)))
        def _():
            pltpu.make_async_remote_copy(
                src_ref=res_all.at[pl.ds(0, R), pl.ds(0, HD)],
                dst_ref=res_t.at[:, pl.ds(i * HD, HD)],
                send_sem=send_tr.at[1 + i],
                recv_sem=recv_tr.at[1 + i],
                device_id={"tp": sibling},
                device_id_type=MESH,
            ).wait_recv()

    last = res_t[...].astype(F32) + tp_send[:, at(tz, Dc)].astype(F32)
    for dz in reversed(dz_far):
        got_tp[dz].wait_recv()
        last += tp_recv[dz].astype(F32)
    out_all[:, at(tc * TZ + tz, Dc)] = last.astype(BF16)

    def out_cols(tt):
        return out_all.at[:, at(lax.rem(tt, 2) * TZ + tt // 2, Dc)]

    got_out = spread_tp(3, out_cols, dz_far)
    for k in ep_far:
        mix_copy(k).wait_send()

    @pl.when(t != 0)
    def _():
        mix_copy(0).wait_send()

    @pl.when(jnp.logical_not(stays))
    def _():
        half_copy(0).wait_send()

    half_copy(1).wait_send()
    for g in range(n_ep):

        @pl.when(g % EX != ex)
        def _():
            stage_a(g).wait_send()

        @pl.when(g // EX != ey)
        def _():
            stage_b(g).wait_send()

    gather_tp(3, out_cols, got_out)
    for b in range(n_ep):
        for c in range(2):
            out_ref[:, pl.ds((2 * b + c) * HD, HD)] = out_all[:, pl.ds(c * DH + b * HD, HD)]
    for copy in pending:
        copy.wait_send()
    store_mat.wait()


def store_kernel(chunks, *refs):
    bufs, sems = refs[8:12], refs[12]
    rows = refs[3].shape[0] // chunks
    moves = [(refs[i], bufs[i], refs[4 + i]) for i in range(3)]
    for c in range(chunks):
        part = pl.ds(c * rows, rows)
        moves.append((refs[3].at[part], bufs[3].at[part], refs[7].at[part]))
    inward = [pltpu.make_async_copy(m[0], m[1], sems.at[0, i]) for i, m in enumerate(moves)]
    outward = [pltpu.make_async_copy(m[1], m[2], sems.at[1, i]) for i, m in enumerate(moves)]
    for copy in inward:
        copy.start()
    for came, goes in zip(inward, outward):
        came.wait()
        goes.start()
    for copy in outward:
        copy.wait()


def on_device(
    n_ep,
    n_tp,
    tokens,
    state_matrix,
    state_norm,
    state_max,
    mixer_gain,
    w_query,
    w_key,
    w_value,
    w_outgate,
    w_ingate,
    w_forget,
    forget_bias,
    w_proj,
    ffn_gain,
    w_branch,
    routes,
    route_weight,
    expert_gate,
    expert_up,
    expert_down,
    dense_gate,
    dense_up,
    dense_down,
):
    R, D = tokens.shape
    hd = state_norm.shape[2]
    N, Dc, DH, W = R * n_ep, D // n_ep, D // 2, hd
    F = dense_gate.shape[1]
    FE = expert_gate.shape[2]
    S, S8 = CAP * n_ep, PAD * n_ep
    EX = {16: 4, 4: 2}[n_ep]
    EY = n_ep // EX
    vmem = pl.BlockSpec(memory_space=pltpu.VMEM)
    hbm = pl.BlockSpec(memory_space=pltpu.HBM)
    V = pltpu.VMEM
    scratch = [
        V(state_matrix.shape, F32),
        V((Dc, 4 * W), BF16),
        V((n_tp * W, Dc), BF16),
        V(expert_gate.shape, BF16),
        V(expert_up.shape, BF16),
        V((2, FE, DH), BF16),
        V((Dc, 2 * F), BF16),
        V(dense_down.shape, BF16),
        V((R, D), BF16),
        V((N, Dc), BF16),
        V((n_ep, LANES), F32),
        V((n_ep, n_ep, LANES), F32),
        V((N, 4 * W), BF16),
        V((n_ep, R, 4 * W), BF16),
        V((R, W), F32),
        V((R, W), BF16),
        V((R, n_tp * W), BF16),
        V((R, Dc), BF16),
        V((N, Dc), BF16),
        V((R, Dc), BF16),
        V((N, Dc), BF16),
        V((n_ep * S, N), BF16),
        V((8, LANES), F32),
        V((n_ep, 8, LANES), F32),
        V((N, 2 * F), BF16),
        V((EX, EY, R, F), BF16),
        V((EY, EX, R, F), BF16),
        V((EY, R, F), BF16),
        V((EY, R, F), BF16),
        V((EX, R, F), BF16),
        V((EX, R, F), BF16),
        V((n_ep * S, Dc // 2), BF16),
        V((S, D), BF16),
        V((N, F), BF16),
        V((S8, DH), BF16),
        V((S8, DH), BF16),
        V((n_ep, PAD, DH), BF16),
        V((n_ep, PAD, DH), BF16),
        V((N, Dc // 2), BF16),
        V((N, Dc // 2), BF16),
        V((N, Dc // 2), BF16),
        V((R, DH), BF16),
        V((R, DH), F32),
        V((R, DH), BF16),
        V((n_tp // 2, R, Dc), BF16),
        V((R, D), BF16),
        pltpu.SemaphoreType.DMA((12 + 2 * n_ep,)),
        pltpu.SemaphoreType.DMA((10, n_ep)),
        pltpu.SemaphoreType.DMA((10, n_ep)),
        pltpu.SemaphoreType.DMA((4, n_tp)),
        pltpu.SemaphoreType.DMA((4, n_tp)),
        pltpu.SemaphoreType.DMA((n_ep,)),
        pltpu.SemaphoreType.DMA((n_tp,)),
        pltpu.SemaphoreType.DMA((3,)),
        pltpu.SemaphoreType.DMA((3,)),
        pltpu.SemaphoreType.DMA((n_ep,)),
        pltpu.SemaphoreType.DMA((n_ep,)),
        pltpu.SemaphoreType.DMA((8,)),
        pltpu.SemaphoreType.DMA((8,)),
        pltpu.SemaphoreType.DMA((n_ep,)),
        pltpu.SemaphoreType.DMA((n_ep,)),
        pltpu.SemaphoreType.DMA((n_ep,)),
        pltpu.SemaphoreType.DMA((n_ep,)),
    ]
    Sh = jax.ShapeDtypeStruct
    results = pl.pallas_call(
        functools.partial(layer_kernel, n_ep, n_tp),
        out_shape=(
            Sh((R, D), BF16),
            Sh((R, hd), F32),
            Sh((1, R), F32),
            Sh(state_matrix.shape, F32),
        ),
        in_specs=[vmem] * 11 + [hbm] * 12,
        out_specs=(vmem,) * 3 + (hbm,),
        scratch_shapes=scratch,
        compiler_params=pltpu.CompilerParams(
            collective_id=0, has_side_effects=True, vmem_limit_bytes=66_000_000
        ),
    )(
        tokens,
        mixer_gain[None, :],
        w_ingate.T,
        w_forget.T,
        forget_bias[None, :],
        state_norm.reshape(R, hd),
        state_max.T,
        ffn_gain[None, :],
        w_branch.reshape(-1, LANES),
        routes.T,
        route_weight.T,
        state_matrix,
        w_query,
        w_key,
        w_value,
        w_outgate,
        w_proj,
        expert_gate,
        expert_up,
        expert_down,
        dense_gate,
        dense_up,
        dense_down,
    )
    layer_out, new_norm, new_max, new_matrix = pl.pallas_call(
        functools.partial(store_kernel, 8),
        out_shape=tuple(Sh(r.shape, r.dtype) for r in results),
        in_specs=[hbm] * 4,
        out_specs=(hbm,) * 4,
        scratch_shapes=[V(r.shape, r.dtype) for r in results] + [pltpu.SemaphoreType.DMA((2, 11))],
        compiler_params=pltpu.CompilerParams(vmem_limit_bytes=66_000_000),
    )(*results)
    return (layer_out, new_matrix, new_norm.reshape(R, 1, hd), new_max.T)


def solution(mesh):
    in_specs = (
        P("ep", None),
        P("ep", "tp", None, None),
        P("ep", "tp", None),
        P("ep", "tp"),
        P(),
        P("ep", "tp"),
        P("ep", "tp"),
        P("ep", "tp"),
        P("ep", "tp"),
        P(),
        P(),
        P(),
        P("tp", "ep"),
        P(),
        P(),
        P("ep", None),
        P("ep", None),
        P("ep", None, "tp"),
        P("ep", None, "tp"),
        P("ep", "tp", None),
        P("ep", "tp"),
        P("ep", "tp"),
        P("tp", "ep"),
    )
    out_specs = (P("ep", None), P("ep", "tp", None, None), P("ep", "tp", None), P("ep", "tp"))
    return jax.shard_map(
        functools.partial(on_device, mesh.shape["ep"], mesh.shape["tp"]),
        mesh=mesh,
        in_specs=in_specs,
        out_specs=out_specs,
        check_vma=False,
    )
```
